256 devices in a mesh: tp: 32 (over z, x), dp: 8 (over y, core).
Axes of the slice: x: 4, y: 4, z: 8, core: 2. Of those that a mesh axis runs over, the one named last changes fastest.
Arguments:
- tokens: bfloat16 [256, 8, 4096], P('dp', None, 'tp'), may hold values from -12 to 12
- lengths: int32 [256], P('dp'), may hold values from 1 to 8, 768 in all
- norm_gains: float32 [2, 4096], replicated, may hold values from 0.1 to 1.9
- drive_proj: bfloat16 [2, 4096, 2048], P(None, 'dp', 'tp'), may hold values from -0.09375 to 0.09375
- open_proj: bfloat16 [2, 4096, 4096], P(None, 'dp', 'tp'), may hold values from -0.09375 to 0.09375
- glu_proj: bfloat16 [2, 2048, 2048], P(None, 'dp', 'tp'), may hold values from -0.125 to 0.125
- merge_proj: bfloat16 [2, 2048, 4096], P(None, 'dp', 'tp'), may hold values from -0.125 to 0.125
- exit_proj: bfloat16 [2, 4096, 4096], P(None, 'dp', 'tp'), may hold values from -0.09375 to 0.09375
- decay_rate: float32 [2, 128, 64], P(None, 'tp'), may hold values from 0.5 to 2
- turn_rate: float32 [2, 128, 64], P(None, 'tp'), may hold values from -3 to 3
- group_step_width: float32 [2, 128], P(None, 'tp'), may hold values from 0.005 to 0.3
- state_in: float32 [2, 2, 128, 64, 16], P(None, None, 'tp'), may hold values from -1 to 1
- state_out: float32 [2, 2, 128, 16, 64], P(None, None, 'tp'), may hold values from -0.5 to 0.5
- skip_gain: float32 [2, 2048], P(None, 'tp'), may hold values from -4 to 4
- carried_state: float32 [2, 2, 256, 8192], P(None, None, 'dp', 'tp'), may hold values from -6 to 6
Outputs:
- updated_tokens: bfloat16 [256, 8, 4096], P('dp', None, 'tp')
- new_state: float32 [2, 2, 256, 8192], P(None, None, 'dp', 'tp')
The draws below stay inside these ranges and needn't reach their ends.
Inputs may be any that keep to these rules, and one draw needn't show every extreme that they name: `lengths`: each sequence has at least one live slot, and some sequence has all 8.
All inputs are finite; a program needn't handle non-finite values. No bound on the sum of `lengths` on one device may be relied on, other than what follows from the above.
Results may differ from the reference program's by a relative error of at most 0.0055.
Values may be sent and summed in bfloat16 or wider, within the bound.
A program may use at most 64 MiB of HBM per device.

```python
import math
import jax
import jax.numpy as jnp
import numpy as np
from jax import lax

D = 4096
WIDTH = 2048
CHANNELS = 16
STATE = 64
STEPS = 8
LAYERS = 2
GROUPS = 128
BATCH = 256


def draw_tokens(key, part):
    first_key, second_key = jax.random.split(jax.random.fold_in(key, 11))
    block_count = 32
    blocks = jax.random.uniform(second_key, (BATCH, 1, block_count, 1), jnp.float32, math.log(0.3), math.log(3.0))
    factor = jnp.exp(blocks)
    values_drawn = jnp.clip(jax.random.normal(first_key, (BATCH, STEPS, block_count, D // block_count), jnp.float32), -4.0, 4.0)
    return (values_drawn * factor).reshape(BATCH, STEPS, D).astype(jnp.bfloat16)


def levels(key, shape, cuts, low, top_value):
    def one(dim, shards_of):
        heights = jax.random.uniform(jax.random.fold_in(jax.random.fold_in(key, 6), dim), (shards_of,), jnp.float32, low / len(cuts), top_value / len(cuts))
        return jnp.repeat(jnp.exp(heights), shape[dim] // shards_of).reshape((-1,) + (1,) * (len(shape) - dim - 1))

    gain = one(*cuts[0])
    for cut in cuts[1:]:
        gain = gain * one(*cut)
    return gain


def split_up(number_of, total, limit, slope):
    loads = [(1 << 20) // math.isqrt(grade ** slope) + 1 for grade in range(2, number_of + 1)]
    surplus, holding = total - limit - (number_of - 1), [1] * (number_of - 1)
    while surplus > 0:
        movable = [i for i in range(number_of - 1) if holding[i] < limit]
        pool, left = sum([loads[i] for i in movable]), surplus
        for i in movable:
            more = min(limit - holding[i], max(1, left * loads[i] // pool), surplus)
            holding[i] = holding[i] + more
            surplus = surplus - more
    return np.array([limit] + holding)


def uneven(stream_key, amount, total, reach, lean):
    if amount == 2:
        one = jax.random.randint(stream_key, (), max(1, total - reach), min(reach, total - 1) + 1)
        return jnp.stack([one, total - one])
    sizes = jnp.asarray(split_up(amount, total, reach, lean), jnp.int32)
    twos = (amount - 1) // 2
    donor, sink = sizes[1:1 + 2 * twos:2], sizes[2:2 + 2 * twos:2]
    room = jnp.minimum(donor - 1, reach - sink)
    passed = jax.random.randint(jax.random.fold_in(stream_key, 1), (twos,), 0, 1 << 20) % (room + 1)
    sizes = sizes.at[1:1 + 2 * twos:2].set(donor - passed).at[2:2 + 2 * twos:2].set(sink + passed)
    return sizes[jax.random.permutation(jax.random.fold_in(stream_key, 2), amount)]


def gaussian(stream_key, extent, scale, limit, cuts=(), dtype=jnp.bfloat16):
    loudness = levels(stream_key, extent, cuts, -0.22, 0.18) if cuts else 1.0
    array = jax.random.normal(stream_key, extent, jnp.float32) * scale * loudness
    return jnp.minimum(jnp.maximum(array, -limit), limit).astype(dtype)


def setup_inputs(seed: int = 0) -> dict:
    splits = jax.random.split(jax.random.key(seed), 16)
    return {
        "tokens": draw_tokens(jax.random.fold_in(splits[15], 71), 0),
        "lengths": uneven(splits[1], BATCH, 3 * BATCH, STEPS, 2).astype(jnp.int32),
        "norm_gains": jnp.clip(1.0 + 0.18 * jax.random.normal(splits[2], (LAYERS, D), jnp.float32), 0.1, 1.9),
        "drive_proj": gaussian(splits[3], (LAYERS, D, WIDTH), D ** -0.5, 0.09375, ((1, 8), (2, 32))),
        "open_proj": gaussian(splits[4], (LAYERS, D, D), D ** -0.5, 0.09375, ((1, 8), (2, 32))),
        "glu_proj": gaussian(splits[5], (LAYERS, WIDTH, WIDTH), WIDTH ** -0.5, 0.125, ((1, 8), (2, 32))),
        "merge_proj": gaussian(splits[6], (LAYERS, WIDTH, D), WIDTH ** -0.5, 0.125, ((1, 8), (2, 32))),
        "exit_proj": gaussian(splits[7], (LAYERS, D, D), D ** -0.5, 0.09375, ((1, 8), (2, 32))),
        "decay_rate": jnp.clip(jnp.exp(math.log(2.0) - 1.3862944 * jax.random.uniform(splits[8], (LAYERS, GROUPS, STATE), jnp.float32) ** levels(splits[8], (LAYERS, GROUPS, STATE), ((1, 32),), -0.2, 0.2)), 0.5, 2.0),
        "turn_rate": jnp.clip(jax.random.uniform(splits[9], (LAYERS, GROUPS, STATE), jnp.float32, -3.0, 3.0) * levels(splits[9], (LAYERS, GROUPS, STATE), ((1, 32),), -0.4, 0.0), -3.0, 3.0),
        "group_step_width": jnp.clip(jnp.exp(math.log(0.3) - 4.0943446 * jax.random.uniform(splits[10], (LAYERS, GROUPS), jnp.float32) ** levels(splits[10], (LAYERS, GROUPS), ((1, 32),), -0.2, 0.2)), 0.005, 0.3),
        "state_in": gaussian(splits[11], (LAYERS, 2, GROUPS, STATE, CHANNELS), (2 * CHANNELS) ** -0.5, 1.0, ((2, 32),), jnp.float32),
        "state_out": gaussian(splits[12], (LAYERS, 2, GROUPS, CHANNELS, STATE), (2 * STATE) ** -0.5, 0.5, ((2, 32),), jnp.float32),
        "skip_gain": gaussian(splits[13], (LAYERS, WIDTH), 1.0, 4.0, ((1, 32),), jnp.float32),
        "carried_state": gaussian(splits[14], (LAYERS, 2, BATCH, GROUPS * STATE), 1.0, 6.0, ((2, 8), (3, 32)), jnp.float32),
    }


EPS = 1e-05

def state_update(drive, active, current_rate, turn_now, size_now, in_pair, output_couple, skip_now, carried):
    sequences, positions = active.shape
    groups, entries = current_rate.shape
    members = in_pair.shape[-1]
    real_eig = -current_rate
    step_len = size_now[:, None]
    magnitude = jnp.exp(step_len * real_eig)
    decay_real = magnitude * jnp.cos(step_len * turn_now)
    decay_imag = magnitude * jnp.sin(step_len * turn_now)
    divisor = real_eig * real_eig + turn_now * turn_now
    hold_real = ((decay_real - 1.0) * real_eig + decay_imag * turn_now) / divisor
    hold_imag = (decay_imag * real_eig - (decay_real - 1.0) * turn_now) / divisor
    inject_real = hold_real[..., None] * in_pair[0] - hold_imag[..., None] * in_pair[1]
    inject_imag = hold_real[..., None] * in_pair[1] + hold_imag[..., None] * in_pair[0]
    inputs = drive.reshape(sequences, positions, groups, members)
    pushed_real = jnp.einsum('gpc,bsgc->bsgp', inject_real, inputs, precision=lax.Precision.HIGHEST)
    pushed_imag = jnp.einsum('gpc,bsgc->bsgp', inject_imag, inputs, precision=lax.Precision.HIGHEST)
    state_real_part = carried[0].reshape(sequences, groups, entries)
    state_imaginary = carried[1].reshape(sequences, groups, entries)
    readings = []
    for position in range(positions):
        active_now = (active[:, position] > 0)[:, None, None]
        moved_real = decay_real * state_real_part - decay_imag * state_imaginary + pushed_real[:, position]
        moved_imag = decay_real * state_imaginary + decay_imag * state_real_part + pushed_imag[:, position]
        state_real_part = jnp.where(active_now, moved_real, state_real_part)
        state_imaginary = jnp.where(active_now, moved_imag, state_imaginary)
        readout_value = jnp.einsum('sal,usl->usa', output_couple[0], state_real_part, precision=lax.Precision.HIGHEST) - jnp.einsum('sal,usl->usa', output_couple[1], state_imaginary, precision=lax.Precision.HIGHEST)
        readings.append(readout_value)
    readout = jnp.stack(readings, axis=1) + skip_now.reshape(groups, members) * inputs
    final = jnp.stack([state_real_part.reshape(sequences, groups * entries), state_imaginary.reshape(sequences, groups * entries)])
    return (readout.reshape(sequences * positions, groups * members), final)

def reference(tokens, lengths, norm_gains, drive_proj, open_proj, glu_proj, merge_proj, exit_proj, decay_rate, turn_rate, group_step_width, state_in, state_out, skip_gain, carried_state):
    sequences, positions, model_width = tokens.shape
    row_count = sequences * positions
    active = (lax.broadcasted_iota(jnp.int32, (sequences, positions), 1) < lengths[:, None]).astype(jnp.int32)
    active_rows = active.reshape(row_count, 1).astype(jnp.float32)
    residual = tokens.reshape(row_count, model_width)
    states = []
    for layer_index in range(LAYERS):
        values = residual.astype(jnp.float32)
        inverse_rms = lax.rsqrt(lax.optimization_barrier(jnp.mean(values * values, axis=1, keepdims=True)) + EPS)
        normed = (values * inverse_rms * norm_gains[layer_index]).astype(jnp.bfloat16)
        drive = jnp.dot(normed, drive_proj[layer_index], preferred_element_type=jnp.float32)
        gate_open = jax.nn.sigmoid(jnp.dot(normed, open_proj[layer_index], preferred_element_type=jnp.float32))
        readout, final = state_update(drive, active, decay_rate[layer_index], turn_rate[layer_index], group_step_width[layer_index], state_in[layer_index], state_out[layer_index], skip_gain[layer_index], carried_state[layer_index])
        states.append(final)
        activated = jax.nn.gelu(readout).astype(jnp.bfloat16)
        gating = jnp.dot(activated, glu_proj[layer_index], preferred_element_type=jnp.float32)
        gated = (activated.astype(jnp.float32) * jax.nn.sigmoid(gating)).astype(jnp.bfloat16)
        merged = jnp.dot(gated, merge_proj[layer_index], preferred_element_type=jnp.float32)
        mixed = (gate_open * merged).astype(jnp.bfloat16)
        branch = jnp.dot(mixed, exit_proj[layer_index], preferred_element_type=jnp.float32)
        residual = (residual.astype(jnp.float32) + active_rows * branch).astype(jnp.bfloat16)
    return (residual.reshape(sequences, positions, model_width), jnp.stack(states))
```

```python
import functools
import math

import jax
import jax.numpy as jnp
from jax import lax
from jax.experimental import pallas as pl
from jax.experimental.pallas import tpu as pltpu
from jax.sharding import PartitionSpec as P

MESH = pl.DeviceIdType.MESH
HIGH = lax.Precision.HIGHEST
EPS = 1e-05
NZ, NX, NY = 8, 4, 4
LANES = 128
F32, BF16 = jnp.float32, jnp.bfloat16
NT = (((1,), (1,)), ((), ()))
PIECES = 7


def dot(a, b, **kw):
    return jnp.dot(a, b, preferred_element_type=F32, **kw)


def dot_nt(a, b):
    return lax.dot_general(a, b, NT, preferred_element_type=F32)


def iota(shape, dim):
    return lax.broadcasted_iota(jnp.int32, shape, dim)


def ones_where(cond, dtype=BF16):
    return jnp.where(cond, 1.0, 0.0).astype(dtype)


def swap_halves(value):
    return pltpu.roll(value, 64, 1)


class Place:
    def __init__(self):
        self.tp = lax.axis_index("tp")
        self.dp = lax.axis_index("dp")
        self.z, self.x = self.tp // NX, self.tp % NX
        self.y, self.core = self.dp // 2, self.dp % 2

    def at_x(self, step):
        return (self.z * NX + (self.x + step) % NX, self.dp)

    def at_z(self, step):
        return ((self.z + step) % NZ * NX + self.x, self.dp)

    def at_y(self, step):
        return (self.tp, (self.y + step) % NY * 2 + self.core)

    def partner(self):
        return (self.tp, self.y * 2 + 1 - self.core)


def remote(ref, send, recv, device):
    return pltpu.make_async_remote_copy(
        src_ref=ref, dst_ref=ref, send_sem=send, recv_sem=recv, device_id=device, device_id_type=MESH
    )


class Gather:
    def __init__(self, place, buf, rows, send, recv):
        self.p, self.buf, self.send, self.recv = place, buf, send, recv
        self.half, self.quarter = rows // 2, rows // 4
        self.sent = []

    def lane(self, step=0):
        return pl.ds(pl.multiple_of((self.p.x + step) % NX * LANES, LANES), LANES)

    def row(self, step):
        return (self.p.z + step) % NZ

    def upper(self, step, x_step=None):
        lanes = slice(None) if x_step is None else self.lane(x_step)
        return self.buf.at[self.row(step), pl.ds(0, self.half), lanes]

    def lower(self, step):
        return self.buf.at[self.row(step), pl.ds(self.half, self.half), self.lane()]

    def lower_column(self, x_step):
        return self.buf.at[:, pl.ds(self.half, self.half), self.lane(x_step)]

    def part(self, step, which):
        return self.buf.at[self.row(step), pl.ds(which * self.quarter, self.quarter), :]

    def go(self, ref, index, device):
        copy = remote(ref, self.send.at[index], self.recv.at[index], device)
        copy.start()
        self.sent.append(copy)

    def arrive(self, ref, index):
        remote(ref, self.send.at[index], self.recv.at[index], self.p.partner()).wait_recv()

    def put(self, value):
        self.buf[self.p.z, :, self.lane()] = value

    def start(self):
        for d in range(1, NX):
            self.go(self.upper(0, 0), d - 1, self.p.at_x(d))
        for d in range(1, NZ):
            self.go(self.lower(0), 2 + d, self.p.at_z(d))

    def middle(self):
        for d in range(1, NX):
            self.arrive(self.upper(0, NX - d), d - 1)
        self.go(self.upper(0), 10, self.p.at_z(1))
        self.go(self.upper(0), 14, self.p.at_z(NZ - 1))
        for d in range(1, NZ):
            self.arrive(self.lower(NZ - d), 2 + d)
        for d in range(1, NX):
            self.go(self.lower_column(0), 17 + d, self.p.at_x(d))

    def ring(self):
        for s in range(1, 4):
            self.arrive(self.upper(NZ - s), 9 + s)
            ref = self.upper(NZ - s) if s < 3 else self.part(NZ - s, 0)
            self.go(ref, 10 + s, self.p.at_z(1))
            self.arrive(self.upper(s), 13 + s)
            ref = self.upper(s) if s < 3 else self.part(s, 1)
            self.go(ref, 14 + s, self.p.at_z(NZ - 1))

    def finish(self):
        self.arrive(self.part(4, 0), 13)
        self.arrive(self.part(4, 1), 17)
        for d in range(1, NX):
            self.arrive(self.lower_column(NX - d), 17 + d)
        for copy in self.sent:
            copy.wait_send()


class Weights:
    def __init__(self, place, wdo, wg, wm, we, y_send, y_recv, c_send, c_recv):
        self.p = place
        self.refs = (wdo, wg, wm, we)
        self.sems = (y_send, y_recv, c_send, c_recv)
        self.sent = []

    def region(self, piece, shard):
        wdo, wg, wm, we = self.refs
        if piece in (0, 3, 4, 6):
            rows = pl.ds(pl.multiple_of(shard * 512, 512), 512)
        else:
            rows = pl.ds(pl.multiple_of(shard * 256, 256), 256)
        if piece == 0:
            return wdo.at[rows, pl.ds(0, 256)]
        if piece == 4:
            return wdo.at[rows, pl.ds(256, 128)]
        if piece == 1:
            return wg.at[rows, :]
        if piece in (2, 5):
            return wm.at[(piece - 2) // 3, rows, :]
        return we.at[(piece - 3) // 3, rows, :]

    def like(self, step):
        return (self.p.y + step) % NY * 2 + self.p.core

    def unlike(self, step):
        return (self.p.y + step) % NY * 2 + 1 - self.p.core

    def y_copy(self, piece, d, shard):
        y_send, y_recv, _, _ = self.sems
        return remote(self.region(piece, shard), y_send.at[piece, d - 1], y_recv.at[piece, d - 1], self.p.at_y(d))

    def c_copy(self, piece, d, shard):
        _, _, c_send, c_recv = self.sems
        return remote(self.region(piece, shard), c_send.at[piece, d], c_recv.at[piece, d], self.p.partner())

    def begin(self, copy):
        copy.start()
        self.sent.append(copy)

    def start(self, piece):
        for d in (1, 3, 2):
            self.begin(self.y_copy(piece, d, self.p.dp))
        self.begin(self.c_copy(piece, 0, self.p.dp))

    def forward(self, piece):
        for d in (1, 3, 2):
            shard = self.like(NY - d)
            self.y_copy(piece, d, shard).wait_recv()
            self.begin(self.c_copy(piece, d, shard))

    def finish(self, piece):
        for d in range(NY):
            self.c_copy(piece, d, self.unlike((NY - d) % NY)).wait_recv()

    def drain(self):
        for copy in self.sent:
            copy.wait_send()


def kernel(
    rows,
    tokens,
    lengths,
    gains,
    drive,
    opening,
    glu,
    merge,
    leaving,
    decay,
    turn,
    step,
    s_in,
    s_out,
    skip,
    carried,
    out_tokens,
    out_state,
    wdo,
    wg,
    wm,
    we,
    gp,
    mp,
    gx,
    ga,
    pick,
    spread_seq,
    spread_slot,
    live,
    params,
    inject,
    readout_w,
    pushed,
    trail,
    y_send,
    y_recv,
    c_send,
    c_recv,
    g_send,
    g_recv,
):
    place = Place()
    half = rows // 2
    barrier = pltpu.get_barrier_semaphore()
    peers = [place.at_x(d) for d in range(1, NX)] + [place.at_z(d) for d in range(1, NZ)]
    peers += [place.at_y(d) for d in range(1, NY)] + [place.partner()]
    for peer in peers:
        pl.semaphore_signal(barrier, inc=1, device_id=peer, device_id_type=MESH)

    def gather(index):
        wide = index in (0, 3)
        return wide

    gathers = []
    for g in range(8):
        layer, kind = g // 4, g % 4
        if kind in (0, 3):
            buf, n = gx.at[layer * 2 + kind // 3], rows
        else:
            buf, n = ga.at[layer * 2 + kind - 1], half
        gathers.append(Gather(place, buf, n, g_send.at[g], g_recv.at[g]))
    weights = Weights(place, wdo, wg, wm, we, y_send, y_recv, c_send, c_recv)

    lens = lengths[...].astype(F32)
    lens_rows = jnp.broadcast_to(lens, (256, 32)).astype(BF16)
    seq, col = iota((32, 256), 0), iota((32, 256), 1)
    by_seq = lax.shift_right_logical(col, 3)
    off = dot(lens_rows[0:8], ones_where(seq < by_seq))[0:1]
    size = dot(lens_rows[0:8], ones_where(seq == by_seq))[0:1]
    slot = jnp.bitwise_and(iota((1, 256), 1), 7).astype(F32)
    target = jnp.where(slot < size, off + slot, -1.0)
    compact = ones_where(iota((rows, 256), 0).astype(F32) == target)
    residual = dot(compact, tokens[...]).astype(BF16)
    gathers[0].put(residual)

    own512 = pl.ds(pl.multiple_of(place.dp * 512, 512), 512)
    own256 = pl.ds(pl.multiple_of(place.dp * 256, 256), 256)
    wdo[own512, 0:128] = opening[0]
    wdo[own512, 128:256] = jnp.concatenate([drive[0], drive[1]], axis=1)
    wdo[own512, 256:384] = opening[1]
    wg[own256, :] = jnp.concatenate([glu[0], glu[1]], axis=1)
    for layer in range(2):
        wm[layer, own256, :] = merge[layer]
        we[layer, own512, :] = leaving[layer]

    pl.semaphore_wait(barrier, len(peers))
    gathers[0].start()
    for piece in range(PIECES):
        weights.start(piece)

    by_slot_seq = jnp.bitwise_and(col, 31)
    off = dot(lens_rows[0:8], ones_where(seq < by_slot_seq))[0:1]
    size = dot(lens_rows[0:8], ones_where(seq == by_slot_seq))[0:1]
    slot = lax.shift_right_logical(iota((1, 256), 1), 5).astype(F32)
    target = jnp.where(slot < size, off + slot, -1.0)
    pick[...] = ones_where(iota((rows, 256), 0).astype(F32) == target)
    row, other = iota((256, 32), 0), iota((256, 32), 1)
    place_of_row = iota((256, rows), 1).astype(F32)
    lens_many = jnp.broadcast_to(lens, (256, 32)).astype(BF16)
    for order, ref in ((0, spread_seq), (1, spread_slot)):
        if order == 0:
            which = lax.shift_right_logical(row, 3)
            at = jnp.bitwise_and(iota((256, 256), 0), 7).astype(F32)
        else:
            which = jnp.bitwise_and(row, 31)
            at = lax.shift_right_logical(iota((256, 256), 0), 5).astype(F32)
        off = dot_nt(ones_where(other < which), lens_many)
        size = dot_nt(ones_where(other == which), lens_many)
        target = jnp.where(at < size, off + at, -1.0)
        ref[...] = ones_where(place_of_row == target[:, 0:rows])
        live[order] = ones_where(at < size, F32)

    gathers[0].middle()

    spread64 = ones_where(iota((64, 256), 0) == jnp.bitwise_and(iota((64, 256), 1), 63), F32)
    spread16 = ones_where(iota((16, 128), 0) == jnp.bitwise_and(iota((16, 128), 1), 15), F32)
    spread2 = ones_where(iota((64, 128), 0) == jnp.bitwise_and(iota((64, 128), 1), 63), F32)
    group4 = iota((4, 256), 0) == lax.shift_right_logical(iota((4, 256), 1), 6)
    size_all = dot(step[...], ones_where(group4, F32), precision=HIGH)
    skip_all = dot(skip[...], spread2, precision=HIGH)
    for layer in range(2):
        rate = dot(decay[layer], spread64, precision=HIGH)
        rate = jnp.sum(jnp.where(group4, rate, 0.0), axis=0, keepdims=True)
        turning = dot(turn[layer], spread64, precision=HIGH)
        turning = jnp.sum(jnp.where(group4, turning, 0.0), axis=0, keepdims=True)
        length = size_all[layer : layer + 1]
        real = -rate
        magnitude = jnp.exp(length * real)
        decay_real = magnitude * jnp.cos(length * turning)
        decay_imag = magnitude * jnp.sin(length * turning)
        divisor = real * real + turning * turning
        params[layer, 0:1, :] = decay_real
        params[layer, 1:2, :] = decay_imag
        params[layer, 2:3, :] = ((decay_real - 1.0) * real + decay_imag * turning) / divisor
        params[layer, 3:4, :] = (decay_imag * real - (decay_real - 1.0) * turning) / divisor
        params[layer, 4:5, 0:128] = skip_all[layer : layer + 1]
        in_group = lax.shift_right_logical(iota((256, 128), 0), 6) == jnp.bitwise_and(
            lax.shift_right_logical(iota((256, 128), 1), 4), 3
        )
        out_group = lax.shift_right_logical(iota((64, 256), 0), 4) == lax.shift_right_logical(
            iota((64, 256), 1), 6
        )
        for part in range(2):
            wide = jnp.where(in_group, dot(s_in[layer, part], spread16, precision=HIGH), 0.0)
            high = wide.astype(BF16)
            inject[layer, part * 256 : part * 256 + 256, 0:128] = high
            inject[layer, part * 256 : part * 256 + 256, 128:256] = (wide - high.astype(F32)).astype(BF16)
            wide = jnp.where(out_group, dot(s_out[layer, part], spread64, precision=HIGH), 0.0)
            wide = (wide if part == 0 else -wide).astype(BF16)
            readout_w[layer, 0:64, part * 256 : part * 256 + 256] = wide
            readout_w[layer, 64:128, part * 256 : part * 256 + 256] = wide

    lane = iota((rows, 128), 1)
    lane_half = iota((half, 128), 1)
    low256 = iota((256, 128), 1) < 64

    def build_gp():
        zero = jnp.zeros((256, 128), BF16)
        for k in range(8):
            plain = wg[k * 256 : k * 256 + 256, :]
            turned = swap_halves(plain.astype(F32)).astype(BF16)
            for layer in range(2):
                first, second = (plain, turned) if layer == 0 else (turned, plain)
                top = jnp.where(low256, first, zero).reshape(4, 64, 128)
                bottom = jnp.where(low256, zero, second).reshape(4, 64, 128)
                gp[layer, k * 512 : k * 512 + 512, :] = jnp.concatenate([top, bottom], axis=1).reshape(512, 128)

    def build_mp(layer):
        zero = jnp.zeros((4, 64, 128), BF16)
        for k in range(8):
            plain = wm[layer, k * 256 : k * 256 + 256, :].reshape(4, 64, 128)
            mp[layer, k * 512 : k * 512 + 512, 0:128] = jnp.concatenate([plain, zero], axis=1).reshape(512, 128)
            mp[layer, k * 512 : k * 512 + 512, 128:256] = jnp.concatenate([zero, plain], axis=1).reshape(512, 128)

    def project(buf, weight):
        total = None
        for k in range(NZ):
            term = dot(buf[k], weight(k * 512, 512))
            total = term if total is None else total + term
        return total

    for layer in range(2):
        first = gathers[layer * 4]
        first.ring()
        if layer == 0:
            weights.forward(0)
        else:
            weights.finish(4)
        first.finish()
        if layer == 0:
            weights.finish(0)
        squares = None
        for k in range(NZ):
            value = first.buf[k].astype(F32)
            term = jnp.sum(value * value, axis=1, keepdims=True)
            squares = term if squares is None else squares + term
        inverse = lax.rsqrt(squares / (NZ * 512.0) + EPS)
        total = None
        for k in range(NZ):
            gain = gains[layer : layer + 1, k * 512 : k * 512 + 512]
            normed = (first.buf[k].astype(F32) * inverse * gain).astype(BF16)
            term = dot(normed, wdo[k * 512 : k * 512 + 512, layer * 128 : layer * 128 + 256])
            total = term if total is None else total + term
        lanes_open = slice(0, 128) if layer == 0 else slice(128, 256)
        lanes_drive = slice(128, 256) if layer == 0 else slice(0, 128)
        gate_open = jax.nn.sigmoid(total[:, lanes_open])
        both = total[:, lanes_drive]
        high = both.astype(BF16).astype(F32)
        rest = swap_halves(both - high)
        mine = lane < 64 if layer == 0 else lane >= 64
        split = jnp.where(mine, high, rest).astype(BF16)
        spread = dot(spread_slot[...], split)
        drives = spread + swap_halves(spread)
        spread = spread.astype(BF16)
        moved = dot_nt(jnp.concatenate([spread, spread], axis=1), inject[layer])
        hold_real, hold_imag = params[layer, 2:3, :], params[layer, 3:4, :]
        pushed[:, 0:256] = hold_real * moved[:, 0:256] - hold_imag * moved[:, 256:512]
        pushed[:, 256:512] = hold_real * moved[:, 256:512] + hold_imag * moved[:, 0:256]
        decay_real = jnp.broadcast_to(params[layer, 0:1, :], (32, 256))
        decay_imag = jnp.broadcast_to(params[layer, 1:2, :], (32, 256))
        state_real, state_imag = carried[layer, 0], carried[layer, 1]
        for t in range(8):
            now = slice(t * 32, t * 32 + 32)
            alive = live[1, now, :] > 0.5
            next_real = decay_real * state_real - decay_imag * state_imag + pushed[now, 0:256]
            next_imag = decay_real * state_imag + decay_imag * state_real + pushed[now, 256:512]
            state_real = jnp.where(alive, next_real, state_real)
            state_imag = jnp.where(alive, next_imag, state_imag)
            trail[now, 0:256] = state_real.astype(BF16)
            trail[now, 256:512] = state_imag.astype(BF16)
        out_state[layer, 0] = state_real
        out_state[layer, 1] = state_imag
        readout = dot_nt(trail[...], readout_w[layer]) + params[layer, 4:5, 0:128] * drives
        inner = math.sqrt(2.0 / math.pi) * (readout + 0.044715 * (readout * readout * readout))
        activated = (readout * (0.5 * (1.0 + jnp.tanh(inner)))).astype(BF16)
        top = dot(pick[0:half, :], activated)
        bottom = dot(pick[half:rows, :], activated)
        packed = jnp.where(lane_half < 64, top, bottom)
        second = gathers[layer * 4 + 1]
        second.put(packed.astype(BF16))
        second.start()
        if layer == 0:
            weights.forward(1)
            weights.forward(2)
        second.middle()
        if layer == 0:
            weights.finish(1)
            build_gp()
        second.ring()
        if layer == 0:
            weights.forward(3)
        second.finish()
        gating = project(second.buf, lambda k, n: gp[layer, k : k + n, :])
        gated = (packed * jax.nn.sigmoid(gating)).astype(BF16)
        third = gathers[layer * 4 + 2]
        third.put(gated)
        third.start()
        if layer == 0:
            weights.forward(4)
        third.middle()
        weights.finish(2 + 3 * layer)
        build_mp(layer)
        third.ring()
        third.finish()
        merged = project(third.buf, lambda k, n: mp[layer, k : k + n, :])
        merged = jnp.concatenate([merged[:, 0:128], merged[:, 128:256]], axis=0)
        mixed = (gate_open * merged).astype(BF16)
        fourth = gathers[layer * 4 + 3]
        fourth.put(mixed)
        fourth.start()
        if layer == 0:
            weights.forward(5)
            weights.forward(6)
        fourth.middle()
        fourth.ring()
        weights.finish(3 + 3 * layer)
        fourth.finish()
        branch = project(fourth.buf, lambda k, n: we[layer, k : k + n, :])
        residual = (residual.astype(F32) + branch).astype(BF16)
        if layer == 0:
            following = gathers[4]
            following.put(residual)
            following.start()
            following.middle()

    spread = dot(spread_seq[...], residual).astype(BF16)
    out_tokens[...] = jnp.where(live[0, :, 0:128] > 0.5, spread, tokens[...])
    weights.drain()


def block(rows, number):
    vmem = pl.BlockSpec(memory_space=pltpu.VMEM)
    half = rows // 2
    return pl.pallas_call(
        functools.partial(kernel, rows),
        name=f"layers_{rows}",
        out_shape=(
            jax.ShapeDtypeStruct((256, 128), BF16),
            jax.ShapeDtypeStruct((2, 2, 32, 256), F32),
        ),
        in_specs=[vmem] * 15,
        out_specs=(vmem, vmem),
        scratch_shapes=[
            pltpu.VMEM((4096, 384), BF16),
            pltpu.VMEM((2048, 128), BF16),
            pltpu.VMEM((2, 2048, 128), BF16),
            pltpu.VMEM((2, 4096, 128), BF16),
            pltpu.VMEM((2, 4096, 128), BF16),
            pltpu.VMEM((2, 4096, 256), BF16),
            pltpu.VMEM((4, NZ, rows, 512), BF16),
            pltpu.VMEM((4, NZ, half, 512), BF16),
            pltpu.VMEM((rows, 256), BF16),
            pltpu.VMEM((256, rows), BF16),
            pltpu.VMEM((256, rows), BF16),
            pltpu.VMEM((2, 256, 256), F32),
            pltpu.VMEM((2, 8, 256), F32),
            pltpu.VMEM((2, 512, 256), BF16),
            pltpu.VMEM((2, 128, 512), BF16),
            pltpu.VMEM((256, 512), F32),
            pltpu.VMEM((256, 512), BF16),
            pltpu.SemaphoreType.DMA((PIECES, 3)),
            pltpu.SemaphoreType.DMA((PIECES, 3)),
            pltpu.SemaphoreType.DMA((PIECES, 4)),
            pltpu.SemaphoreType.DMA((PIECES, 4)),
            pltpu.SemaphoreType.DMA((8, 21)),
            pltpu.SemaphoreType.DMA((8, 21)),
        ],
        compiler_params=pltpu.CompilerParams(
            collective_id=number, has_side_effects=True, vmem_limit_bytes=60 * 1024 * 1024
        ),
    )


def shards(tokens, lengths, norm_gains, drive, opening, glu, merge, leaving, decay, turn, step, s_in, s_out, skip, carried):
    arrays = (
        tokens.reshape(256, 128),
        lengths.reshape(1, 32),
        norm_gains,
        drive,
        opening,
        glu,
        merge,
        leaving,
        decay,
        turn,
        step,
        s_in.reshape(2, 2, 256, 16),
        s_out.reshape(2, 2, 64, 64),
        skip,
        carried,
    )
    updated, state = block(256, 0)(*arrays)
    return updated.reshape(32, 8, 128), state


def solution(mesh):
    placed = (
        P("dp", None, "tp"),
        P("dp"),
        P(),
        P(None, "dp", "tp"),
        P(None, "dp", "tp"),
        P(None, "dp", "tp"),
        P(None, "dp", "tp"),
        P(None, "dp", "tp"),
        P(None, "tp", None),
        P(None, "tp", None),
        P(None, "tp"),
        P(None, None, "tp", None, None),
        P(None, None, "tp", None, None),
        P(None, "tp"),
        P(None, None, "dp", "tp"),
    )
    return jax.shard_map(
        shards,
        mesh=mesh,
        in_specs=placed,
        out_specs=(P("dp", None, "tp"), P(None, None, "dp", "tp")),
        check_vma=False,
    )
```

```python
import math

import jax
import jax.numpy as jnp
from jax import lax
from jax.experimental import pallas as pl
from jax.experimental.pallas import tpu as pltpu
from jax.sharding import PartitionSpec as P

MESH = pl.DeviceIdType.MESH
HIGH = lax.Precision.HIGHEST
EPS = 1e-05
NZ, NX, NY, NDP = 8, 4, 4, 8
Z_ORDER, X_ORDER = (1, 7, 2, 6, 3, 5, 4), (1, 3, 2)
ROWS, STREAMS = 128, 1
PART = ROWS // STREAMS
LANES = 128
F32, BF16 = jnp.float32, jnp.bfloat16
NT = (((1,), (1,)), ((), ()))
PIECES = 7


def dot(a, b, **kw):
    return jnp.dot(a, b, preferred_element_type=F32, **kw)


def dot_nt(a, b):
    return lax.dot_general(a, b, NT, preferred_element_type=F32)


def iota(shape, dim):
    return lax.broadcasted_iota(jnp.int32, shape, dim)


def ones_where(cond, dtype=BF16):
    return jnp.where(cond, 1.0, 0.0).astype(dtype)


def swap_halves(value):
    return pltpu.roll(value, 64, 1)


class Place:
    def __init__(self):
        self.tp = lax.axis_index("tp")
        self.dp = lax.axis_index("dp")
        self.z, self.x = self.tp // NX, self.tp % NX
        self.y, self.core = self.dp // 2, self.dp % 2

    def at_x(self, step):
        return (self.z * NX + (self.x + step) % NX, self.dp)

    def at_z(self, step):
        return ((self.z + step) % NZ * NX + self.x, self.dp)

    def at_y(self, step):
        return (self.tp, (self.y + step) % NY * 2 + self.core)

    def at_dp(self, step):
        return (self.tp, (self.dp + step) % NDP)

    def partner(self):
        return (self.tp, self.y * 2 + 1 - self.core)


def remote(ref, send, recv, device):
    return pltpu.make_async_remote_copy(
        src_ref=ref, dst_ref=ref, send_sem=send, recv_sem=recv, device_id=device, device_id_type=MESH
    )


class Gather:
    def __init__(self, place, buf, send, recv):
        self.p, self.buf, self.send, self.recv = place, buf, send, recv
        self.sent = []

    def block(self, dz, dx):
        lanes = pl.ds(pl.multiple_of((self.p.x + dx) % NX * LANES, LANES), LANES)
        return self.buf.at[(self.p.z + dz) % NZ, :, lanes]

    def go(self, ref, index, device):
        copy = remote(ref, self.send.at[index], self.recv.at[index], device)
        copy.start()
        self.sent.append(copy)

    def arrive(self, ref, index):
        remote(ref, self.send.at[index], self.recv.at[index], self.p.partner()).wait_recv()

    def put(self, value):
        lanes = pl.ds(pl.multiple_of(self.p.x * LANES, LANES), LANES)
        self.buf[self.p.z, :, lanes] = value

    def start(self):
        for d in Z_ORDER:
            self.go(self.block(0, 0), d - 1, self.p.at_z(d))
        for e in X_ORDER:
            self.go(self.block(0, 0), 6 + e, self.p.at_x(e))

    def forward(self, d):
        ref = self.block(NZ - d, 0)
        self.arrive(ref, d - 1)
        for e in X_ORDER:
            self.go(ref, 6 + d * 3 + e, self.p.at_x(e))

    def finish(self):
        for e in X_ORDER:
            self.arrive(self.block(0, NX - e), 6 + e)
        for d in Z_ORDER:
            for e in X_ORDER:
                self.arrive(self.block(NZ - d, NX - e), 6 + d * 3 + e)
        for copy in self.sent:
            copy.wait_send()


class Weights:
    def __init__(self, place, wdo, wg, wm, we, y_send, y_recv, c_send, c_recv):
        self.p = place
        self.refs = (wdo, wg, wm, we)
        self.sems = (y_send, y_recv, c_send, c_recv)
        self.sent = []

    def region(self, piece, shard):
        wdo, wg, wm, we = self.refs
        if piece in (0, 3, 4, 6):
            rows = pl.ds(pl.multiple_of(shard * 512, 512), 512)
        else:
            rows = pl.ds(pl.multiple_of(shard * 256, 256), 256)
        if piece == 0:
            return wdo.at[rows, pl.ds(0, 256)]
        if piece == 4:
            return wdo.at[rows, pl.ds(256, 128)]
        if piece == 1:
            return wg.at[rows, :]
        if piece in (2, 5):
            return wm.at[(piece - 2) // 3, rows, :]
        return we.at[(piece - 3) // 3, rows, :]

    def like(self, step):
        return (self.p.y + step) % NY * 2 + self.p.core

    def unlike(self, step):
        return (self.p.y + step) % NY * 2 + 1 - self.p.core

    def y_copy(self, piece, d, shard):
        y_send, y_recv, _, _ = self.sems
        return remote(self.region(piece, shard), y_send.at[piece, d - 1], y_recv.at[piece, d - 1], self.p.at_y(d))

    def c_copy(self, piece, d, shard):
        _, _, c_send, c_recv = self.sems
        return remote(self.region(piece, shard), c_send.at[piece, d], c_recv.at[piece, d], self.p.partner())

    def begin(self, copy):
        copy.start()
        self.sent.append(copy)

    def start(self, piece):
        for d in (1, 3, 2):
            self.begin(self.y_copy(piece, d, self.p.dp))
        self.begin(self.c_copy(piece, 0, self.p.dp))

    def forward(self, piece):
        for d in (1, 3, 2):
            shard = self.like(NY - d)
            self.y_copy(piece, d, shard).wait_recv()
            self.begin(self.c_copy(piece, d, shard))

    def finish(self, piece):
        for d in range(NY):
            self.c_copy(piece, d, self.unlike((NY - d) % NY)).wait_recv()

    def drain(self):
        for copy in self.sent:
            copy.wait_send()


def kernel(
    tokens,
    lengths,
    base,
    gains,
    drive,
    opening,
    glu,
    merge,
    leaving,
    decay,
    turn,
    step,
    s_in,
    s_out,
    skip,
    carried,
    out_tokens,
    out_state,
    out_count,
    wdo,
    wg,
    wm,
    we,
    gp,
    mp,
    gx,
    ga,
    pick,
    spread_seq,
    spread_slot,
    live_seq,
    live_slot,
    params,
    inject,
    readout_w,
    pushed,
    trail,
    counts,
    y_send,
    y_recv,
    c_send,
    c_recv,
    g_send,
    g_recv,
    n_send,
    n_recv,
):
    place = Place()
    half = PART // 2
    barrier = pltpu.get_barrier_semaphore()
    peers = [place.at_x(d) for d in range(1, NX)] + [place.at_z(d) for d in range(1, NZ)]
    peers += [place.at_dp(d) for d in range(1, NDP)]
    for peer in peers:
        pl.semaphore_signal(barrier, inc=1, device_id=peer, device_id_type=MESH)

    gathers = {}
    for layer in range(2):
        for kind in range(4):
            for s in range(STREAMS):
                ref = (gx.at[layer, kind // 3, s]) if kind in (0, 3) else ga.at[layer, kind - 1, s]
                index = (layer * 4 + kind) * STREAMS + s
                gathers[layer, kind, s] = Gather(place, ref, g_send.at[index], g_recv.at[index])
    weights = Weights(place, wdo, wg, wm, we, y_send, y_recv, c_send, c_recv)

    lens = lengths[...].astype(F32)
    lens_rows = jnp.broadcast_to(lens, (256, 32)).astype(BF16)
    seq, col = iota((32, 256), 0), iota((32, 256), 1)
    row, other = iota((256, 256), 0), iota((256, 256), 1)
    size_slot = dot(lens_rows, ones_where(seq == jnp.bitwise_and(col, 31)))
    is_live_slot = lax.shift_right_logical(other, 5).astype(F32) < size_slot
    counted = ones_where(is_live_slot)
    size_seq = dot(lens_rows[0:8], ones_where(seq == lax.shift_right_logical(col, 3)))[0:1]
    is_live_seq = jnp.bitwise_and(iota((1, 256), 1), 7).astype(F32) < size_seq
    rank_seq = jnp.bitwise_and(other, 7) * 32 + lax.shift_right_logical(other, 3)
    number_seq = dot(counted[0:8], ones_where(row < rank_seq))[0:1]
    origin = base[...]
    target = jnp.where(is_live_seq, number_seq - origin, -1.0)
    residuals = []
    for s in range(STREAMS):
        compact = ones_where((iota((PART, 256), 0) + s * PART).astype(F32) == target)
        residual = dot(compact, tokens[...]).astype(BF16)
        gathers[0, 0, s].put(residual)
        residuals.append(residual)

    own512 = pl.ds(pl.multiple_of(place.dp * 512, 512), 512)
    own256 = pl.ds(pl.multiple_of(place.dp * 256, 256), 256)
    wdo[own512, 0:128] = opening[0]
    wdo[own512, 128:256] = drive[...].astype(F32).reshape(128, 512).T.astype(BF16)
    wdo[own512, 256:384] = opening[1]
    wg[own256, :] = glu[...].astype(F32).reshape(128, 256).T.astype(BF16)
    for layer in range(2):
        wm[layer, own256, :] = merge[layer]
        we[layer, own512, :] = leaving[layer]
    counts[place.dp] = jnp.broadcast_to(jnp.sum(lens, axis=1, keepdims=True), (8, 128))

    pl.semaphore_wait(barrier, len(peers))
    for s in range(STREAMS):
        gathers[0, 0, s].start()
    for piece in range(PIECES):
        weights.start(piece)
    noted = []
    for d in range(1, NDP):
        copy = remote(counts.at[place.dp], n_send.at[d - 1], n_recv.at[d - 1], place.at_dp(d))
        copy.start()
        noted.append(copy)

    def forward(layer, kind):
        for d in Z_ORDER:
            for s in range(STREAMS):
                gathers[layer, kind, s].forward(d)

    target = jnp.where(is_live_slot[0:1], dot(counted[0:8], ones_where(row < other))[0:1] - origin, -1.0)
    for s in range(STREAMS):
        pick[s] = ones_where((iota((PART, 256), 0) + s * PART).astype(F32) == target)
    size = dot_nt(ones_where(iota((256, 32), 1) == jnp.bitwise_and(iota((256, 32), 0), 31)), lens_rows)
    number = dot_nt(ones_where(other < row), counted) - origin
    target = jnp.where(lax.shift_right_logical(row, 5).astype(F32) < size, number, -1.0)
    for s in range(STREAMS):
        spread_slot[s] = ones_where((iota((256, PART), 1) + s * PART).astype(F32) == target[:, 0:PART])
        live_slot[s] = ones_where((target >= s * PART) & (target < (s + 1) * PART), F32)
    forward(0, 0)
    size = dot_nt(ones_where(iota((256, 32), 1) == lax.shift_right_logical(iota((256, 32), 0), 3)), lens_rows)
    rank = jnp.bitwise_and(row, 7) * 32 + lax.shift_right_logical(row, 3)
    number = dot_nt(ones_where(other < rank), counted) - origin
    target = jnp.where(jnp.bitwise_and(row, 7).astype(F32) < size, number, -1.0)[:, 0:128]
    for s in range(STREAMS):
        spread_seq[s] = ones_where((iota((256, PART), 1) + s * PART).astype(F32) == target[:, 0:PART])
    live_seq[...] = ones_where((target >= 0.0) & (target < ROWS), F32)

    spread64 = ones_where(iota((64, 256), 0) == jnp.bitwise_and(iota((64, 256), 1), 63), F32)
    spread2 = ones_where(iota((64, 128), 0) == jnp.bitwise_and(iota((64, 128), 1), 63), F32)
    group4 = iota((4, 256), 0) == lax.shift_right_logical(iota((4, 256), 1), 6)
    in_group = lax.shift_right_logical(iota((64, 256), 0), 4) == lax.shift_right_logical(iota((64, 256), 1), 6)
    size_all = dot(step[...], ones_where(group4, F32), precision=HIGH)
    skip_all = dot(skip[...], spread2, precision=HIGH)
    for layer in range(2):
        rate = dot(decay[layer], spread64, precision=HIGH)
        rate = jnp.sum(jnp.where(group4, rate, 0.0), axis=0, keepdims=True)
        turning = dot(turn[layer], spread64, precision=HIGH)
        turning = jnp.sum(jnp.where(group4, turning, 0.0), axis=0, keepdims=True)
        length = size_all[layer : layer + 1]
        real = -rate
        magnitude = jnp.exp(length * real)
        decay_real = magnitude * jnp.cos(length * turning)
        decay_imag = magnitude * jnp.sin(length * turning)
        divisor = real * real + turning * turning
        params[layer, 0:1, :] = decay_real
        params[layer, 1:2, :] = decay_imag
        params[layer, 2:3, :] = ((decay_real - 1.0) * real + decay_imag * turning) / divisor
        params[layer, 3:4, :] = (decay_imag * real - (decay_real - 1.0) * turning) / divisor
        params[layer, 4:5, 0:128] = skip_all[layer : layer + 1]
        for part in range(2):
            lanes = slice(part * 256, part * 256 + 256)
            wide = jnp.where(in_group, dot(s_in[layer, part], spread64, precision=HIGH), 0.0)
            high = wide.astype(BF16)
            low = (wide - high.astype(F32)).astype(BF16)
            for k in range(2):
                inject[layer, k * 64 : k * 64 + 64, lanes] = high
                inject[layer, 128 + k * 64 : 192 + k * 64, lanes] = low
            wide = jnp.where(in_group, dot(s_out[layer, part], spread64, precision=HIGH), 0.0)
            wide = (wide if part == 0 else -wide).astype(BF16)
            readout_w[layer, 0:64, lanes] = wide
            readout_w[layer, 64:128, lanes] = wide
    weights.forward(0)

    lane = iota((PART, 128), 1)
    lane_half = iota((half, 128), 1)
    low256 = iota((256, 128), 1) < 64

    def build_gp():
        zero = jnp.zeros((256, 128), BF16)
        for k in range(8):
            plain = wg[k * 256 : k * 256 + 256, :]
            turned = swap_halves(plain.astype(F32)).astype(BF16)
            for layer in range(2):
                first, second = (plain, turned) if layer == 0 else (turned, plain)
                top = jnp.where(low256, first, zero).reshape(4, 64, 128)
                bottom = jnp.where(low256, zero, second).reshape(4, 64, 128)
                gp[layer, k * 512 : k * 512 + 512, :] = jnp.concatenate([top, bottom], axis=1).reshape(512, 128)

    def build_mp(layer):
        zero = jnp.zeros((4, 64, 128), BF16)
        for k in range(8):
            plain = wm[layer, k * 256 : k * 256 + 256, :].reshape(4, 64, 128)
            mp[layer, k * 512 : k * 512 + 512, 0:128] = jnp.concatenate([plain, zero], axis=1).reshape(512, 128)
            mp[layer, k * 512 : k * 512 + 512, 128:256] = jnp.concatenate([zero, plain], axis=1).reshape(512, 128)

    def project(buf, weight):
        total = None
        for k in range(NZ):
            term = dot(buf[k], weight(k * 512, 512))
            total = term if total is None else total + term
        return total

    gates, branches = {}, {}

    def enter(layer, s, buf):
        squares = None
        for k in range(NZ):
            value = buf[k].astype(F32)
            term = jnp.sum(value * value, axis=1, keepdims=True)
            squares = term if squares is None else squares + term
        inverse = lax.rsqrt(squares / (NZ * 512.0) + EPS)
        total = None
        for k in range(NZ):
            gain = gains[layer : layer + 1, k * 512 : k * 512 + 512]
            normed = (buf[k].astype(F32) * inverse * gain).astype(BF16)
            term = dot(normed, wdo[k * 512 : k * 512 + 512, layer * 128 : layer * 128 + 256])
            total = term if total is None else total + term
        lanes_open = slice(0, 128) if layer == 0 else slice(128, 256)
        lanes_drive = slice(128, 256) if layer == 0 else slice(0, 128)
        gates[s] = jax.nn.sigmoid(total[:, lanes_open])
        both = total[:, lanes_drive]
        mine = lane < 64 if layer == 0 else lane >= 64
        drives = jnp.where(mine, both, swap_halves(both))
        high = drives.astype(BF16).astype(F32)
        split = jnp.where(lane < 64, high, drives - high).astype(BF16)
        spread = dot(spread_slot[s], split).astype(BF16)
        moved = dot(jnp.concatenate([spread, spread], axis=1), inject[layer])
        hold_real, hold_imag = params[layer, 2:3, :], params[layer, 3:4, :]
        pushed[:, 0:256] = hold_real * moved[:, 0:256] - hold_imag * moved[:, 256:512]
        pushed[:, 256:512] = hold_real * moved[:, 256:512] + hold_imag * moved[:, 0:256]
        decay_real = jnp.broadcast_to(params[layer, 0:1, :], (32, 256))
        decay_imag = jnp.broadcast_to(params[layer, 1:2, :], (32, 256))
        before = carried if s == 0 else out_state
        state_real, state_imag = before[layer, 0], before[layer, 1]
        for t in range(8):
            now = slice(t * 32, t * 32 + 32)
            alive = live_slot[s, now, :] > 0.5
            next_real = decay_real * state_real - decay_imag * state_imag + pushed[now, 0:256]
            next_imag = decay_real * state_imag + decay_imag * state_real + pushed[now, 256:512]
            state_real = jnp.where(alive, next_real, state_real)
            state_imag = jnp.where(alive, next_imag, state_imag)
            trail[now, 0:256] = state_real.astype(BF16)
            trail[now, 256:512] = state_imag.astype(BF16)
        out_state[layer, 0] = state_real
        out_state[layer, 1] = state_imag
        chosen = dot(pick[s], trail[...]).astype(BF16)
        readout = dot_nt(chosen, readout_w[layer]) + params[layer, 4:5, 0:128] * drives
        inner = math.sqrt(2.0 / math.pi) * (readout + 0.044715 * (readout * readout * readout))
        activated = (readout * (0.5 * (1.0 + jnp.tanh(inner)))).astype(BF16).astype(F32)
        packed = jnp.where(lane_half < 64, activated[0:half], activated[half:PART])
        branches[s] = packed
        return packed.astype(BF16)

    def switch(layer, s, buf):
        gating = project(buf, lambda k, n: gp[layer, k : k + n, :])
        return (branches[s] * jax.nn.sigmoid(gating)).astype(BF16)

    def join(layer, s, buf):
        merged = project(buf, lambda k, n: mp[layer, k : k + n, :])
        merged = jnp.concatenate([merged[:, 0:128], merged[:, 128:256]], axis=0)
        return (gates[s] * merged).astype(BF16)

    def leave(layer, s, buf):
        branch = project(buf, lambda k, n: we[layer, k : k + n, :])
        residuals[s] = (residuals[s].astype(F32) + branch).astype(BF16)
        return residuals[s]

    def ready(layer, kind):
        if kind == 0:
            weights.finish(4 * layer)
        elif kind == 1 and layer == 0:
            weights.finish(1)
            build_gp()
        elif kind == 2:
            weights.finish(2 + 3 * layer)
            build_mp(layer)
        elif kind == 3:
            weights.finish(3 + 3 * layer)

    relays = {(0, 0): (1, 2), (0, 1): (3, 4), (0, 2): (5,), (0, 3): (6,)}
    for layer in range(2):
        for kind, compute in enumerate((enter, switch, join, leave)):
            ready(layer, kind)
            following = (layer, kind + 1) if kind < 3 else (layer + 1, 0)
            for s in range(STREAMS):
                done = gathers[layer, kind, s]
                done.finish()
                value = compute(layer, s, done.buf)
                if following[0] < 2:
                    gathers[following + (s,)].put(value)
                    gathers[following + (s,)].start()
            if following[0] < 2:
                forward(*following)
            for piece in relays.get((layer, kind), ()):
                weights.forward(piece)

    spread = None
    for s in range(STREAMS):
        term = dot(spread_seq[s], residuals[s])
        spread = term if spread is None else spread + term
    out_tokens[...] = jnp.where(live_seq[...] > 0.5, spread.astype(BF16), tokens[...])
    for d in range(1, NDP):
        theirs = counts.at[(place.dp + NDP - d) % NDP]
        remote(theirs, n_send.at[d - 1], n_recv.at[d - 1], place.at_dp(d)).wait_recv()
    out_count[...] = jnp.max(counts[...], axis=0)
    for copy in noted:
        copy.wait_send()
    weights.drain()


def layers(number):
    vmem = pl.BlockSpec(memory_space=pltpu.VMEM)
    half = PART // 2
    gather_count = 8 * STREAMS
    return pl.pallas_call(
        kernel,
        name="layers",
        out_shape=(
            jax.ShapeDtypeStruct((256, 128), BF16),
            jax.ShapeDtypeStruct((2, 2, 32, 256), F32),
            jax.ShapeDtypeStruct((8, 128), F32),
        ),
        in_specs=[vmem] * 16,
        out_specs=(vmem, vmem, vmem),
        scratch_shapes=[
            pltpu.VMEM((4096, 384), BF16),
            pltpu.VMEM((2048, 128), BF16),
            pltpu.VMEM((2, 2048, 128), BF16),
            pltpu.VMEM((2, 4096, 128), BF16),
            pltpu.VMEM((2, 4096, 128), BF16),
            pltpu.VMEM((2, 4096, 256), BF16),
            pltpu.VMEM((2, 2, STREAMS, NZ, PART, 512), BF16),
            pltpu.VMEM((2, 2, STREAMS, NZ, half, 512), BF16),
            pltpu.VMEM((STREAMS, PART, 256), BF16),
            pltpu.VMEM((STREAMS, 256, PART), BF16),
            pltpu.VMEM((STREAMS, 256, PART), BF16),
            pltpu.VMEM((256, 128), F32),
            pltpu.VMEM((STREAMS, 256, 256), F32),
            pltpu.VMEM((2, 8, 256), F32),
            pltpu.VMEM((2, 256, 512), BF16),
            pltpu.VMEM((2, 128, 512), BF16),
            pltpu.VMEM((256, 512), F32),
            pltpu.VMEM((256, 512), BF16),
            pltpu.VMEM((NDP, 8, 128), F32),
            pltpu.SemaphoreType.DMA((PIECES, 3)),
            pltpu.SemaphoreType.DMA((PIECES, 3)),
            pltpu.SemaphoreType.DMA((PIECES, 4)),
            pltpu.SemaphoreType.DMA((PIECES, 4)),
            pltpu.SemaphoreType.DMA((gather_count, 31)),
            pltpu.SemaphoreType.DMA((gather_count, 31)),
            pltpu.SemaphoreType.DMA((NDP - 1,)),
            pltpu.SemaphoreType.DMA((NDP - 1,)),
        ],
        compiler_params=pltpu.CompilerParams(
            collective_id=number, has_side_effects=True, vmem_limit_bytes=60 * 1024 * 1024
        ),
    )


def shards(tokens, lengths, norm_gains, drive, opening, glu, merge, leaving, decay, turn, step, s_in, s_out, skip, carried):
    lengths = lengths.reshape(1, 32)
    rest = (
        norm_gains,
        drive.swapaxes(1, 2),
        opening,
        glu.swapaxes(1, 2),
        merge,
        leaving,
        decay,
        turn,
        step,
        s_in.swapaxes(3, 4).reshape(2, 2, 64, 64),
        s_out.reshape(2, 2, 64, 64),
        skip,
    )

    def some(number, start, tokens, state):
        return layers(number)(tokens, lengths, jnp.full((1, 1), start, F32), *rest, state)

    updated, state, count = some(0, 0.0, tokens.reshape(256, 128), carried)
    updated, state = lax.cond(
        count[0, 0] > ROWS,
        lambda tokens, state: some(1, float(ROWS), tokens, state)[0:2],
        lambda tokens, state: (tokens, state),
        updated,
        state,
    )
    return updated.reshape(32, 8, 128), state


def solution(mesh):
    placed = (
        P("dp", None, "tp"),
        P("dp"),
        P(),
        P(None, "dp", "tp"),
        P(None, "dp", "tp"),
        P(None, "dp", "tp"),
        P(None, "dp", "tp"),
        P(None, "dp", "tp"),
        P(None, "tp", None),
        P(None, "tp", None),
        P(None, "tp"),
        P(None, None, "tp", None, None),
        P(None, None, "tp", None, None),
        P(None, "tp"),
        P(None, None, "dp", "tp"),
    )
    return jax.shard_map(
        shards,
        mesh=mesh,
        in_specs=placed,
        out_specs=(P("dp", None, "tp"), P(None, None, "dp", "tp")),
        check_vma=False,
    )
```

```python
import functools
import math

import jax
import jax.numpy as jnp
from jax import lax
from jax.experimental import pallas as pl
from jax.experimental.pallas import tpu as pltpu
from jax.sharding import PartitionSpec as P

MESH = pl.DeviceIdType.MESH
HIGH = lax.Precision.HIGHEST
EPS = 1e-05
NZ, NX, NY, NDP = 8, 4, 4, 8
Z_ORDER, X_ORDER = (1, 7, 2, 6, 3, 5, 4), (1, 3, 2)
ROWS, STREAMS = 128, 2
PART = ROWS // STREAMS
LANES = 128
F32, BF16 = jnp.float32, jnp.bfloat16
NT = (((1,), (1,)), ((), ()))
PIECES = 7


def dot(a, b, **kw):
    return jnp.dot(a, b, preferred_element_type=F32, **kw)


def dot_nt(a, b):
    return lax.dot_general(a, b, NT, preferred_element_type=F32)


def iota(shape, dim):
    return lax.broadcasted_iota(jnp.int32, shape, dim)


def ones_where(cond, dtype=BF16):
    return jnp.where(cond, 1.0, 0.0).astype(dtype)


def swap_halves(value):
    return pltpu.roll(value, 64, 1)


class Place:
    def __init__(self):
        self.tp = lax.axis_index("tp")
        self.dp = lax.axis_index("dp")
        self.z, self.x = self.tp // NX, self.tp % NX
        self.y, self.core = self.dp // 2, self.dp % 2

    def at_x(self, step):
        return (self.z * NX + (self.x + step) % NX, self.dp)

    def at_z(self, step):
        return ((self.z + step) % NZ * NX + self.x, self.dp)

    def at_y(self, step):
        return (self.tp, (self.y + step) % NY * 2 + self.core)

    def at_dp(self, step):
        return (self.tp, (self.dp + step) % NDP)

    def partner(self):
        return (self.tp, self.y * 2 + 1 - self.core)


def remote(ref, send, recv, device):
    return pltpu.make_async_remote_copy(
        src_ref=ref, dst_ref=ref, send_sem=send, recv_sem=recv, device_id=device, device_id_type=MESH
    )


class Gather:
    def __init__(self, place, buf, send, recv):
        self.p, self.buf, self.send, self.recv = place, buf, send, recv

    def block(self, dz, dx):
        lanes = pl.ds(pl.multiple_of((self.p.x + dx) % NX * LANES, LANES), LANES)
        return self.buf.at[(self.p.z + dz) % NZ, :, lanes]

    def put(self, value):
        lanes = pl.ds(pl.multiple_of(self.p.x * LANES, LANES), LANES)
        self.buf[self.p.z, :, lanes] = value

    def along_x(self, ref):
        for e in X_ORDER:
            remote(ref, self.send.at[1], self.recv.at[7], self.p.at_x(e)).start()

    def start(self):
        for d in Z_ORDER:
            remote(self.block(0, 0), self.send.at[0], self.recv.at[d - 1], self.p.at_z(d)).start()
        self.along_x(self.block(0, 0))

    def forward(self, d):
        ref = self.block(NZ - d, 0)
        remote(ref, self.send.at[0], self.recv.at[d - 1], self.p.partner()).wait_recv()
        self.along_x(ref)

    def finish(self):
        seven, most = self.buf.at[pl.ds(0, 7), :, pl.ds(0, 128)], self.buf.at[:, :, pl.ds(0, 384)]
        remote(most, self.send.at[1], self.recv.at[7], self.p.partner()).wait_recv()
        remote(seven, self.send.at[0], self.recv.at[0], self.p.partner()).wait_send()
        remote(most, self.send.at[1], self.recv.at[7], self.p.partner()).wait_send()


class Weights:
    def __init__(self, place, wdo, wg, wm, we, send, recv):
        self.p = place
        self.refs = (wdo, wg, wm, we)
        self.send, self.recv = send, recv

    def region(self, piece, shard, count=1):
        wdo, wg, wm, we = self.refs
        if piece in (0, 3, 4, 6):
            rows = pl.ds(pl.multiple_of(shard * 512, 512), 512 * count)
        else:
            rows = pl.ds(pl.multiple_of(shard * 256, 256), 256 * count)
        if piece == 0:
            return wdo.at[rows, pl.ds(0, 256)]
        if piece == 4:
            return wdo.at[rows, pl.ds(256, 128)]
        if piece == 1:
            return wg.at[rows, :]
        if piece in (2, 5):
            return wm.at[(piece - 2) // 3, rows, :]
        return we.at[(piece - 3) // 3, rows, :]

    def like(self, step):
        return (self.p.y + step) % NY * 2 + self.p.core

    def unlike(self, step):
        return (self.p.y + step) % NY * 2 + 1 - self.p.core

    def y_copy(self, piece, d, shard):
        ref = self.region(piece, shard)
        return remote(ref, self.send.at[piece], self.recv.at[piece, d - 1], self.p.at_y(d))

    def c_copy(self, piece, shard, count=1):
        ref = self.region(piece, shard, count)
        return remote(ref, self.send.at[piece], self.recv.at[piece, 3], self.p.partner())

    def start(self, piece):
        for d in (1, 3, 2):
            self.y_copy(piece, d, self.p.dp).start()
        self.c_copy(piece, self.p.dp).start()

    def forward(self, piece):
        for d in (1, 3, 2):
            shard = (self.p.y + NY - d) % NY * 2 + self.p.core
            self.y_copy(piece, d, shard).wait_recv()
            self.c_copy(piece, shard).start()

    def finish(self, piece):
        self.c_copy(piece, 0, 4).wait_recv()

    def drain(self):
        for piece in range(PIECES):
            self.c_copy(piece, 0, 7).wait_send()


def kernel(
    origin,
    tokens_h,
    lengths_h,
    gains_h,
    drive_h,
    opening_h,
    glu_h,
    merge_h,
    leaving_h,
    decay_h,
    turn_h,
    step_h,
    s_in_h,
    s_out_h,
    skip_h,
    carried_h,
    out_tokens_h,
    out_state_h,
    out_count_h,
    tokens,
    lengths,
    gains,
    drive,
    glu,
    decay,
    turn,
    step,
    s_in,
    s_out,
    skip,
    carried,
    out_tokens,
    out_state,
    out_count,
    wdo,
    wg,
    wm,
    we,
    gp,
    mp,
    gx,
    ga,
    pick,
    spread_seq,
    spread_slot,
    live_seq,
    live_slot,
    params,
    inject,
    readout_w,
    pushed,
    trail,
    counts,
    w_send,
    w_recv,
    g_send,
    g_recv,
    n_sem,
    l_sem,
):
    place = Place()
    own512 = pl.ds(pl.multiple_of(place.dp * 512, 512), 512)
    own256 = pl.ds(pl.multiple_of(place.dp * 256, 256), 256)
    local = {}
    for name, source, target in (
        ("tokens", tokens_h, tokens),
        ("lengths", lengths_h, lengths),
        ("open0", opening_h.at[0], wdo.at[own512, pl.ds(0, 128)]),
        ("drive", drive_h, drive),
        ("glu", glu_h, glu),
        ("merge0", merge_h.at[0], wm.at[0, own256, :]),
        ("exit0", leaving_h.at[0], we.at[0, own512, :]),
        ("open1", opening_h.at[1], wdo.at[own512, pl.ds(256, 128)]),
        ("merge1", merge_h.at[1], wm.at[1, own256, :]),
        ("exit1", leaving_h.at[1], we.at[1, own512, :]),
        ("decay", decay_h, decay),
        ("turn", turn_h, turn),
        ("step", step_h, step),
        ("s_in", s_in_h, s_in),
        ("s_out", s_out_h, s_out),
        ("skip", skip_h, skip),
        ("gains", gains_h, gains),
        ("carried", carried_h, carried),
        ("out0", out_state.at[0], out_state_h.at[0]),
        ("out1", out_state.at[1], out_state_h.at[1]),
        ("out_tokens", out_tokens, out_tokens_h),
        ("out_count", out_count, out_count_h),
    ):
        local[name] = pltpu.make_async_copy(source, target, l_sem.at[len(local)])
        if not name.startswith("out"):
            local[name].start()
    half = PART // 2
    barrier = pltpu.get_barrier_semaphore()
    peers = [place.at_x(d) for d in range(1, NX)] + [place.at_z(d) for d in range(1, NZ)]
    peers += [place.at_dp(d) for d in range(1, NDP)]
    for peer in peers:
        pl.semaphore_signal(barrier, inc=1, device_id=peer, device_id_type=MESH)

    gathers = {}
    for layer in range(2):
        for kind in range(4):
            for s in range(STREAMS):
                ref = (gx.at[layer, kind // 3, s]) if kind in (0, 3) else ga.at[layer, kind - 1, s]
                index = (layer * 4 + kind) * STREAMS + s
                gathers[layer, kind, s] = Gather(place, ref, g_send.at[index], g_recv.at[index])
    weights = Weights(place, wdo, wg, wm, we, w_send, w_recv)

    local["lengths"].wait()
    lens = lengths[...].astype(F32)
    lens_rows = jnp.broadcast_to(lens, (256, 32)).astype(BF16)
    seq, col = iota((32, 256), 0), iota((32, 256), 1)
    row, other = iota((256, 256), 0), iota((256, 256), 1)
    size_slot = dot(lens_rows, ones_where(seq == jnp.bitwise_and(col, 31)))
    is_live_slot = lax.shift_right_logical(other, 5).astype(F32) < size_slot
    counted = ones_where(is_live_slot)
    size_seq = dot(lens_rows[0:8], ones_where(seq == lax.shift_right_logical(col, 3)))[0:1]
    is_live_seq = jnp.bitwise_and(iota((1, 256), 1), 7).astype(F32) < size_seq
    rank_seq = jnp.bitwise_and(other, 7) * 32 + lax.shift_right_logical(other, 3)
    number_seq = dot(counted[0:8], ones_where(row < rank_seq))[0:1]
    target = jnp.where(is_live_seq, number_seq - origin, -1.0)
    residuals = []
    local["tokens"].wait()
    for s in range(STREAMS):
        compact = ones_where((iota((PART, 256), 0) + s * PART).astype(F32) == target)
        residual = dot(compact, tokens[...]).astype(BF16)
        gathers[0, 0, s].put(residual)
        residuals.append(residual)

    counts[place.dp] = jnp.broadcast_to(jnp.sum(lens, axis=1, keepdims=True), (8, 128))

    pl.semaphore_wait(barrier, len(peers))
    for s in range(STREAMS):
        gathers[0, 0, s].start()
    local["drive"].wait()
    wdo[own512, 128:256] = drive[...].astype(F32).reshape(128, 512).T.astype(BF16)
    local["open0"].wait()
    weights.start(0)
    local["glu"].wait()
    wg[own256, :] = glu[...].astype(F32).reshape(128, 256).T.astype(BF16)
    weights.start(1)
    for piece, name in enumerate(("merge0", "exit0", "open1", "merge1", "exit1")):
        local[name].wait()
        weights.start(piece + 2)
    for d in range(1, NDP):
        remote(counts.at[place.dp], n_sem.at[0], n_sem.at[1], place.at_dp(d)).start()

    def forward(layer, kind):
        for s in range(STREAMS):
            for d in Z_ORDER:
                gathers[layer, kind, s].forward(d)

    target = jnp.where(is_live_slot[0:1], dot(counted[0:8], ones_where(row < other))[0:1] - origin, -1.0)
    for s in range(STREAMS):
        pick[s] = ones_where((iota((PART, 256), 0) + s * PART).astype(F32) == target)
    size = dot_nt(ones_where(iota((256, 32), 1) == jnp.bitwise_and(iota((256, 32), 0), 31)), lens_rows)
    number = dot_nt(ones_where(other < row), counted) - origin
    target = jnp.where(lax.shift_right_logical(row, 5).astype(F32) < size, number, -1.0)
    for s in range(STREAMS):
        spread_slot[s] = ones_where((iota((256, PART), 1) + s * PART).astype(F32) == target[:, 0:PART])
        live_slot[s] = ones_where((target >= s * PART) & (target < (s + 1) * PART), F32)
    forward(0, 0)
    size = dot_nt(ones_where(iota((256, 32), 1) == lax.shift_right_logical(iota((256, 32), 0), 3)), lens_rows)
    rank = jnp.bitwise_and(row, 7) * 32 + lax.shift_right_logical(row, 3)
    number = dot_nt(ones_where(other < rank), counted) - origin
    target = jnp.where(jnp.bitwise_and(row, 7).astype(F32) < size, number, -1.0)[:, 0:128]
    for s in range(STREAMS):
        spread_seq[s] = ones_where((iota((256, PART), 1) + s * PART).astype(F32) == target[:, 0:PART])
    live_seq[...] = ones_where((target >= 0.0) & (target < ROWS), F32)

    for name in ("decay", "turn", "step", "s_in", "s_out", "skip", "gains", "carried"):
        local[name].wait()
    spread64 = ones_where(iota((64, 256), 0) == jnp.bitwise_and(iota((64, 256), 1), 63), F32)
    spread2 = ones_where(iota((64, 128), 0) == jnp.bitwise_and(iota((64, 128), 1), 63), F32)
    group4 = iota((4, 256), 0) == lax.shift_right_logical(iota((4, 256), 1), 6)
    in_group = lax.shift_right_logical(iota((64, 256), 0), 4) == lax.shift_right_logical(iota((64, 256), 1), 6)
    size_all = dot(step[...], ones_where(group4, F32), precision=HIGH)
    skip_all = dot(skip[...], spread2, precision=HIGH)
    for layer in range(2):
        rate = dot(decay[layer], spread64, precision=HIGH)
        rate = jnp.sum(jnp.where(group4, rate, 0.0), axis=0, keepdims=True)
        turning = dot(turn[layer], spread64, precision=HIGH)
        turning = jnp.sum(jnp.where(group4, turning, 0.0), axis=0, keepdims=True)
        length = size_all[layer : layer + 1]
        real = -rate
        magnitude = jnp.exp(length * real)
        decay_real = magnitude * jnp.cos(length * turning)
        decay_imag = magnitude * jnp.sin(length * turning)
        divisor = real * real + turning * turning
        params[layer, 0:1, :] = decay_real
        params[layer, 1:2, :] = decay_imag
        params[layer, 2:3, :] = ((decay_real - 1.0) * real + decay_imag * turning) / divisor
        params[layer, 3:4, :] = (decay_imag * real - (decay_real - 1.0) * turning) / divisor
        params[layer, 4:5, 0:128] = skip_all[layer : layer + 1]
        for part in range(2):
            lanes = slice(part * 256, part * 256 + 256)
            wide = jnp.where(in_group, dot(s_in[layer, part], spread64, precision=HIGH), 0.0)
            high = wide.astype(BF16)
            low = (wide - high.astype(F32)).astype(BF16)
            for k in range(2):
                inject[layer, k * 64 : k * 64 + 64, lanes] = high
                inject[layer, 128 + k * 64 : 192 + k * 64, lanes] = low
            wide = jnp.where(in_group, dot(s_out[layer, part], spread64, precision=HIGH), 0.0)
            wide = (wide if part == 0 else -wide).astype(BF16)
            readout_w[layer, 0:64, lanes] = wide
            readout_w[layer, 64:128, lanes] = wide
    weights.forward(0)

    lane = iota((PART, 128), 1)
    lane_half = iota((half, 128), 1)
    low256 = iota((256, 128), 1) < 64

    def build_gp():
        zero = jnp.zeros((256, 128), BF16)
        for k in range(8):
            plain = wg[k * 256 : k * 256 + 256, :]
            turned = swap_halves(plain.astype(F32)).astype(BF16)
            for layer in range(2):
                first, second = (plain, turned) if layer == 0 else (turned, plain)
                top = jnp.where(low256, first, zero).reshape(4, 64, 128)
                bottom = jnp.where(low256, zero, second).reshape(4, 64, 128)
                gp[layer, k * 512 : k * 512 + 512, :] = jnp.concatenate([top, bottom], axis=1).reshape(512, 128)

    def build_mp(layer):
        zero = jnp.zeros((4, 64, 128), BF16)
        for k in range(8):
            plain = wm[layer, k * 256 : k * 256 + 256, :].reshape(4, 64, 128)
            mp[layer, k * 512 : k * 512 + 512, 0:128] = jnp.concatenate([plain, zero], axis=1).reshape(512, 128)
            mp[layer, k * 512 : k * 512 + 512, 128:256] = jnp.concatenate([zero, plain], axis=1).reshape(512, 128)

    def project(buf, weight):
        total = None
        for k in range(NZ):
            term = dot(buf[k], weight(k * 512, 512))
            total = term if total is None else total + term
        return total

    gates, branches = {}, {}

    def enter(layer, s, buf):
        squares = None
        for k in range(NZ):
            value = buf[k].astype(F32)
            term = jnp.sum(value * value, axis=1, keepdims=True)
            squares = term if squares is None else squares + term
        inverse = lax.rsqrt(squares / (NZ * 512.0) + EPS)
        total = None
        for k in range(NZ):
            gain = gains[layer : layer + 1, k * 512 : k * 512 + 512]
            normed = (buf[k].astype(F32) * inverse * gain).astype(BF16)
            term = dot(normed, wdo[k * 512 : k * 512 + 512, layer * 128 : layer * 128 + 256])
            total = term if total is None else total + term
        lanes_open = slice(0, 128) if layer == 0 else slice(128, 256)
        lanes_drive = slice(128, 256) if layer == 0 else slice(0, 128)
        gates[s] = jax.nn.sigmoid(total[:, lanes_open])
        both = total[:, lanes_drive]
        mine = lane < 64 if layer == 0 else lane >= 64
        drives = jnp.where(mine, both, swap_halves(both))
        high = drives.astype(BF16).astype(F32)
        split = jnp.where(lane < 64, high, drives - high).astype(BF16)
        spread = dot(spread_slot[s], split).astype(BF16)
        moved = dot(jnp.concatenate([spread, spread], axis=1), inject[layer])
        hold_real, hold_imag = params[layer, 2:3, :], params[layer, 3:4, :]
        pushed[:, 0:256] = hold_real * moved[:, 0:256] - hold_imag * moved[:, 256:512]
        pushed[:, 256:512] = hold_real * moved[:, 256:512] + hold_imag * moved[:, 0:256]
        decay_real = jnp.broadcast_to(params[layer, 0:1, :], (32, 256))
        decay_imag = jnp.broadcast_to(params[layer, 1:2, :], (32, 256))
        before = carried if s == 0 else out_state
        state_real, state_imag = before[layer, 0], before[layer, 1]
        for t in range(8):
            now = slice(t * 32, t * 32 + 32)
            alive = live_slot[s, now, :] > 0.5
            next_real = decay_real * state_real - decay_imag * state_imag + pushed[now, 0:256]
            next_imag = decay_real * state_imag + decay_imag * state_real + pushed[now, 256:512]
            state_real = jnp.where(alive, next_real, state_real)
            state_imag = jnp.where(alive, next_imag, state_imag)
            trail[now, 0:256] = state_real.astype(BF16)
            trail[now, 256:512] = state_imag.astype(BF16)
        out_state[layer, 0] = state_real
        out_state[layer, 1] = state_imag
        chosen = dot(pick[s], trail[...]).astype(BF16)
        readout = dot_nt(chosen, readout_w[layer]) + params[layer, 4:5, 0:128] * drives
        inner = math.sqrt(2.0 / math.pi) * (readout + 0.044715 * (readout * readout * readout))
        activated = (readout * (0.5 * (1.0 + jnp.tanh(inner)))).astype(BF16).astype(F32)
        packed = jnp.where(lane_half < 64, activated[0:half], activated[half:PART])
        branches[s] = packed
        return packed.astype(BF16)

    def switch(layer, s, buf):
        gating = project(buf, lambda k, n: gp[layer, k : k + n, :])
        return (branches[s] * jax.nn.sigmoid(gating)).astype(BF16)

    def join(layer, s, buf):
        merged = project(buf, lambda k, n: mp[layer, k : k + n, :])
        merged = jnp.concatenate([merged[:, 0:128], merged[:, 128:256]], axis=0)
        return (gates[s] * merged).astype(BF16)

    def leave(layer, s, buf):
        branch = project(buf, lambda k, n: we[layer, k : k + n, :])
        residuals[s] = (residuals[s].astype(F32) + branch).astype(BF16)
        return residuals[s]

    def ready(layer, kind):
        if kind == 0:
            weights.finish(4 * layer)
        elif kind == 1 and layer == 0:
            weights.finish(1)
            build_gp()
        elif kind == 2:
            weights.finish(2 + 3 * layer)
            build_mp(layer)
        elif kind == 3:
            weights.finish(3 + 3 * layer)

    relays = {(0, 0): (1, 2), (0, 1): (3, 4), (0, 2): (5,), (0, 3): (6,)}
    for layer in range(2):
        for kind, compute in enumerate((enter, switch, join, leave)):
            ready(layer, kind)
            following = (layer, kind + 1) if kind < 3 else (layer + 1, 0)
            for s in range(STREAMS):
                done = gathers[layer, kind, s]
                done.finish()
                value = compute(layer, s, done.buf)
                if following[0] < 2:
                    gathers[following + (s,)].put(value)
                    gathers[following + (s,)].start()
            if following[0] < 2:
                forward(*following)
            if kind == 0:
                local[f"out{layer}"].start()
            for piece in relays.get((layer, kind), ()):
                weights.forward(piece)

    spread = None
    for s in range(STREAMS):
        term = dot(spread_seq[s], residuals[s])
        spread = term if spread is None else spread + term
    out_tokens[...] = jnp.where(live_seq[...] > 0.5, spread.astype(BF16), tokens[...])
    local["out_tokens"].start()
    theirs = remote(counts.at[pl.ds(0, NDP - 1)], n_sem.at[0], n_sem.at[1], place.partner())
    theirs.wait_recv()
    theirs.wait_send()
    out_count[...] = jnp.max(counts[...], axis=0)
    local["out_count"].start()
    weights.drain()
    for name in ("out0", "out1", "out_tokens", "out_count"):
        local[name].wait()


def layers(number):
    anywhere = pl.BlockSpec(memory_space=pl.ANY)
    half = PART // 2
    gather_count = 8 * STREAMS
    return pl.pallas_call(
        functools.partial(kernel, float(number * ROWS)),
        name=f"layers_{number}",
        out_shape=(
            jax.ShapeDtypeStruct((256, 128), BF16),
            jax.ShapeDtypeStruct((2, 2, 32, 256), F32),
            jax.ShapeDtypeStruct((8, 128), F32),
        ),
        in_specs=[anywhere] * 15,
        out_specs=(anywhere, anywhere, anywhere),
        scratch_shapes=[
            pltpu.VMEM((256, 128), BF16),
            pltpu.VMEM((1, 32), jnp.int32),
            pltpu.VMEM((2, 4096), F32),
            pltpu.VMEM((2, 64, 512), BF16),
            pltpu.VMEM((2, 64, 256), BF16),
            pltpu.VMEM((2, 4, 64), F32),
            pltpu.VMEM((2, 4, 64), F32),
            pltpu.VMEM((2, 4), F32),
            pltpu.VMEM((2, 2, 64, 64), F32),
            pltpu.VMEM((2, 2, 64, 64), F32),
            pltpu.VMEM((2, 64), F32),
            pltpu.VMEM((2, 2, 32, 256), F32),
            pltpu.VMEM((256, 128), BF16),
            pltpu.VMEM((2, 2, 32, 256), F32),
            pltpu.VMEM((8, 128), F32),
            pltpu.VMEM((4096, 384), BF16),
            pltpu.VMEM((2048, 128), BF16),
            pltpu.VMEM((2, 2048, 128), BF16),
            pltpu.VMEM((2, 4096, 128), BF16),
            pltpu.VMEM((2, 4096, 128), BF16),
            pltpu.VMEM((2, 4096, 256), BF16),
            pltpu.VMEM((2, 2, STREAMS, NZ, PART, 512), BF16),
            pltpu.VMEM((2, 2, STREAMS, NZ, half, 512), BF16),
            pltpu.VMEM((STREAMS, PART, 256), BF16),
            pltpu.VMEM((STREAMS, 256, PART), BF16),
            pltpu.VMEM((STREAMS, 256, PART), BF16),
            pltpu.VMEM((256, 128), F32),
            pltpu.VMEM((STREAMS, 256, 256), F32),
            pltpu.VMEM((2, 8, 256), F32),
            pltpu.VMEM((2, 256, 512), BF16),
            pltpu.VMEM((2, 128, 512), BF16),
            pltpu.VMEM((256, 512), F32),
            pltpu.VMEM((256, 512), BF16),
            pltpu.VMEM((NDP, 8, 128), F32),
            pltpu.SemaphoreType.DMA((PIECES,)),
            pltpu.SemaphoreType.DMA((PIECES, 4)),
            pltpu.SemaphoreType.DMA((gather_count, 2)),
            pltpu.SemaphoreType.DMA((gather_count, 8)),
            pltpu.SemaphoreType.DMA((2,)),
            pltpu.SemaphoreType.DMA((22,)),
        ],
        compiler_params=pltpu.CompilerParams(
            collective_id=number, has_side_effects=True, vmem_limit_bytes=60 * 1024 * 1024
        ),
    )


def shards(tokens, lengths, norm_gains, drive, opening, glu, merge, leaving, decay, turn, step, s_in, s_out, skip, carried):
    lengths = lengths.reshape(1, 32)
    rest = (
        norm_gains,
        drive.swapaxes(1, 2),
        opening,
        glu.swapaxes(1, 2),
        merge,
        leaving,
        decay,
        turn,
        step,
        s_in.swapaxes(3, 4).reshape(2, 2, 64, 64),
        s_out.reshape(2, 2, 64, 64),
        skip,
    )

    def some(number, tokens, state):
        return layers(number)(tokens, lengths, *rest, state)

    updated, state, count = some(0, tokens.reshape(256, 128), carried)
    updated, state = lax.cond(
        count[0, 0] > ROWS,
        lambda tokens, state: some(1, tokens, state)[0:2],
        lambda tokens, state: (tokens, state),
        updated,
        state,
    )
    return updated.reshape(32, 8, 128), state


def solution(mesh):
    placed = (
        P("dp", None, "tp"),
        P("dp"),
        P(),
        P(None, "dp", "tp"),
        P(None, "dp", "tp"),
        P(None, "dp", "tp"),
        P(None, "dp", "tp"),
        P(None, "dp", "tp"),
        P(None, "tp", None),
        P(None, "tp", None),
        P(None, "tp"),
        P(None, None, "tp", None, None),
        P(None, None, "tp", None, None),
        P(None, "tp"),
        P(None, None, "dp", "tp"),
    )
    return jax.shard_map(
        shards,
        mesh=mesh,
        in_specs=placed,
        out_specs=(P("dp", None, "tp"), P(None, None, "dp", "tp")),
        check_vma=False,
    )
```

```python
import functools
import math

import jax
import jax.numpy as jnp
from jax import lax
from jax.experimental import pallas as pl
from jax.experimental.pallas import tpu as pltpu
from jax.sharding import PartitionSpec as P

MESH = pl.DeviceIdType.MESH
HIGH = lax.Precision.HIGHEST
EPS = 1e-05
NZ, NX, NY, NDP = 8, 4, 4, 8
Z_ORDER, X_ORDER = (1, 7, 2, 6, 3, 5, 4), (1, 3, 2)
ROWS, STREAMS = 128, 2
PART = ROWS // STREAMS
LANES = 128
F32, BF16 = jnp.float32, jnp.bfloat16
NT = (((1,), (1,)), ((), ()))
PIECES = 7


def dot(a, b, **kw):
    return jnp.dot(a, b, preferred_element_type=F32, **kw)


def dot_nt(a, b):
    return lax.dot_general(a, b, NT, preferred_element_type=F32)


def iota(shape, dim):
    return lax.broadcasted_iota(jnp.int32, shape, dim)


def ones_where(cond, dtype=BF16):
    return jnp.where(cond, 1.0, 0.0).astype(dtype)


def swap_halves(value):
    return pltpu.roll(value, 64, 1)


class Place:
    def __init__(self):
        self.tp = lax.axis_index("tp")
        self.dp = lax.axis_index("dp")
        self.z, self.x = self.tp // NX, self.tp % NX
        self.y, self.core = self.dp // 2, self.dp % 2

    def at_x(self, step):
        return (self.z * NX + (self.x + step) % NX, self.dp)

    def at_z(self, step):
        return ((self.z + step) % NZ * NX + self.x, self.dp)

    def at_y(self, step):
        return (self.tp, (self.y + step) % NY * 2 + self.core)

    def at_dp(self, step):
        return (self.tp, (self.dp + step) % NDP)

    def partner(self):
        return (self.tp, self.y * 2 + 1 - self.core)


def remote(ref, send, recv, device):
    return pltpu.make_async_remote_copy(
        src_ref=ref, dst_ref=ref, send_sem=send, recv_sem=recv, device_id=device, device_id_type=MESH
    )


class Gather:
    def __init__(self, place, buf, send, recv):
        self.p, self.buf, self.send, self.recv = place, buf, send, recv

    def block(self, dz, dx):
        lanes = pl.ds(pl.multiple_of((self.p.x + dx) % NX * LANES, LANES), LANES)
        return self.buf.at[(self.p.z + dz) % NZ, :, lanes]

    def put(self, value):
        lanes = pl.ds(pl.multiple_of(self.p.x * LANES, LANES), LANES)
        self.buf[self.p.z, :, lanes] = value

    def along_x(self, ref):
        for e in X_ORDER:
            remote(ref, self.send.at[1], self.recv.at[7], self.p.at_x(e)).start()

    def start(self):
        for d in Z_ORDER:
            remote(self.block(0, 0), self.send.at[0], self.recv.at[d - 1], self.p.at_z(d)).start()
        self.along_x(self.block(0, 0))

    def forward(self, d):
        ref = self.block(NZ - d, 0)
        remote(ref, self.send.at[0], self.recv.at[d - 1], self.p.partner()).wait_recv()
        self.along_x(ref)

    def finish(self):
        seven, most = self.buf.at[pl.ds(0, 7), :, pl.ds(0, 128)], self.buf.at[:, :, pl.ds(0, 384)]
        remote(most, self.send.at[1], self.recv.at[7], self.p.partner()).wait_recv()
        remote(seven, self.send.at[0], self.recv.at[0], self.p.partner()).wait_send()
        remote(most, self.send.at[1], self.recv.at[7], self.p.partner()).wait_send()


class Weights:
    def __init__(self, place, wdo, wg, wm, we, send, recv):
        self.p = place
        self.refs = (wdo, wg, wm, we)
        self.send, self.recv = send, recv

    def region(self, piece, shard, count=1):
        wdo, wg, wm, we = self.refs
        if piece in (0, 3, 4, 6):
            rows = pl.ds(pl.multiple_of(shard * 512, 512), 512 * count)
        else:
            rows = pl.ds(pl.multiple_of(shard * 256, 256), 256 * count)
        if piece == 0:
            return wdo.at[rows, pl.ds(0, 256)]
        if piece == 4:
            return wdo.at[rows, pl.ds(256, 128)]
        if piece == 1:
            return wg.at[rows, :]
        if piece in (2, 5):
            return wm.at[(piece - 2) // 3, rows, :]
        return we.at[(piece - 3) // 3, rows, :]

    def like(self, step):
        return (self.p.y + step) % NY * 2 + self.p.core

    def unlike(self, step):
        return (self.p.y + step) % NY * 2 + 1 - self.p.core

    def y_copy(self, piece, d, shard):
        ref = self.region(piece, shard)
        return remote(ref, self.send.at[piece], self.recv.at[piece, d - 1], self.p.at_y(d))

    def c_copy(self, piece, shard, count=1):
        ref = self.region(piece, shard, count)
        return remote(ref, self.send.at[piece], self.recv.at[piece, 3], self.p.partner())

    def start(self, piece):
        for d in (1, 3, 2):
            self.y_copy(piece, d, self.p.dp).start()
        self.c_copy(piece, self.p.dp).start()

    def forward(self, piece):
        for d in (1, 3, 2):
            shard = (self.p.y + NY - d) % NY * 2 + self.p.core
            self.y_copy(piece, d, shard).wait_recv()
            self.c_copy(piece, shard).start()

    def finish(self, piece):
        self.c_copy(piece, 0, 4).wait_recv()

    def drain(self):
        for piece in range(PIECES):
            self.c_copy(piece, 0, 7).wait_send()


def kernel(
    origin,
    tokens_h,
    lengths_h,
    gains_h,
    drive_h,
    opening_h,
    glu_h,
    merge_h,
    leaving_h,
    decay_h,
    turn_h,
    step_h,
    s_in_h,
    s_out_h,
    skip_h,
    carried_h,
    out_tokens_h,
    out_state_h,
    out_more,
    tokens,
    lengths,
    gains,
    drive,
    glu,
    decay,
    turn,
    step,
    s_in,
    s_out,
    skip,
    carried,
    out_tokens,
    out_state,
    wdo,
    wg,
    wm,
    we,
    gp,
    mp,
    gx,
    ga,
    pick,
    spread_seq,
    spread_slot,
    live_seq,
    live_slot,
    params,
    inject,
    readout_w,
    pushed,
    trail,
    counts,
    w_send,
    w_recv,
    g_send,
    g_recv,
    n_sem,
    l_sem,
):
    place = Place()
    own512 = pl.ds(pl.multiple_of(place.dp * 512, 512), 512)
    own256 = pl.ds(pl.multiple_of(place.dp * 256, 256), 256)
    local = {}
    for name, source, target in (
        ("tokens", tokens_h, tokens),
        ("lengths", lengths_h, lengths),
        ("open0", opening_h.at[0], wdo.at[own512, pl.ds(0, 128)]),
        ("drive", drive_h, drive),
        ("glu", glu_h, glu),
        ("merge0", merge_h.at[0], wm.at[0, own256, :]),
        ("exit0", leaving_h.at[0], we.at[0, own512, :]),
        ("open1", opening_h.at[1], wdo.at[own512, pl.ds(256, 128)]),
        ("merge1", merge_h.at[1], wm.at[1, own256, :]),
        ("exit1", leaving_h.at[1], we.at[1, own512, :]),
        ("decay", decay_h, decay),
        ("turn", turn_h, turn),
        ("step", step_h, step),
        ("s_in", s_in_h, s_in),
        ("s_out", s_out_h, s_out),
        ("skip", skip_h, skip),
        ("gains", gains_h, gains),
        ("carried", carried_h, carried),
        ("out0", out_state.at[0], out_state_h.at[0]),
        ("out1", out_state.at[1], out_state_h.at[1]),
        ("out_tokens", out_tokens, out_tokens_h),
    ):
        local[name] = pltpu.make_async_copy(source, target, l_sem.at[len(local)])
        if not name.startswith("out"):
            local[name].start()
    half = PART // 2
    barrier = pltpu.get_barrier_semaphore()
    peers = [place.at_x(d) for d in range(1, NX)] + [place.at_z(d) for d in range(1, NZ)]
    peers += [place.at_dp(d) for d in range(1, NDP)]
    for peer in peers:
        pl.semaphore_signal(barrier, inc=1, device_id=peer, device_id_type=MESH)

    gathers = {}
    for layer in range(2):
        for kind in range(4):
            for s in range(STREAMS):
                ref = (gx.at[layer, kind // 3, s]) if kind in (0, 3) else ga.at[layer, kind - 1, s]
                index = kind % 2 * STREAMS + s
                gathers[layer, kind, s] = Gather(place, ref, g_send.at[index], g_recv.at[index])
    weights = Weights(place, wdo, wg, wm, we, w_send, w_recv)

    local["lengths"].wait()
    lens = lengths[...].astype(F32)
    lens_rows = jnp.broadcast_to(lens, (256, 32)).astype(BF16)
    seq, col = iota((32, 256), 0), iota((32, 256), 1)
    row, other = iota((256, 256), 0), iota((256, 256), 1)
    size_slot = dot(lens_rows, ones_where(seq == jnp.bitwise_and(col, 31)))
    is_live_slot = lax.shift_right_logical(other, 5).astype(F32) < size_slot
    counted = ones_where(is_live_slot)
    size_seq = dot(lens_rows[0:8], ones_where(seq == lax.shift_right_logical(col, 3)))[0:1]
    is_live_seq = jnp.bitwise_and(iota((1, 256), 1), 7).astype(F32) < size_seq
    rank_seq = jnp.bitwise_and(other, 7) * 32 + lax.shift_right_logical(other, 3)
    number_seq = dot(counted[0:8], ones_where(row < rank_seq))[0:1]
    target = jnp.where(is_live_seq, number_seq - origin, -1.0)
    residuals = []
    local["tokens"].wait()
    for s in range(STREAMS):
        compact = ones_where((iota((PART, 256), 0) + s * PART).astype(F32) == target)
        residual = dot(compact, tokens[...]).astype(BF16)
        gathers[0, 0, s].put(residual)
        residuals.append(residual)

    counts[place.dp] = jnp.broadcast_to(jnp.sum(lens, axis=1, keepdims=True), (8, 128))

    pl.semaphore_wait(barrier, len(peers))
    for s in range(STREAMS):
        gathers[0, 0, s].start()
    local["drive"].wait()
    wdo[own512, 128:256] = drive[...].astype(F32).reshape(128, 512).T.astype(BF16)
    local["open0"].wait()
    weights.start(0)
    local["glu"].wait()
    wg[own256, :] = glu[...].astype(F32).reshape(128, 256).T.astype(BF16)
    weights.start(1)
    for piece, name in enumerate(("merge0", "exit0", "open1", "merge1", "exit1")):
        local[name].wait()
        weights.start(piece + 2)
    for d in range(1, NDP):
        remote(counts.at[place.dp], n_sem.at[0], n_sem.at[1], place.at_dp(d)).start()

    def forward(layer, kind):
        for s in range(STREAMS):
            for d in Z_ORDER:
                gathers[layer, kind, s].forward(d)

    target = jnp.where(is_live_slot[0:1], dot(counted[0:8], ones_where(row < other))[0:1] - origin, -1.0)
    for s in range(STREAMS):
        pick[s] = ones_where((iota((PART, 256), 0) + s * PART).astype(F32) == target)
    size = dot_nt(ones_where(iota((256, 32), 1) == jnp.bitwise_and(iota((256, 32), 0), 31)), lens_rows)
    number = dot_nt(ones_where(other < row), counted) - origin
    target = jnp.where(lax.shift_right_logical(row, 5).astype(F32) < size, number, -1.0)
    for s in range(STREAMS):
        spread_slot[s] = ones_where((iota((256, PART), 1) + s * PART).astype(F32) == target[:, 0:PART])
        live_slot[s] = ones_where((target >= s * PART) & (target < (s + 1) * PART), F32)
    forward(0, 0)
    size = dot_nt(ones_where(iota((256, 32), 1) == lax.shift_right_logical(iota((256, 32), 0), 3)), lens_rows)
    rank = jnp.bitwise_and(row, 7) * 32 + lax.shift_right_logical(row, 3)
    number = dot_nt(ones_where(other < rank), counted) - origin
    target = jnp.where(jnp.bitwise_and(row, 7).astype(F32) < size, number, -1.0)[:, 0:128]
    for s in range(STREAMS):
        spread_seq[s] = ones_where((iota((256, PART), 1) + s * PART).astype(F32) == target[:, 0:PART])
    live_seq[...] = ones_where((target >= 0.0) & (target < ROWS), F32)

    for name in ("decay", "turn", "step", "s_in", "s_out", "skip", "gains", "carried"):
        local[name].wait()
    spread64 = ones_where(iota((64, 256), 0) == jnp.bitwise_and(iota((64, 256), 1), 63), F32)
    spread2 = ones_where(iota((64, 128), 0) == jnp.bitwise_and(iota((64, 128), 1), 63), F32)
    group4 = iota((4, 256), 0) == lax.shift_right_logical(iota((4, 256), 1), 6)
    in_group = lax.shift_right_logical(iota((64, 256), 0), 4) == lax.shift_right_logical(iota((64, 256), 1), 6)
    size_all = dot(step[...], ones_where(group4, F32), precision=HIGH)
    skip_all = dot(skip[...], spread2, precision=HIGH)
    for layer in range(2):
        rate = dot(decay[layer], spread64, precision=HIGH)
        rate = jnp.sum(jnp.where(group4, rate, 0.0), axis=0, keepdims=True)
        turning = dot(turn[layer], spread64, precision=HIGH)
        turning = jnp.sum(jnp.where(group4, turning, 0.0), axis=0, keepdims=True)
        length = size_all[layer : layer + 1]
        real = -rate
        magnitude = jnp.exp(length * real)
        decay_real = magnitude * jnp.cos(length * turning)
        decay_imag = magnitude * jnp.sin(length * turning)
        divisor = real * real + turning * turning
        params[layer, 0:1, :] = decay_real
        params[layer, 1:2, :] = decay_imag
        params[layer, 2:3, :] = ((decay_real - 1.0) * real + decay_imag * turning) / divisor
        params[layer, 3:4, :] = (decay_imag * real - (decay_real - 1.0) * turning) / divisor
        params[layer, 4:5, 0:128] = skip_all[layer : layer + 1]
        for part in range(2):
            lanes = slice(part * 256, part * 256 + 256)
            wide = jnp.where(in_group, dot(s_in[layer, part], spread64, precision=HIGH), 0.0)
            high = wide.astype(BF16)
            low = (wide - high.astype(F32)).astype(BF16)
            for k in range(2):
                inject[layer, k * 64 : k * 64 + 64, lanes] = high
                inject[layer, 128 + k * 64 : 192 + k * 64, lanes] = low
            wide = jnp.where(in_group, dot(s_out[layer, part], spread64, precision=HIGH), 0.0)
            wide = (wide if part == 0 else -wide).astype(BF16)
            readout_w[layer, 0:64, lanes] = wide
            readout_w[layer, 64:128, lanes] = wide
    weights.forward(0)

    lane = iota((PART, 128), 1)
    lane_half = iota((half, 128), 1)
    low256 = iota((256, 128), 1) < 64

    def build_gp():
        zero = jnp.zeros((256, 128), BF16)
        for k in range(8):
            plain = wg[k * 256 : k * 256 + 256, :]
            turned = swap_halves(plain.astype(F32)).astype(BF16)
            for layer in range(2):
                first, second = (plain, turned) if layer == 0 else (turned, plain)
                top = jnp.where(low256, first, zero).reshape(4, 64, 128)
                bottom = jnp.where(low256, zero, second).reshape(4, 64, 128)
                gp[layer, k * 512 : k * 512 + 512, :] = jnp.concatenate([top, bottom], axis=1).reshape(512, 128)

    def build_mp(layer):
        zero = jnp.zeros((4, 64, 128), BF16)
        for k in range(8):
            plain = wm[layer, k * 256 : k * 256 + 256, :].reshape(4, 64, 128)
            mp[layer, k * 512 : k * 512 + 512, 0:128] = jnp.concatenate([plain, zero], axis=1).reshape(512, 128)
            mp[layer, k * 512 : k * 512 + 512, 128:256] = jnp.concatenate([zero, plain], axis=1).reshape(512, 128)

    def project(buf, weight):
        total = None
        for k in range(NZ):
            term = dot(buf[k], weight(k * 512, 512))
            total = term if total is None else total + term
        return total

    gates, branches = {}, {}

    def enter(layer, s, buf):
        squares = None
        for k in range(NZ):
            value = buf[k].astype(F32)
            term = jnp.sum(value * value, axis=1, keepdims=True)
            squares = term if squares is None else squares + term
        inverse = lax.rsqrt(squares / (NZ * 512.0) + EPS)
        total = None
        for k in range(NZ):
            gain = gains[layer : layer + 1, k * 512 : k * 512 + 512]
            normed = (buf[k].astype(F32) * inverse * gain).astype(BF16)
            term = dot(normed, wdo[k * 512 : k * 512 + 512, layer * 128 : layer * 128 + 256])
            total = term if total is None else total + term
        lanes_open = slice(0, 128) if layer == 0 else slice(128, 256)
        lanes_drive = slice(128, 256) if layer == 0 else slice(0, 128)
        gates[s] = jax.nn.sigmoid(total[:, lanes_open])
        both = total[:, lanes_drive]
        mine = lane < 64 if layer == 0 else lane >= 64
        drives = jnp.where(mine, both, swap_halves(both))
        high = drives.astype(BF16).astype(F32)
        split = jnp.where(lane < 64, high, drives - high).astype(BF16)
        spread = dot(spread_slot[s], split).astype(BF16)
        moved = dot(jnp.concatenate([spread, spread], axis=1), inject[layer])
        hold_real, hold_imag = params[layer, 2:3, :], params[layer, 3:4, :]
        pushed[:, 0:256] = hold_real * moved[:, 0:256] - hold_imag * moved[:, 256:512]
        pushed[:, 256:512] = hold_real * moved[:, 256:512] + hold_imag * moved[:, 0:256]
        decay_real = jnp.broadcast_to(params[layer, 0:1, :], (32, 256))
        decay_imag = jnp.broadcast_to(params[layer, 1:2, :], (32, 256))
        before = carried if s == 0 else out_state
        state_real, state_imag = before[layer, 0], before[layer, 1]
        for t in range(8):
            now = slice(t * 32, t * 32 + 32)
            alive = live_slot[s, now, :] > 0.5
            next_real = decay_real * state_real - decay_imag * state_imag + pushed[now, 0:256]
            next_imag = decay_real * state_imag + decay_imag * state_real + pushed[now, 256:512]
            state_real = jnp.where(alive, next_real, state_real)
            state_imag = jnp.where(alive, next_imag, state_imag)
            trail[now, 0:256] = state_real.astype(BF16)
            trail[now, 256:512] = state_imag.astype(BF16)
        out_state[layer, 0] = state_real
        out_state[layer, 1] = state_imag
        chosen = dot(pick[s], trail[...]).astype(BF16)
        readout = dot_nt(chosen, readout_w[layer]) + params[layer, 4:5, 0:128] * drives
        inner = math.sqrt(2.0 / math.pi) * (readout + 0.044715 * (readout * readout * readout))
        activated = (readout * (0.5 * (1.0 + jnp.tanh(inner)))).astype(BF16).astype(F32)
        packed = jnp.where(lane_half < 64, activated[0:half], activated[half:PART])
        branches[s] = packed
        return packed.astype(BF16)

    def switch(layer, s, buf):
        gating = project(buf, lambda k, n: gp[layer, k : k + n, :])
        return (branches[s] * jax.nn.sigmoid(gating)).astype(BF16)

    def join(layer, s, buf):
        merged = project(buf, lambda k, n: mp[layer, k : k + n, :])
        merged = jnp.concatenate([merged[:, 0:128], merged[:, 128:256]], axis=0)
        return (gates[s] * merged).astype(BF16)

    def leave(layer, s, buf):
        branch = project(buf, lambda k, n: we[layer, k : k + n, :])
        residuals[s] = (residuals[s].astype(F32) + branch).astype(BF16)
        return residuals[s]

    def ready(layer, kind):
        if kind == 0:
            weights.finish(4 * layer)
        elif kind == 1 and layer == 0:
            weights.finish(1)
            build_gp()
        elif kind == 2:
            weights.finish(2 + 3 * layer)
            build_mp(layer)
        elif kind == 3:
            weights.finish(3 + 3 * layer)

    relays = {(0, 0): (1, 2), (0, 1): (3, 4), (0, 2): (5,), (0, 3): (6,)}
    for layer in range(2):
        for kind, compute in enumerate((enter, switch, join, leave)):
            ready(layer, kind)
            following = (layer, kind + 1) if kind < 3 else (layer + 1, 0)
            for s in range(STREAMS):
                done = gathers[layer, kind, s]
                done.finish()
                value = compute(layer, s, done.buf)
                if following[0] < 2:
                    gathers[following + (s,)].put(value)
                    gathers[following + (s,)].start()
            if following[0] < 2:
                forward(*following)
            if kind == 0:
                local[f"out{layer}"].start()
            for piece in relays.get((layer, kind), ()):
                weights.forward(piece)

    spread = None
    for s in range(STREAMS):
        term = dot(spread_seq[s], residuals[s])
        spread = term if spread is None else spread + term
    out_tokens[...] = jnp.where(live_seq[...] > 0.5, spread.astype(BF16), tokens[...])
    local["out_tokens"].start()
    theirs = remote(counts.at[pl.ds(0, NDP - 1)], n_sem.at[0], n_sem.at[1], place.partner())
    theirs.wait_recv()
    theirs.wait_send()
    out_more[0, 0] = (jnp.max(counts[...]) > ROWS).astype(jnp.int32)
    weights.drain()
    for name in ("out0", "out1", "out_tokens"):
        local[name].wait()


def layers(number):
    anywhere = pl.BlockSpec(memory_space=pltpu.HBM)
    half = PART // 2
    gather_count = 2 * STREAMS
    return pl.pallas_call(
        functools.partial(kernel, float(number * ROWS)),
        name=f"layers_{number}",
        out_shape=(
            jax.ShapeDtypeStruct((256, 128), BF16),
            jax.ShapeDtypeStruct((2, 2, 32, 256), F32),
            jax.ShapeDtypeStruct((1, 1), jnp.int32),
        ),
        in_specs=[anywhere] * 15,
        out_specs=(anywhere, anywhere, pl.BlockSpec(memory_space=pltpu.SMEM)),
        scratch_shapes=[
            pltpu.VMEM((256, 128), BF16),
            pltpu.VMEM((1, 32), jnp.int32),
            pltpu.VMEM((2, 4096), F32),
            pltpu.VMEM((2, 64, 512), BF16),
            pltpu.VMEM((2, 64, 256), BF16),
            pltpu.VMEM((2, 4, 64), F32),
            pltpu.VMEM((2, 4, 64), F32),
            pltpu.VMEM((2, 4), F32),
            pltpu.VMEM((2, 2, 64, 64), F32),
            pltpu.VMEM((2, 2, 64, 64), F32),
            pltpu.VMEM((2, 64), F32),
            pltpu.VMEM((2, 2, 32, 256), F32),
            pltpu.VMEM((256, 128), BF16),
            pltpu.VMEM((2, 2, 32, 256), F32),
            pltpu.VMEM((4096, 384), BF16),
            pltpu.VMEM((2048, 128), BF16),
            pltpu.VMEM((2, 2048, 128), BF16),
            pltpu.VMEM((2, 4096, 128), BF16),
            pltpu.VMEM((2, 4096, 128), BF16),
            pltpu.VMEM((2, 4096, 256), BF16),
            pltpu.VMEM((2, 2, STREAMS, NZ, PART, 512), BF16),
            pltpu.VMEM((2, 2, STREAMS, NZ, half, 512), BF16),
            pltpu.VMEM((STREAMS, PART, 256), BF16),
            pltpu.VMEM((STREAMS, 256, PART), BF16),
            pltpu.VMEM((STREAMS, 256, PART), BF16),
            pltpu.VMEM((256, 128), F32),
            pltpu.VMEM((STREAMS, 256, 256), F32),
            pltpu.VMEM((2, 8, 256), F32),
            pltpu.VMEM((2, 256, 512), BF16),
            pltpu.VMEM((2, 128, 512), BF16),
            pltpu.VMEM((256, 512), F32),
            pltpu.VMEM((256, 512), BF16),
            pltpu.VMEM((NDP, 8, 128), F32),
            pltpu.SemaphoreType.DMA((PIECES,)),
            pltpu.SemaphoreType.DMA((PIECES, 4)),
            pltpu.SemaphoreType.DMA((gather_count, 2)),
            pltpu.SemaphoreType.DMA((gather_count, 8)),
            pltpu.SemaphoreType.DMA((2,)),
            pltpu.SemaphoreType.DMA((22,)),
        ],
        compiler_params=pltpu.CompilerParams(
            collective_id=number, has_side_effects=True, vmem_limit_bytes=60 * 1024 * 1024
        ),
    )


def shards(tokens, lengths, norm_gains, drive, opening, glu, merge, leaving, decay, turn, step, s_in, s_out, skip, carried):
    lengths = lengths.reshape(1, 32)
    rest = (
        norm_gains,
        drive.swapaxes(1, 2),
        opening,
        glu.swapaxes(1, 2),
        merge,
        leaving,
        decay,
        turn,
        step,
        s_in.swapaxes(3, 4).reshape(2, 2, 64, 64),
        s_out.reshape(2, 2, 64, 64),
        skip,
    )

    def some(number, tokens, state):
        return layers(number)(tokens, lengths, *rest, state)

    updated, state, more = some(0, tokens.reshape(256, 128), carried)
    updated, state = lax.cond(
        more[0, 0] != 0,
        lambda tokens, state: some(1, tokens, state)[0:2],
        lambda tokens, state: (tokens, state),
        updated,
        state,
    )
    return updated.reshape(32, 8, 128), state


def solution(mesh):
    placed = (
        P("dp", None, "tp"),
        P("dp"),
        P(),
        P(None, "dp", "tp"),
        P(None, "dp", "tp"),
        P(None, "dp", "tp"),
        P(None, "dp", "tp"),
        P(None, "dp", "tp"),
        P(None, "tp", None),
        P(None, "tp", None),
        P(None, "tp"),
        P(None, None, "tp", None, None),
        P(None, None, "tp", None, None),
        P(None, "tp"),
        P(None, None, "dp", "tp"),
    )
    return jax.shard_map(
        shards,
        mesh=mesh,
        in_specs=placed,
        out_specs=(P("dp", None, "tp"), P(None, None, "dp", "tp")),
        check_vma=False,
    )
```

```python
import functools
import math

import jax
import jax.numpy as jnp
from jax import lax
from jax.experimental import pallas as pl
from jax.experimental.pallas import tpu as pltpu
from jax.sharding import PartitionSpec as P

MESH = pl.DeviceIdType.MESH
HIGH = lax.Precision.HIGHEST
EPS = 1e-05
NZ, NX, NY, NDP = 8, 4, 4, 8
Z_ORDER, X_ORDER = (1, 7, 2, 6, 3, 5, 4), (1, 3, 2)
ROWS, STREAMS = 128, 2
PART = ROWS // STREAMS
LANES = 128
F32, BF16 = jnp.float32, jnp.bfloat16
NT = (((1,), (1,)), ((), ()))
PIECES = 8


def dot(a, b, **kw):
    return jnp.dot(a, b, preferred_element_type=F32, **kw)


def dot_nt(a, b):
    return lax.dot_general(a, b, NT, preferred_element_type=F32)


def iota(shape, dim):
    return lax.broadcasted_iota(jnp.int32, shape, dim)


def ones_where(cond, dtype=BF16):
    return jnp.where(cond, 1.0, 0.0).astype(dtype)


def swap_halves(value):
    return pltpu.roll(value, 64, 1)


class Place:
    def __init__(self):
        self.tp = lax.axis_index("tp")
        self.dp = lax.axis_index("dp")
        self.z, self.x = self.tp // NX, self.tp % NX
        self.y, self.core = self.dp // 2, self.dp % 2

    def at_x(self, step):
        return (self.z * NX + (self.x + step) % NX, self.dp)

    def at_z(self, step):
        return ((self.z + step) % NZ * NX + self.x, self.dp)

    def at_y(self, step):
        return (self.tp, (self.y + step) % NY * 2 + self.core)

    def at_dp(self, step):
        return (self.tp, (self.dp + step) % NDP)

    def partner(self):
        return (self.tp, self.y * 2 + 1 - self.core)


def remote(ref, send, recv, device):
    return pltpu.make_async_remote_copy(
        src_ref=ref, dst_ref=ref, send_sem=send, recv_sem=recv, device_id=device, device_id_type=MESH
    )


class Gather:
    def __init__(self, place, buf, send, recv):
        self.p, self.buf, self.send, self.recv = place, buf, send, recv

    def block(self, dz, dx):
        lanes = pl.ds(pl.multiple_of((self.p.x + dx) % NX * LANES, LANES), LANES)
        return self.buf.at[(self.p.z + dz) % NZ, :, lanes]

    def put(self, value):
        lanes = pl.ds(pl.multiple_of(self.p.x * LANES, LANES), LANES)
        self.buf[self.p.z, :, lanes] = value

    def along_x(self, ref):
        for e in X_ORDER:
            remote(ref, self.send.at[1], self.recv.at[7], self.p.at_x(e)).start()

    def start(self):
        for d in Z_ORDER:
            remote(self.block(0, 0), self.send.at[0], self.recv.at[d - 1], self.p.at_z(d)).start()
        self.along_x(self.block(0, 0))

    def forward(self, d):
        ref = self.block(NZ - d, 0)
        remote(ref, self.send.at[0], self.recv.at[d - 1], self.p.partner()).wait_recv()
        self.along_x(ref)

    def finish(self):
        seven, most = self.buf.at[pl.ds(0, 7), :, pl.ds(0, 128)], self.buf.at[:, :, pl.ds(0, 384)]
        remote(most, self.send.at[1], self.recv.at[7], self.p.partner()).wait_recv()
        remote(seven, self.send.at[0], self.recv.at[0], self.p.partner()).wait_send()
        remote(most, self.send.at[1], self.recv.at[7], self.p.partner()).wait_send()


class Weights:
    def __init__(self, place, wdo, wg, wm, we, send, recv):
        self.p = place
        self.refs = (wdo, wg, wm, we)
        self.send, self.recv = send, recv

    def region(self, piece, shard, count=1):
        wdo, wg, wm, we = self.refs
        if piece in (0, 4, 7):
            rows = pl.ds(pl.multiple_of(shard * 512, 512), 512 * count)
        else:
            rows = pl.ds(pl.multiple_of(shard * 256, 256), 256 * count)
        if piece == 0:
            return wdo.at[rows, pl.ds(128, 128)]
        if piece == 7:
            return wdo.at[rows, pl.ds(0, 128)]
        if piece == 4:
            return wdo.at[rows, pl.ds(256, 128)]
        if piece == 1:
            return wg.at[rows, :]
        if piece in (2, 5):
            return wm.at[(piece - 2) // 3, rows, :]
        return we.at[(piece - 3) // 3, pl.ds(shard, count)]

    def like(self, step):
        return (self.p.y + step) % NY * 2 + self.p.core

    def unlike(self, step):
        return (self.p.y + step) % NY * 2 + 1 - self.p.core

    def y_copy(self, piece, d, shard):
        ref = self.region(piece, shard)
        return remote(ref, self.send.at[piece], self.recv.at[piece, d - 1], self.p.at_y(d))

    def c_copy(self, piece, shard, count=1):
        ref = self.region(piece, shard, count)
        return remote(ref, self.send.at[piece], self.recv.at[piece, 3], self.p.partner())

    def start(self, piece):
        for d in (1, 3, 2):
            self.y_copy(piece, d, self.p.dp).start()
        self.c_copy(piece, self.p.dp).start()

    def forward(self, piece):
        for d in (1, 3, 2):
            shard = (self.p.y + NY - d) % NY * 2 + self.p.core
            self.y_copy(piece, d, shard).wait_recv()
            self.c_copy(piece, shard).start()

    def finish(self, piece):
        self.c_copy(piece, 0, 4).wait_recv()

    def drain(self):
        for piece in range(PIECES):
            self.c_copy(piece, 0, 7).wait_send()


def kernel(
    origin,
    tokens_h,
    lengths_h,
    gains_h,
    drive_h,
    opening_h,
    glu_h,
    merge_h,
    leaving_h,
    decay_h,
    turn_h,
    step_h,
    s_in_h,
    s_out_h,
    skip_h,
    carried_h,
    out_tokens_h,
    out_state_h,
    out_more,
    tokens,
    lengths,
    gains,
    drive,
    glu,
    decay,
    turn,
    step,
    s_in,
    s_out,
    skip,
    carried,
    out_tokens,
    out_state,
    wdo,
    wg,
    wm,
    we,
    gp,
    mp,
    gx,
    ga,
    gm,
    tx,
    rx,
    pick,
    spread_seq,
    spread_slot,
    live_seq,
    live_slot,
    params,
    inject,
    readout_w,
    pushed,
    trail,
    counts,
    w_send,
    w_recv,
    g_send,
    g_recv,
    n_sem,
    l_sem,
    q_sem,
    e_sem,
):
    place = Place()
    own512 = pl.ds(pl.multiple_of(place.dp * 512, 512), 512)
    own256 = pl.ds(pl.multiple_of(place.dp * 256, 256), 256)
    own_lanes = pl.ds(pl.multiple_of(place.x * LANES, LANES), LANES)
    own_rows = pl.ds(pl.multiple_of(place.x * 128, 128), 128)
    local = {}
    for name, source, target in (
        ("tokens", tokens_h, tokens),
        ("lengths", lengths_h, lengths),
        ("open0", opening_h.at[0], wdo.at[own512, pl.ds(0, 128)]),
        ("drive", drive_h, drive),
        ("glu", glu_h, glu),
        ("merge0", merge_h.at[0], wm.at[0, own256, :]),
        ("exit0", leaving_h.at[0, own_rows, :], we.at[0, place.dp, :, own_lanes]),
        ("open1", opening_h.at[1], wdo.at[own512, pl.ds(256, 128)]),
        ("merge1", merge_h.at[1], wm.at[1, own256, :]),
        ("exit1", leaving_h.at[1, own_rows, :], we.at[1, place.dp, :, own_lanes]),
        ("decay", decay_h, decay),
        ("turn", turn_h, turn),
        ("step", step_h, step),
        ("s_in", s_in_h, s_in),
        ("s_out", s_out_h, s_out),
        ("skip", skip_h, skip),
        ("gains", gains_h, gains),
        ("carried", carried_h, carried),
        ("out0", out_state.at[0], out_state_h.at[0]),
        ("out1", out_state.at[1], out_state_h.at[1]),
        ("out_tokens", out_tokens, out_tokens_h),
    ):
        local[name] = pltpu.make_async_copy(source, target, l_sem.at[len(local)])
        if not name.startswith("out"):
            local[name].start()
    half = PART // 2
    barrier = pltpu.get_barrier_semaphore()
    peers = [place.at_x(d) for d in range(1, NX)] + [place.at_z(d) for d in range(1, NZ)]
    peers += [place.at_dp(d) for d in range(1, NDP)]
    for peer in peers:
        pl.semaphore_signal(barrier, inc=1, device_id=peer, device_id_type=MESH)

    gathers = {}
    for layer in range(2):
        for kind in range(3):
            for s in range(STREAMS):
                ref = gx.at[layer, s] if kind == 0 else ga.at[layer, kind - 1, s]
                index = (layer * 3 + kind) % 2 * STREAMS + s
                gathers[layer, kind, s] = Gather(place, ref, g_send.at[index], g_recv.at[index])
    weights = Weights(place, wdo, wg, wm, we, w_send, w_recv)

    local["lengths"].wait()
    lens = lengths[...].astype(F32)
    lens_rows = jnp.broadcast_to(lens, (256, 32)).astype(BF16)
    seq, col = iota((32, 256), 0), iota((32, 256), 1)
    row, other = iota((256, 256), 0), iota((256, 256), 1)
    size_slot = dot(lens_rows, ones_where(seq == jnp.bitwise_and(col, 31)))
    is_live_slot = lax.shift_right_logical(other, 5).astype(F32) < size_slot
    counted = ones_where(is_live_slot)
    size_seq = dot(lens_rows[0:8], ones_where(seq == lax.shift_right_logical(col, 3)))[0:1]
    is_live_seq = jnp.bitwise_and(iota((1, 256), 1), 7).astype(F32) < size_seq
    rank_seq = jnp.bitwise_and(other, 7) * 32 + lax.shift_right_logical(other, 3)
    number_seq = dot(counted[0:8], ones_where(row < rank_seq))[0:1]
    target = jnp.where(is_live_seq, number_seq - origin, -1.0)
    residuals = []
    local["tokens"].wait()
    for s in range(STREAMS):
        compact = ones_where((iota((PART, 256), 0) + s * PART).astype(F32) == target)
        residual = dot(compact, tokens[...]).astype(BF16)
        gathers[0, 0, s].put(residual)
        residuals.append(residual)

    counts[place.dp] = jnp.broadcast_to(jnp.sum(lens, axis=1, keepdims=True), (8, 128))

    pl.semaphore_wait(barrier, len(peers))
    for s in range(STREAMS):
        gathers[0, 0, s].start()
    local["drive"].wait()
    wdo[own512, 128:256] = drive[...].astype(F32).reshape(128, 512).T.astype(BF16)
    weights.start(0)
    local["glu"].wait()
    wg[own256, :] = glu[...].astype(F32).reshape(128, 256).T.astype(BF16)
    weights.start(1)
    local["open0"].wait()
    weights.start(7)
    local["merge0"].wait()
    weights.start(2)
    for layer in range(2):
        for e in X_ORDER:
            rows = pl.ds(pl.multiple_of((place.x + e) % NX * 128, 128), 128)
            pltpu.make_async_remote_copy(
                src_ref=leaving_h.at[layer, rows, :],
                dst_ref=we.at[layer, place.dp, :, own_lanes],
                send_sem=q_sem.at[layer, 0],
                recv_sem=q_sem.at[layer, 1],
                device_id=place.at_x(e),
                device_id_type=MESH,
            ).start()

    def quarters(layer):
        ref = we.at[layer, place.dp, :, pl.ds(0, 384)]
        copy = remote(ref, q_sem.at[layer, 0], q_sem.at[layer, 1], place.partner())
        copy.wait_recv()
        copy.wait_send()
    for d in range(1, NDP):
        remote(counts.at[place.dp], n_sem.at[0], n_sem.at[1], place.at_dp(d)).start()

    def forward(layer, kind):
        for s in range(STREAMS):
            for d in Z_ORDER:
                gathers[layer, kind, s].forward(d)

    target = jnp.where(is_live_slot[0:1], dot(counted[0:8], ones_where(row < other))[0:1] - origin, -1.0)
    for s in range(STREAMS):
        pick[s] = ones_where((iota((PART, 256), 0) + s * PART).astype(F32) == target)
    size = dot_nt(ones_where(iota((256, 32), 1) == jnp.bitwise_and(iota((256, 32), 0), 31)), lens_rows)
    number = dot_nt(ones_where(other < row), counted) - origin
    target = jnp.where(lax.shift_right_logical(row, 5).astype(F32) < size, number, -1.0)
    for s in range(STREAMS):
        spread_slot[s] = ones_where((iota((256, PART), 1) + s * PART).astype(F32) == target[:, 0:PART])
        live_slot[s] = ones_where((target >= s * PART) & (target < (s + 1) * PART), F32)
    forward(0, 0)
    quarters(0)
    quarters(1)
    for piece, name in enumerate(("exit0", "open1", "merge1", "exit1")):
        local[name].wait()
        weights.start(piece + 3)
    size = dot_nt(ones_where(iota((256, 32), 1) == lax.shift_right_logical(iota((256, 32), 0), 3)), lens_rows)
    rank = jnp.bitwise_and(row, 7) * 32 + lax.shift_right_logical(row, 3)
    number = dot_nt(ones_where(other < rank), counted) - origin
    target = jnp.where(jnp.bitwise_and(row, 7).astype(F32) < size, number, -1.0)[:, 0:128]
    for s in range(STREAMS):
        spread_seq[s] = ones_where((iota((256, PART), 1) + s * PART).astype(F32) == target[:, 0:PART])
    live_seq[...] = ones_where((target >= 0.0) & (target < ROWS), F32)

    for name in ("decay", "turn", "step", "s_in", "s_out", "skip", "gains", "carried"):
        local[name].wait()
    spread64 = ones_where(iota((64, 256), 0) == jnp.bitwise_and(iota((64, 256), 1), 63), F32)
    spread2 = ones_where(iota((64, 128), 0) == jnp.bitwise_and(iota((64, 128), 1), 63), F32)
    group4 = iota((4, 256), 0) == lax.shift_right_logical(iota((4, 256), 1), 6)
    in_group = lax.shift_right_logical(iota((64, 256), 0), 4) == lax.shift_right_logical(iota((64, 256), 1), 6)
    size_all = dot(step[...], ones_where(group4, F32), precision=HIGH)
    skip_all = dot(skip[...], spread2, precision=HIGH)
    for layer in range(2):
        rate = dot(decay[layer], spread64, precision=HIGH)
        rate = jnp.sum(jnp.where(group4, rate, 0.0), axis=0, keepdims=True)
        turning = dot(turn[layer], spread64, precision=HIGH)
        turning = jnp.sum(jnp.where(group4, turning, 0.0), axis=0, keepdims=True)
        length = size_all[layer : layer + 1]
        real = -rate
        magnitude = jnp.exp(length * real)
        decay_real = magnitude * jnp.cos(length * turning)
        decay_imag = magnitude * jnp.sin(length * turning)
        divisor = real * real + turning * turning
        params[layer, 0:1, :] = decay_real
        params[layer, 1:2, :] = decay_imag
        params[layer, 2:3, :] = ((decay_real - 1.0) * real + decay_imag * turning) / divisor
        params[layer, 3:4, :] = (decay_imag * real - (decay_real - 1.0) * turning) / divisor
        params[layer, 4:5, 0:128] = skip_all[layer : layer + 1]
        for part in range(2):
            lanes = slice(part * 256, part * 256 + 256)
            wide = jnp.where(in_group, dot(s_in[layer, part], spread64, precision=HIGH), 0.0)
            high = wide.astype(BF16)
            low = (wide - high.astype(F32)).astype(BF16)
            for k in range(2):
                inject[layer, k * 64 : k * 64 + 64, lanes] = high
                inject[layer, 128 + k * 64 : 192 + k * 64, lanes] = low
            wide = jnp.where(in_group, dot(s_out[layer, part], spread64, precision=HIGH), 0.0)
            wide = (wide if part == 0 else -wide).astype(BF16)
            readout_w[layer, 0:64, lanes] = wide
            readout_w[layer, 64:128, lanes] = wide
    weights.forward(0)

    lane = iota((PART, 128), 1)
    lane_half = iota((half, 128), 1)
    low256 = iota((256, 128), 1) < 64

    def build_gp():
        zero = jnp.zeros((256, 128), BF16)
        for k in range(8):
            plain = wg[k * 256 : k * 256 + 256, :]
            turned = swap_halves(plain.astype(F32)).astype(BF16)
            for layer in range(2):
                first, second = (plain, turned) if layer == 0 else (turned, plain)
                top = jnp.where(low256, first, zero).reshape(4, 64, 128)
                bottom = jnp.where(low256, zero, second).reshape(4, 64, 128)
                gp[layer, k * 512 : k * 512 + 512, :] = jnp.concatenate([top, bottom], axis=1).reshape(512, 128)

    def build_mp(layer):
        zero = jnp.zeros((4, 64, 128), BF16)
        for k in range(8):
            plain = wm[layer, k * 256 : k * 256 + 256, :].reshape(4, 64, 128)
            mp[layer, k * 512 : k * 512 + 512, 0:128] = jnp.concatenate([plain, zero], axis=1).reshape(512, 128)
            mp[layer, k * 512 : k * 512 + 512, 128:256] = jnp.concatenate([zero, plain], axis=1).reshape(512, 128)

    def project(buf, weight):
        total = None
        for k in range(NZ):
            term = dot(buf[k], weight(k * 512, 512))
            total = term if total is None else total + term
        return total

    gates, branches = {}, {}

    def enter(layer, s, buf):
        squares = None
        for k in range(NZ):
            value = buf[k].astype(F32)
            term = jnp.sum(value * value, axis=1, keepdims=True)
            squares = term if squares is None else squares + term
        inverse = lax.rsqrt(squares / (NZ * 512.0) + EPS)
        both = None
        for k in range(NZ):
            gain = gains[layer : layer + 1, k * 512 : k * 512 + 512]
            normed = (buf[k].astype(F32) * inverse * gain).astype(BF16)
            buf[k] = normed
            term = dot(normed, wdo[k * 512 : k * 512 + 512, 128:256])
            both = term if both is None else both + term
        mine = lane < 64 if layer == 0 else lane >= 64
        drives = jnp.where(mine, both, swap_halves(both))
        high = drives.astype(BF16).astype(F32)
        split = jnp.where(lane < 64, high, drives - high).astype(BF16)
        spread = dot(spread_slot[s], split).astype(BF16)
        moved = dot(jnp.concatenate([spread, spread], axis=1), inject[layer])
        hold_real, hold_imag = params[layer, 2:3, :], params[layer, 3:4, :]
        pushed[:, 0:256] = hold_real * moved[:, 0:256] - hold_imag * moved[:, 256:512]
        pushed[:, 256:512] = hold_real * moved[:, 256:512] + hold_imag * moved[:, 0:256]
        decay_real = jnp.broadcast_to(params[layer, 0:1, :], (32, 256))
        decay_imag = jnp.broadcast_to(params[layer, 1:2, :], (32, 256))
        before = carried if s == 0 else out_state
        state_real, state_imag = before[layer, 0], before[layer, 1]
        for t in range(8):
            now = slice(t * 32, t * 32 + 32)
            alive = live_slot[s, now, :] > 0.5
            next_real = decay_real * state_real - decay_imag * state_imag + pushed[now, 0:256]
            next_imag = decay_real * state_imag + decay_imag * state_real + pushed[now, 256:512]
            state_real = jnp.where(alive, next_real, state_real)
            state_imag = jnp.where(alive, next_imag, state_imag)
            trail[now, 0:256] = state_real.astype(BF16)
            trail[now, 256:512] = state_imag.astype(BF16)
        out_state[layer, 0] = state_real
        out_state[layer, 1] = state_imag
        chosen = dot(pick[s], trail[...]).astype(BF16)
        readout = dot_nt(chosen, readout_w[layer]) + params[layer, 4:5, 0:128] * drives
        inner = math.sqrt(2.0 / math.pi) * (readout + 0.044715 * (readout * readout * readout))
        activated = (readout * (0.5 * (1.0 + jnp.tanh(inner)))).astype(BF16).astype(F32)
        packed = jnp.where(lane_half < 64, activated[0:half], activated[half:PART])
        branches[s] = packed
        return packed.astype(BF16)

    def open_gates(layer):
        weights.finish(7 if layer == 0 else 4)
        for s in range(STREAMS):
            total = project(
                gathers[layer, 0, s].buf, lambda k, n: wdo[k : k + n, layer * 256 : layer * 256 + 128]
            )
            gates[s] = jax.nn.sigmoid(total)

    def switch(layer, s, buf):
        gating = project(buf, lambda k, n: gp[layer, k : k + n, :])
        return (branches[s] * jax.nn.sigmoid(gating)).astype(BF16)

    def join(layer, s, buf):
        merged = project(buf, lambda k, n: mp[layer, k : k + n, :])
        merged = jnp.concatenate([merged[:, 0:128], merged[:, 128:256]], axis=0)
        return (gates[s] * merged).astype(BF16)

    def spread_mixed(layer, s, value):
        lanes = pl.ds(pl.multiple_of(place.z * LANES, LANES), LANES)
        gm[layer, s, :, lanes] = value
        for d in Z_ORDER:
            ref = gm.at[layer, s, :, lanes]
            remote(ref, e_sem.at[layer, s, 0], e_sem.at[layer, s, 1], place.at_z(d)).start()

    def leave(layer, s):
        ref = gm.at[layer, s, :, pl.ds(0, 896)]
        copy = remote(ref, e_sem.at[layer, s, 0], e_sem.at[layer, s, 1], place.partner())
        copy.wait_recv()
        copy.wait_send()
        partial = dot(gm[layer, s], we[layer].reshape(1024, 512)).astype(BF16)
        for k in range(NX):
            tx[layer, s, k] = partial[:, k * 128 : k * 128 + 128]
        for e in X_ORDER:
            pltpu.make_async_remote_copy(
                src_ref=tx.at[layer, s, (place.x + e) % NX],
                dst_ref=rx.at[layer, s, place.x],
                send_sem=e_sem.at[layer, s, 2],
                recv_sem=e_sem.at[layer, s, 3],
                device_id=place.at_x(e),
                device_id_type=MESH,
            ).start()
        rx[layer, s, place.x] = tx[layer, s, place.x]

    def settle(layer, s):
        ref = rx.at[layer, s, pl.ds(0, 3)]
        copy = remote(ref, e_sem.at[layer, s, 2], e_sem.at[layer, s, 3], place.partner())
        copy.wait_recv()
        copy.wait_send()
        branch = rx[layer, s, 0].astype(F32)
        for k in range(1, NX):
            branch = branch + rx[layer, s, k].astype(F32)
        residuals[s] = (residuals[s].astype(F32) + branch).astype(BF16)
        return residuals[s]

    def ready(layer, kind):
        if kind == 0 and layer == 0:
            weights.finish(0)
        elif kind == 1 and layer == 0:
            weights.finish(1)
            build_gp()
        elif kind == 2:
            weights.finish(2 + 3 * layer)
            build_mp(layer)
        elif kind == 3:
            weights.finish(3 + 3 * layer)

    relays = {(0, 0): (1, 7, 2), (0, 1): (3, 4), (0, 2): (5, 6)}
    for layer in range(2):
        for kind, compute in enumerate((enter, switch, join)):
            ready(layer, kind)
            for s in range(STREAMS):
                done = gathers[layer, kind, s]
                done.finish()
                value = compute(layer, s, done.buf)
                if kind < 2:
                    gathers[layer, kind + 1, s].put(value)
                    gathers[layer, kind + 1, s].start()
                else:
                    spread_mixed(layer, s, value)
            if kind < 2:
                forward(layer, kind + 1)
            if kind == 0:
                local[f"out{layer}"].start()
            for piece in relays.get((layer, kind), ()):
                weights.forward(piece)
            if kind == 0:
                open_gates(layer)
        ready(layer, 3)
        for s in range(STREAMS):
            leave(layer, s)
        for s in range(STREAMS):
            value = settle(layer, s)
            if layer == 0:
                gathers[1, 0, s].put(value)
                gathers[1, 0, s].start()
        if layer == 0:
            forward(1, 0)

    spread = None
    for s in range(STREAMS):
        term = dot(spread_seq[s], residuals[s])
        spread = term if spread is None else spread + term
    out_tokens[...] = jnp.where(live_seq[...] > 0.5, spread.astype(BF16), tokens[...])
    local["out_tokens"].start()
    theirs = remote(counts.at[pl.ds(0, NDP - 1)], n_sem.at[0], n_sem.at[1], place.partner())
    theirs.wait_recv()
    theirs.wait_send()
    out_more[0, 0] = (jnp.max(counts[...]) > ROWS).astype(jnp.int32)
    weights.drain()
    for name in ("out0", "out1", "out_tokens"):
        local[name].wait()


def layers(number):
    anywhere = pl.BlockSpec(memory_space=pltpu.HBM)
    half = PART // 2
    gather_count = 2 * STREAMS
    return pl.pallas_call(
        functools.partial(kernel, float(number * ROWS)),
        name=f"layers_{number}",
        out_shape=(
            jax.ShapeDtypeStruct((256, 128), BF16),
            jax.ShapeDtypeStruct((2, 2, 32, 256), F32),
            jax.ShapeDtypeStruct((1, 1), jnp.int32),
        ),
        in_specs=[anywhere] * 15,
        out_specs=(anywhere, anywhere, pl.BlockSpec(memory_space=pltpu.SMEM)),
        scratch_shapes=[
            pltpu.VMEM((256, 128), BF16),
            pltpu.VMEM((1, 32), jnp.int32),
            pltpu.VMEM((2, 4096), F32),
            pltpu.VMEM((2, 64, 512), BF16),
            pltpu.VMEM((2, 64, 256), BF16),
            pltpu.VMEM((2, 4, 64), F32),
            pltpu.VMEM((2, 4, 64), F32),
            pltpu.VMEM((2, 4), F32),
            pltpu.VMEM((2, 2, 64, 64), F32),
            pltpu.VMEM((2, 2, 64, 64), F32),
            pltpu.VMEM((2, 64), F32),
            pltpu.VMEM((2, 2, 32, 256), F32),
            pltpu.VMEM((256, 128), BF16),
            pltpu.VMEM((2, 2, 32, 256), F32),
            pltpu.VMEM((4096, 384), BF16),
            pltpu.VMEM((2048, 128), BF16),
            pltpu.VMEM((2, 2048, 128), BF16),
            pltpu.VMEM((2, NDP, 128, 512), BF16),
            pltpu.VMEM((2, 4096, 128), BF16),
            pltpu.VMEM((2, 4096, 256), BF16),
            pltpu.VMEM((2, STREAMS, NZ, PART, 512), BF16),
            pltpu.VMEM((2, 2, STREAMS, NZ, half, 512), BF16),
            pltpu.VMEM((2, STREAMS, PART, 1024), BF16),
            pltpu.VMEM((2, STREAMS, NX, PART, 128), BF16),
            pltpu.VMEM((2, STREAMS, NX, PART, 128), BF16),
            pltpu.VMEM((STREAMS, PART, 256), BF16),
            pltpu.VMEM((STREAMS, 256, PART), BF16),
            pltpu.VMEM((STREAMS, 256, PART), BF16),
            pltpu.VMEM((256, 128), F32),
            pltpu.VMEM((STREAMS, 256, 256), F32),
            pltpu.VMEM((2, 8, 256), F32),
            pltpu.VMEM((2, 256, 512), BF16),
            pltpu.VMEM((2, 128, 512), BF16),
            pltpu.VMEM((256, 512), F32),
            pltpu.VMEM((256, 512), BF16),
            pltpu.VMEM((NDP, 8, 128), F32),
            pltpu.SemaphoreType.DMA((PIECES,)),
            pltpu.SemaphoreType.DMA((PIECES, 4)),
            pltpu.SemaphoreType.DMA((gather_count, 2)),
            pltpu.SemaphoreType.DMA((gather_count, 8)),
            pltpu.SemaphoreType.DMA((2,)),
            pltpu.SemaphoreType.DMA((21,)),
            pltpu.SemaphoreType.DMA((2, 2)),
            pltpu.SemaphoreType.DMA((2, STREAMS, 4)),
        ],
        compiler_params=pltpu.CompilerParams(
            collective_id=number, has_side_effects=True, vmem_limit_bytes=60 * 1024 * 1024
        ),
    )


def shards(tokens, lengths, norm_gains, drive, opening, glu, merge, leaving, decay, turn, step, s_in, s_out, skip, carried):
    lengths = lengths.reshape(1, 32)
    rest = (
        norm_gains,
        drive.swapaxes(1, 2),
        opening,
        glu.swapaxes(1, 2),
        merge,
        leaving,
        decay,
        turn,
        step,
        s_in.swapaxes(3, 4).reshape(2, 2, 64, 64),
        s_out.reshape(2, 2, 64, 64),
        skip,
    )

    def some(number, tokens, state):
        return layers(number)(tokens, lengths, *rest, state)

    updated, state, more = some(0, tokens.reshape(256, 128), carried)
    updated, state = lax.cond(
        more[0, 0] != 0,
        lambda tokens, state: some(1, tokens, state)[0:2],
        lambda tokens, state: (tokens, state),
        updated,
        state,
    )
    return updated.reshape(32, 8, 128), state


def solution(mesh):
    placed = (
        P("dp", None, "tp"),
        P("dp"),
        P(),
        P(None, "dp", "tp"),
        P(None, "dp", "tp"),
        P(None, "dp", "tp"),
        P(None, "dp", "tp"),
        P(None, "dp", "tp"),
        P(None, "tp", None),
        P(None, "tp", None),
        P(None, "tp"),
        P(None, None, "tp", None, None),
        P(None, None, "tp", None, None),
        P(None, "tp"),
        P(None, None, "dp", "tp"),
    )
    return jax.shard_map(
        shards,
        mesh=mesh,
        in_specs=placed,
        out_specs=(P("dp", None, "tp"), P(None, None, "dp", "tp")),
        check_vma=False,
    )
```

```python
import functools
import math

import jax
import jax.numpy as jnp
from jax import lax
from jax.experimental import pallas as pl
from jax.experimental.pallas import tpu as pltpu
from jax.sharding import PartitionSpec as P

MESH = pl.DeviceIdType.MESH
HIGH = lax.Precision.HIGHEST
EPS = 1e-05
NZ, NX, NY, NDP = 8, 4, 4, 8
Z_ORDER, X_ORDER = (1, 7, 2, 6, 3, 5, 4), (2, 1, 3)
ROWS, STREAMS = 128, 2
PART = ROWS // STREAMS
LANES = 128
F32, BF16 = jnp.float32, jnp.bfloat16
NT = (((1,), (1,)), ((), ()))
PIECES = 8


def dot(a, b, **kw):
    return jnp.dot(a, b, preferred_element_type=F32, **kw)


def dot_nt(a, b):
    return lax.dot_general(a, b, NT, preferred_element_type=F32)


def iota(shape, dim):
    return lax.broadcasted_iota(jnp.int32, shape, dim)


def ones_where(cond, dtype=BF16):
    return jnp.where(cond, 1.0, 0.0).astype(dtype)


def swap_halves(value):
    return pltpu.roll(value, 64, 1)


class Place:
    def __init__(self):
        self.tp = lax.axis_index("tp")
        self.dp = lax.axis_index("dp")
        self.z, self.x = self.tp // NX, self.tp % NX
        self.y, self.core = self.dp // 2, self.dp % 2

    def at_x(self, step):
        return (self.z * NX + (self.x + step) % NX, self.dp)

    def at_z(self, step):
        return ((self.z + step) % NZ * NX + self.x, self.dp)

    def at_y(self, step):
        return (self.tp, (self.y + step) % NY * 2 + self.core)

    def at_dp(self, step):
        return (self.tp, (self.dp + step) % NDP)

    def partner(self):
        return (self.tp, self.y * 2 + 1 - self.core)


def remote(ref, send, recv, device):
    return pltpu.make_async_remote_copy(
        src_ref=ref, dst_ref=ref, send_sem=send, recv_sem=recv, device_id=device, device_id_type=MESH
    )


class Gather:
    def __init__(self, place, buf, send, recv):
        self.p, self.buf, self.send, self.recv = place, buf, send, recv

    def block(self, dz, dx):
        lanes = pl.ds(pl.multiple_of((self.p.x + dx) % NX * LANES, LANES), LANES)
        return self.buf.at[(self.p.z + dz) % NZ, :, lanes]

    def put(self, value):
        lanes = pl.ds(pl.multiple_of(self.p.x * LANES, LANES), LANES)
        self.buf[self.p.z, :, lanes] = value

    def along_x(self, ref):
        for e in X_ORDER:
            remote(ref, self.send.at[1], self.recv.at[7], self.p.at_x(e)).start()

    def start(self):
        for d in Z_ORDER:
            remote(self.block(0, 0), self.send.at[0], self.recv.at[d - 1], self.p.at_z(d)).start()
        self.along_x(self.block(0, 0))

    def forward(self, d):
        ref = self.block(NZ - d, 0)
        remote(ref, self.send.at[0], self.recv.at[d - 1], self.p.partner()).wait_recv()
        self.along_x(ref)

    def finish(self):
        most = self.buf.at[:, :, pl.ds(0, 384)]
        remote(most, self.send.at[1], self.recv.at[7], self.p.partner()).wait_recv()

    def drain(self):
        seven, most = self.buf.at[pl.ds(0, 7), :, pl.ds(0, 128)], self.buf.at[:, :, pl.ds(0, 384)]
        remote(seven, self.send.at[0], self.recv.at[0], self.p.partner()).wait_send()
        remote(most, self.send.at[1], self.recv.at[7], self.p.partner()).wait_send()


class Weights:
    def __init__(self, place, wdo, wg, wm, we, send, recv):
        self.p = place
        self.refs = (wdo, wg, wm, we)
        self.send, self.recv = send, recv

    def region(self, piece, shard, count=1):
        wdo, wg, wm, we = self.refs
        if piece in (0, 4, 7):
            rows = pl.ds(pl.multiple_of(shard * 512, 512), 512 * count)
        else:
            rows = pl.ds(pl.multiple_of(shard * 256, 256), 256 * count)
        if piece == 0:
            return wdo.at[rows, pl.ds(128, 128)]
        if piece == 7:
            return wdo.at[rows, pl.ds(0, 128)]
        if piece == 4:
            return wdo.at[rows, pl.ds(256, 128)]
        if piece == 1:
            return wg.at[rows, :]
        if piece in (2, 5):
            return wm.at[(piece - 2) // 3, rows, :]
        return we.at[(piece - 3) // 3, pl.ds(shard, count)]

    def like(self, step):
        return (self.p.y + step) % NY * 2 + self.p.core

    def unlike(self, step):
        return (self.p.y + step) % NY * 2 + 1 - self.p.core

    def y_copy(self, piece, d, shard):
        ref = self.region(piece, shard)
        return remote(ref, self.send.at[piece], self.recv.at[piece, d - 1], self.p.at_y(d))

    def c_copy(self, piece, shard, count=1):
        ref = self.region(piece, shard, count)
        return remote(ref, self.send.at[piece], self.recv.at[piece, 3], self.p.partner())

    def start(self, piece):
        for d in (1, 3, 2):
            self.y_copy(piece, d, self.p.dp).start()
        self.c_copy(piece, self.p.dp).start()

    def forward(self, piece):
        for d in (1, 3, 2):
            shard = (self.p.y + NY - d) % NY * 2 + self.p.core
            self.y_copy(piece, d, shard).wait_recv()
            self.c_copy(piece, shard).start()

    def finish(self, piece):
        self.c_copy(piece, 0, 4).wait_recv()

    def drain(self):
        for piece in range(PIECES):
            self.c_copy(piece, 0, 7).wait_send()


def kernel(
    origin,
    tokens_h,
    lengths_h,
    gains_h,
    drive_h,
    opening_h,
    glu_h,
    merge_h,
    leaving_h,
    decay_h,
    turn_h,
    step_h,
    s_in_h,
    s_out_h,
    skip_h,
    carried_h,
    out_tokens_h,
    out_state_h,
    out_more,
    tokens,
    lengths,
    gains,
    drive,
    glu,
    decay,
    turn,
    step,
    s_in,
    s_out,
    skip,
    carried,
    out_tokens,
    out_state,
    wdo,
    wg,
    wm,
    we,
    gp,
    mp,
    gx,
    ga,
    gm,
    nx,
    tx,
    rx,
    pick,
    spread_seq,
    spread_slot,
    live_seq,
    live_slot,
    params,
    inject,
    readout_w,
    pushed,
    trail,
    counts,
    w_send,
    w_recv,
    g_send,
    g_recv,
    n_sem,
    l_sem,
    q_sem,
    e_sem,
):
    place = Place()
    own512 = pl.ds(pl.multiple_of(place.dp * 512, 512), 512)
    own256 = pl.ds(pl.multiple_of(place.dp * 256, 256), 256)
    own_lanes = pl.ds(pl.multiple_of(place.x * LANES, LANES), LANES)
    own_rows = pl.ds(pl.multiple_of(place.x * 128, 128), 128)
    local = {}
    for name, source, target in (
        ("tokens", tokens_h, tokens),
        ("lengths", lengths_h, lengths),
        ("open0", opening_h.at[0], wdo.at[own512, pl.ds(0, 128)]),
        ("drive", drive_h, drive),
        ("glu", glu_h, glu),
        ("merge0", merge_h.at[0], wm.at[0, own256, :]),
        ("exit0", leaving_h.at[0, own_rows, :], we.at[0, place.dp, :, own_lanes]),
        ("open1", opening_h.at[1], wdo.at[own512, pl.ds(256, 128)]),
        ("merge1", merge_h.at[1], wm.at[1, own256, :]),
        ("exit1", leaving_h.at[1, own_rows, :], we.at[1, place.dp, :, own_lanes]),
        ("decay", decay_h, decay),
        ("turn", turn_h, turn),
        ("step", step_h, step),
        ("s_in", s_in_h, s_in),
        ("s_out", s_out_h, s_out),
        ("skip", skip_h, skip),
        ("gains", gains_h, gains),
        ("carried", carried_h, carried),
        ("out0", out_state.at[0], out_state_h.at[0]),
        ("out1", out_state.at[1], out_state_h.at[1]),
        ("out_tokens", out_tokens, out_tokens_h),
    ):
        local[name] = pltpu.make_async_copy(source, target, l_sem.at[len(local)])
        if not name.startswith("out"):
            local[name].start()
    half = PART // 2
    barrier = pltpu.get_barrier_semaphore()
    peers = [place.at_x(d) for d in range(1, NX)] + [place.at_z(d) for d in range(1, NZ)]
    peers += [place.at_dp(d) for d in range(1, NDP)]
    for peer in peers:
        pl.semaphore_signal(barrier, inc=1, device_id=peer, device_id_type=MESH)

    gathers = {}
    for layer in range(2):
        for kind in range(3):
            for s in range(STREAMS):
                ref = gx.at[layer, s] if kind == 0 else ga.at[layer, kind - 1, s]
                index = (layer * 3 + kind) % 2 * STREAMS + s
                gathers[layer, kind, s] = Gather(place, ref, g_send.at[index], g_recv.at[index])
    weights = Weights(place, wdo, wg, wm, we, w_send, w_recv)

    local["lengths"].wait()
    lens = lengths[...].astype(F32)
    lens_rows = jnp.broadcast_to(lens, (256, 32)).astype(BF16)
    seq, col = iota((32, 256), 0), iota((32, 256), 1)
    row, other = iota((256, 256), 0), iota((256, 256), 1)
    size_slot = dot(lens_rows, ones_where(seq == jnp.bitwise_and(col, 31)))
    is_live_slot = lax.shift_right_logical(other, 5).astype(F32) < size_slot
    counted = ones_where(is_live_slot)
    size_seq = dot(lens_rows[0:8], ones_where(seq == lax.shift_right_logical(col, 3)))[0:1]
    is_live_seq = jnp.bitwise_and(iota((1, 256), 1), 7).astype(F32) < size_seq
    rank_seq = jnp.bitwise_and(other, 7) * 32 + lax.shift_right_logical(other, 3)
    number_seq = dot(counted[0:8], ones_where(row < rank_seq))[0:1]
    target = jnp.where(is_live_seq, number_seq - origin, -1.0)
    residuals = []
    local["tokens"].wait()
    for s in range(STREAMS):
        compact = ones_where((iota((PART, 256), 0) + s * PART).astype(F32) == target)
        residual = dot(compact, tokens[...]).astype(BF16)
        gathers[0, 0, s].put(residual)
        residuals.append(residual)

    counts[place.dp] = jnp.broadcast_to(jnp.sum(lens, axis=1, keepdims=True), (8, 128))

    pl.semaphore_wait(barrier, len(peers))
    for s in range(STREAMS):
        gathers[0, 0, s].start()
    local["drive"].wait()
    wdo[own512, 128:256] = drive[...].astype(F32).reshape(128, 512).T.astype(BF16)
    weights.start(0)
    local["glu"].wait()
    wg[own256, :] = glu[...].astype(F32).reshape(128, 256).T.astype(BF16)
    weights.start(1)
    local["open0"].wait()
    weights.start(7)
    local["merge0"].wait()
    weights.start(2)
    for layer in range(2):
        for e in X_ORDER:
            rows = pl.ds(pl.multiple_of((place.x + e) % NX * 128, 128), 128)
            pltpu.make_async_remote_copy(
                src_ref=leaving_h.at[layer, rows, :],
                dst_ref=we.at[layer, place.dp, :, own_lanes],
                send_sem=q_sem.at[layer, 0],
                recv_sem=q_sem.at[layer, 1],
                device_id=place.at_x(e),
                device_id_type=MESH,
            ).start()

    def quarters(layer):
        ref = we.at[layer, place.dp, :, pl.ds(0, 384)]
        copy = remote(ref, q_sem.at[layer, 0], q_sem.at[layer, 1], place.partner())
        copy.wait_recv()
        copy.wait_send()
    for d in range(1, NDP):
        remote(counts.at[place.dp], n_sem.at[0], n_sem.at[1], place.at_dp(d)).start()

    def forward(layer, kind):
        for s in range(STREAMS):
            for d in Z_ORDER:
                gathers[layer, kind, s].forward(d)

    target = jnp.where(is_live_slot[0:1], dot(counted[0:8], ones_where(row < other))[0:1] - origin, -1.0)
    for s in range(STREAMS):
        pick[s] = ones_where((iota((PART, 256), 0) + s * PART).astype(F32) == target)
    size = dot_nt(ones_where(iota((256, 32), 1) == jnp.bitwise_and(iota((256, 32), 0), 31)), lens_rows)
    number = dot_nt(ones_where(other < row), counted) - origin
    target = jnp.where(lax.shift_right_logical(row, 5).astype(F32) < size, number, -1.0)
    for s in range(STREAMS):
        spread_slot[s] = ones_where((iota((256, PART), 1) + s * PART).astype(F32) == target[:, 0:PART])
        live_slot[s] = ones_where((target >= s * PART) & (target < (s + 1) * PART), F32)
    forward(0, 0)
    quarters(0)
    quarters(1)
    for piece, name in enumerate(("exit0", "open1", "merge1", "exit1")):
        local[name].wait()
        weights.start(piece + 3)
    size = dot_nt(ones_where(iota((256, 32), 1) == lax.shift_right_logical(iota((256, 32), 0), 3)), lens_rows)
    rank = jnp.bitwise_and(row, 7) * 32 + lax.shift_right_logical(row, 3)
    number = dot_nt(ones_where(other < rank), counted) - origin
    target = jnp.where(jnp.bitwise_and(row, 7).astype(F32) < size, number, -1.0)[:, 0:128]
    for s in range(STREAMS):
        spread_seq[s] = ones_where((iota((256, PART), 1) + s * PART).astype(F32) == target[:, 0:PART])
    live_seq[...] = ones_where((target >= 0.0) & (target < ROWS), F32)

    for name in ("decay", "turn", "step", "s_in", "s_out", "skip", "gains", "carried"):
        local[name].wait()
    spread64 = ones_where(iota((64, 256), 0) == jnp.bitwise_and(iota((64, 256), 1), 63), F32)
    spread2 = ones_where(iota((64, 128), 0) == jnp.bitwise_and(iota((64, 128), 1), 63), F32)
    group4 = iota((4, 256), 0) == lax.shift_right_logical(iota((4, 256), 1), 6)
    in_group = lax.shift_right_logical(iota((64, 256), 0), 4) == lax.shift_right_logical(iota((64, 256), 1), 6)
    size_all = dot(step[...], ones_where(group4, F32), precision=HIGH)
    skip_all = dot(skip[...], spread2, precision=HIGH)
    for layer in range(2):
        rate = dot(decay[layer], spread64, precision=HIGH)
        rate = jnp.sum(jnp.where(group4, rate, 0.0), axis=0, keepdims=True)
        turning = dot(turn[layer], spread64, precision=HIGH)
        turning = jnp.sum(jnp.where(group4, turning, 0.0), axis=0, keepdims=True)
        length = size_all[layer : layer + 1]
        real = -rate
        magnitude = jnp.exp(length * real)
        decay_real = magnitude * jnp.cos(length * turning)
        decay_imag = magnitude * jnp.sin(length * turning)
        divisor = real * real + turning * turning
        params[layer, 0:1, :] = decay_real
        params[layer, 1:2, :] = decay_imag
        params[layer, 2:3, :] = ((decay_real - 1.0) * real + decay_imag * turning) / divisor
        params[layer, 3:4, :] = (decay_imag * real - (decay_real - 1.0) * turning) / divisor
        params[layer, 4:5, 0:128] = skip_all[layer : layer + 1]
        for part in range(2):
            lanes = slice(part * 256, part * 256 + 256)
            wide = jnp.where(in_group, dot(s_in[layer, part], spread64, precision=HIGH), 0.0)
            high = wide.astype(BF16)
            low = (wide - high.astype(F32)).astype(BF16)
            for k in range(2):
                inject[layer, k * 64 : k * 64 + 64, lanes] = high
                inject[layer, 128 + k * 64 : 192 + k * 64, lanes] = low
            wide = jnp.where(in_group, dot(s_out[layer, part], spread64, precision=HIGH), 0.0)
            wide = (wide if part == 0 else -wide).astype(BF16)
            readout_w[layer, 0:64, lanes] = wide
            readout_w[layer, 64:128, lanes] = wide
    weights.forward(0)

    lane = iota((PART, 128), 1)
    lane_half = iota((half, 128), 1)
    low256 = iota((256, 128), 1) < 64

    def build_gp():
        zero = jnp.zeros((256, 128), BF16)
        for k in range(8):
            plain = wg[k * 256 : k * 256 + 256, :]
            turned = swap_halves(plain.astype(F32)).astype(BF16)
            for layer in range(2):
                first, second = (plain, turned) if layer == 0 else (turned, plain)
                top = jnp.where(low256, first, zero).reshape(4, 64, 128)
                bottom = jnp.where(low256, zero, second).reshape(4, 64, 128)
                gp[layer, k * 512 : k * 512 + 512, :] = jnp.concatenate([top, bottom], axis=1).reshape(512, 128)

    def build_mp(layer):
        zero = jnp.zeros((4, 64, 128), BF16)
        for k in range(8):
            plain = wm[layer, k * 256 : k * 256 + 256, :].reshape(4, 64, 128)
            mp[layer, k * 512 : k * 512 + 512, 0:128] = jnp.concatenate([plain, zero], axis=1).reshape(512, 128)
            mp[layer, k * 512 : k * 512 + 512, 128:256] = jnp.concatenate([zero, plain], axis=1).reshape(512, 128)

    def project(buf, weight):
        total = None
        for k in range(NZ):
            term = dot(buf[k], weight(k * 512, 512))
            total = term if total is None else total + term
        return total

    gates, branches, waiting = {}, {}, []

    def enter(layer, s, buf):
        squares = None
        for k in range(NZ):
            value = buf[k].astype(F32)
            term = jnp.sum(value * value, axis=1, keepdims=True)
            squares = term if squares is None else squares + term
        inverse = lax.rsqrt(squares / (NZ * 512.0) + EPS)
        both = None
        for k in range(NZ):
            gain = gains[layer : layer + 1, k * 512 : k * 512 + 512]
            normed = (buf[k].astype(F32) * inverse * gain).astype(BF16)
            nx[s, k] = normed
            term = dot(normed, wdo[k * 512 : k * 512 + 512, 128:256])
            both = term if both is None else both + term
        mine = lane < 64 if layer == 0 else lane >= 64
        drives = jnp.where(mine, both, swap_halves(both))
        high = drives.astype(BF16).astype(F32)
        split = jnp.where(lane < 64, high, drives - high).astype(BF16)
        spread = dot(spread_slot[s], split).astype(BF16)
        moved = dot(jnp.concatenate([spread, spread], axis=1), inject[layer])
        hold_real, hold_imag = params[layer, 2:3, :], params[layer, 3:4, :]
        pushed[:, 0:256] = hold_real * moved[:, 0:256] - hold_imag * moved[:, 256:512]
        pushed[:, 256:512] = hold_real * moved[:, 256:512] + hold_imag * moved[:, 0:256]
        decay_real = jnp.broadcast_to(params[layer, 0:1, :], (32, 256))
        decay_imag = jnp.broadcast_to(params[layer, 1:2, :], (32, 256))
        before = carried if s == 0 else out_state
        state_real, state_imag = before[layer, 0], before[layer, 1]
        for t in range(8):
            now = slice(t * 32, t * 32 + 32)
            alive = live_slot[s, now, :] > 0.5
            next_real = decay_real * state_real - decay_imag * state_imag + pushed[now, 0:256]
            next_imag = decay_real * state_imag + decay_imag * state_real + pushed[now, 256:512]
            state_real = jnp.where(alive, next_real, state_real)
            state_imag = jnp.where(alive, next_imag, state_imag)
            trail[now, 0:256] = state_real.astype(BF16)
            trail[now, 256:512] = state_imag.astype(BF16)
        out_state[layer, 0] = state_real
        out_state[layer, 1] = state_imag
        chosen = dot(pick[s], trail[...]).astype(BF16)
        readout = dot_nt(chosen, readout_w[layer]) + params[layer, 4:5, 0:128] * drives
        inner = math.sqrt(2.0 / math.pi) * (readout + 0.044715 * (readout * readout * readout))
        activated = (readout * (0.5 * (1.0 + jnp.tanh(inner)))).astype(BF16).astype(F32)
        packed = jnp.where(lane_half < 64, activated[0:half], activated[half:PART])
        branches[s] = packed
        return packed.astype(BF16)

    def open_gates(layer):
        weights.finish(7 if layer == 0 else 4)
        for s in range(STREAMS):
            total = project(
                nx.at[s], lambda k, n: wdo[k : k + n, layer * 256 : layer * 256 + 128]
            )
            gates[s] = jax.nn.sigmoid(total)

    def switch(layer, s, buf):
        gating = project(buf, lambda k, n: gp[layer, k : k + n, :])
        return (branches[s] * jax.nn.sigmoid(gating)).astype(BF16)

    def join(layer, s, buf):
        merged = project(buf, lambda k, n: mp[layer, k : k + n, :])
        merged = jnp.concatenate([merged[:, 0:128], merged[:, 128:256]], axis=0)
        return (gates[s] * merged).astype(BF16)

    def spread_mixed(layer, s, value):
        lanes = pl.ds(pl.multiple_of(place.z * LANES, LANES), LANES)
        gm[layer, s, :, lanes] = value
        for d in Z_ORDER:
            ref = gm.at[layer, s, :, lanes]
            remote(ref, e_sem.at[layer, s, 0], e_sem.at[layer, s, 1], place.at_z(d)).start()

    def leave(layer, s):
        ref = gm.at[layer, s, :, pl.ds(0, 896)]
        copy = remote(ref, e_sem.at[layer, s, 0], e_sem.at[layer, s, 1], place.partner())
        copy.wait_recv()
        waiting.append(copy)
        partial = dot(gm[layer, s], we[layer].reshape(1024, 512)).astype(BF16)
        for k in range(NX):
            tx[layer, s, k] = partial[:, k * 128 : k * 128 + 128]
        for e in X_ORDER:
            pltpu.make_async_remote_copy(
                src_ref=tx.at[layer, s, (place.x + e) % NX],
                dst_ref=rx.at[layer, s, place.x],
                send_sem=e_sem.at[layer, s, 2],
                recv_sem=e_sem.at[layer, s, 3],
                device_id=place.at_x(e),
                device_id_type=MESH,
            ).start()
        rx[layer, s, place.x] = tx[layer, s, place.x]

    def settle(layer, s):
        ref = rx.at[layer, s, pl.ds(0, 3)]
        copy = remote(ref, e_sem.at[layer, s, 2], e_sem.at[layer, s, 3], place.partner())
        copy.wait_recv()
        waiting.append(copy)
        branch = rx[layer, s, 0].astype(F32)
        for k in range(1, NX):
            branch = branch + rx[layer, s, k].astype(F32)
        residuals[s] = (residuals[s].astype(F32) + branch).astype(BF16)
        return residuals[s]

    def ready(layer, kind):
        if kind == 0 and layer == 0:
            weights.finish(0)
        elif kind == 1 and layer == 0:
            weights.finish(1)
            build_gp()
        elif kind == 2:
            weights.finish(2 + 3 * layer)
            build_mp(layer)
        elif kind == 3:
            weights.finish(3 + 3 * layer)

    relays = {(0, 0): (1, 7, 2), (0, 1): (3, 4), (0, 2): (5, 6)}
    for layer in range(2):
        for kind, compute in enumerate((enter, switch, join)):
            ready(layer, kind)
            for s in range(STREAMS):
                done = gathers[layer, kind, s]
                done.finish()
                value = compute(layer, s, done.buf)
                if kind < 2:
                    gathers[layer, kind + 1, s].put(value)
                    gathers[layer, kind + 1, s].start()
                else:
                    spread_mixed(layer, s, value)
            if kind < 2:
                forward(layer, kind + 1)
            for s in range(STREAMS):
                gathers[layer, kind, s].drain()
            if kind == 0:
                local[f"out{layer}"].start()
            for piece in relays.get((layer, kind), ()):
                weights.forward(piece)
            if kind == 0:
                open_gates(layer)
        ready(layer, 3)
        for s in range(STREAMS):
            leave(layer, s)
        for s in range(STREAMS):
            value = settle(layer, s)
            if layer == 0:
                gathers[1, 0, s].put(value)
                gathers[1, 0, s].start()
        if layer == 0:
            forward(1, 0)

    spread = None
    for s in range(STREAMS):
        term = dot(spread_seq[s], residuals[s])
        spread = term if spread is None else spread + term
    out_tokens[...] = jnp.where(live_seq[...] > 0.5, spread.astype(BF16), tokens[...])
    local["out_tokens"].start()
    theirs = remote(counts.at[pl.ds(0, NDP - 1)], n_sem.at[0], n_sem.at[1], place.partner())
    theirs.wait_recv()
    theirs.wait_send()
    out_more[0, 0] = (jnp.max(counts[...]) > ROWS).astype(jnp.int32)
    weights.drain()
    for copy in waiting:
        copy.wait_send()
    for name in ("out0", "out1", "out_tokens"):
        local[name].wait()


def layers(number):
    anywhere = pl.BlockSpec(memory_space=pltpu.HBM)
    half = PART // 2
    gather_count = 2 * STREAMS
    return pl.pallas_call(
        functools.partial(kernel, float(number * ROWS)),
        name=f"layers_{number}",
        out_shape=(
            jax.ShapeDtypeStruct((256, 128), BF16),
            jax.ShapeDtypeStruct((2, 2, 32, 256), F32),
            jax.ShapeDtypeStruct((1, 1), jnp.int32),
        ),
        in_specs=[anywhere] * 15,
        out_specs=(anywhere, anywhere, pl.BlockSpec(memory_space=pltpu.SMEM)),
        scratch_shapes=[
            pltpu.VMEM((256, 128), BF16),
            pltpu.VMEM((1, 32), jnp.int32),
            pltpu.VMEM((2, 4096), F32),
            pltpu.VMEM((2, 64, 512), BF16),
            pltpu.VMEM((2, 64, 256), BF16),
            pltpu.VMEM((2, 4, 64), F32),
            pltpu.VMEM((2, 4, 64), F32),
            pltpu.VMEM((2, 4), F32),
            pltpu.VMEM((2, 2, 64, 64), F32),
            pltpu.VMEM((2, 2, 64, 64), F32),
            pltpu.VMEM((2, 64), F32),
            pltpu.VMEM((2, 2, 32, 256), F32),
            pltpu.VMEM((256, 128), BF16),
            pltpu.VMEM((2, 2, 32, 256), F32),
            pltpu.VMEM((4096, 384), BF16),
            pltpu.VMEM((2048, 128), BF16),
            pltpu.VMEM((2, 2048, 128), BF16),
            pltpu.VMEM((2, NDP, 128, 512), BF16),
            pltpu.VMEM((2, 4096, 128), BF16),
            pltpu.VMEM((2, 4096, 256), BF16),
            pltpu.VMEM((2, STREAMS, NZ, PART, 512), BF16),
            pltpu.VMEM((2, 2, STREAMS, NZ, half, 512), BF16),
            pltpu.VMEM((2, STREAMS, PART, 1024), BF16),
            pltpu.VMEM((STREAMS, NZ, PART, 512), BF16),
            pltpu.VMEM((2, STREAMS, NX, PART, 128), BF16),
            pltpu.VMEM((2, STREAMS, NX, PART, 128), BF16),
            pltpu.VMEM((STREAMS, PART, 256), BF16),
            pltpu.VMEM((STREAMS, 256, PART), BF16),
            pltpu.VMEM((STREAMS, 256, PART), BF16),
            pltpu.VMEM((256, 128), F32),
            pltpu.VMEM((STREAMS, 256, 256), F32),
            pltpu.VMEM((2, 8, 256), F32),
            pltpu.VMEM((2, 256, 512), BF16),
            pltpu.VMEM((2, 128, 512), BF16),
            pltpu.VMEM((256, 512), F32),
            pltpu.VMEM((256, 512), BF16),
            pltpu.VMEM((NDP, 8, 128), F32),
            pltpu.SemaphoreType.DMA((PIECES,)),
            pltpu.SemaphoreType.DMA((PIECES, 4)),
            pltpu.SemaphoreType.DMA((gather_count, 2)),
            pltpu.SemaphoreType.DMA((gather_count, 8)),
            pltpu.SemaphoreType.DMA((2,)),
            pltpu.SemaphoreType.DMA((21,)),
            pltpu.SemaphoreType.DMA((2, 2)),
            pltpu.SemaphoreType.DMA((2, STREAMS, 4)),
        ],
        compiler_params=pltpu.CompilerParams(
            collective_id=number, has_side_effects=True, vmem_limit_bytes=60 * 1024 * 1024
        ),
    )


def shards(tokens, lengths, norm_gains, drive, opening, glu, merge, leaving, decay, turn, step, s_in, s_out, skip, carried):
    lengths = lengths.reshape(1, 32)
    rest = (
        norm_gains,
        drive.swapaxes(1, 2),
        opening,
        glu.swapaxes(1, 2),
        merge,
        leaving,
        decay,
        turn,
        step,
        s_in.swapaxes(3, 4).reshape(2, 2, 64, 64),
        s_out.reshape(2, 2, 64, 64),
        skip,
    )

    def some(number, tokens, state):
        return layers(number)(tokens, lengths, *rest, state)

    updated, state, more = some(0, tokens.reshape(256, 128), carried)
    updated, state = lax.cond(
        more[0, 0] != 0,
        lambda tokens, state: some(1, tokens, state)[0:2],
        lambda tokens, state: (tokens, state),
        updated,
        state,
    )
    return updated.reshape(32, 8, 128), state


def solution(mesh):
    placed = (
        P("dp", None, "tp"),
        P("dp"),
        P(),
        P(None, "dp", "tp"),
        P(None, "dp", "tp"),
        P(None, "dp", "tp"),
        P(None, "dp", "tp"),
        P(None, "dp", "tp"),
        P(None, "tp", None),
        P(None, "tp", None),
        P(None, "tp"),
        P(None, None, "tp", None, None),
        P(None, None, "tp", None, None),
        P(None, "tp"),
        P(None, None, "dp", "tp"),
    )
    return jax.shard_map(
        shards,
        mesh=mesh,
        in_specs=placed,
        out_specs=(P("dp", None, "tp"), P(None, None, "dp", "tp")),
        check_vma=False,
    )
```

```python
import functools
import math

import jax
import jax.numpy as jnp
from jax import lax
from jax.experimental import pallas as pl
from jax.experimental.pallas import tpu as pltpu
from jax.sharding import PartitionSpec as P

MESH = pl.DeviceIdType.MESH
HIGH = lax.Precision.HIGHEST
EPS = 1e-05
NZ, NX, NY, NDP = 8, 4, 4, 8
Z_ORDER, X_ORDER = (1, 7, 2, 6, 3, 5, 4), (2, 1, 3)
Z_FAR, Z_MIXED = (4, 3, 5, 2, 6, 1, 7), (1, 7, 4, 3, 5, 2, 6)
ROWS, STREAMS = 128, 2
PART = ROWS // STREAMS
LANES = 128
F32, BF16 = jnp.float32, jnp.bfloat16
NT = (((1,), (1,)), ((), ()))
PIECES = 8


def dot(a, b, **kw):
    return jnp.dot(a, b, preferred_element_type=F32, **kw)


def dot_nt(a, b):
    return lax.dot_general(a, b, NT, preferred_element_type=F32)


def iota(shape, dim):
    return lax.broadcasted_iota(jnp.int32, shape, dim)


def ones_where(cond, dtype=BF16):
    return jnp.where(cond, 1.0, 0.0).astype(dtype)


def swap_halves(value):
    return pltpu.roll(value, 64, 1)


class Place:
    def __init__(self):
        self.tp = lax.axis_index("tp")
        self.dp = lax.axis_index("dp")
        self.z, self.x = self.tp // NX, self.tp % NX
        self.y, self.core = self.dp // 2, self.dp % 2

    def at_x(self, step):
        return (self.z * NX + (self.x + step) % NX, self.dp)

    def at_z(self, step):
        return ((self.z + step) % NZ * NX + self.x, self.dp)

    def at_y(self, step):
        return (self.tp, (self.y + step) % NY * 2 + self.core)

    def at_dp(self, step):
        return (self.tp, (self.dp + step) % NDP)

    def partner(self):
        return (self.tp, self.y * 2 + 1 - self.core)


def remote(ref, send, recv, device):
    return pltpu.make_async_remote_copy(
        src_ref=ref, dst_ref=ref, send_sem=send, recv_sem=recv, device_id=device, device_id_type=MESH
    )


class Gather:
    def __init__(self, place, buf, send, recv):
        self.p, self.buf, self.send, self.recv = place, buf, send, recv

    def block(self, dz, dx):
        lanes = pl.ds(pl.multiple_of((self.p.x + dx) % NX * LANES, LANES), LANES)
        return self.buf.at[(self.p.z + dz) % NZ, :, lanes]

    def put(self, value):
        lanes = pl.ds(pl.multiple_of(self.p.x * LANES, LANES), LANES)
        self.buf[self.p.z, :, lanes] = value

    def along_x(self, ref):
        for e in X_ORDER:
            remote(ref, self.send.at[1], self.recv.at[7], self.p.at_x(e)).start()

    def start(self):
        for d in Z_MIXED:
            remote(self.block(0, 0), self.send.at[0], self.recv.at[d - 1], self.p.at_z(d)).start()
        self.along_x(self.block(0, 0))

    def forward(self, d):
        ref = self.block(NZ - d, 0)
        remote(ref, self.send.at[0], self.recv.at[d - 1], self.p.partner()).wait_recv()
        self.along_x(ref)

    def finish(self):
        most = self.buf.at[:, :, pl.ds(0, 384)]
        remote(most, self.send.at[1], self.recv.at[7], self.p.partner()).wait_recv()

    def drain(self):
        seven, most = self.buf.at[pl.ds(0, 7), :, pl.ds(0, 128)], self.buf.at[:, :, pl.ds(0, 384)]
        remote(seven, self.send.at[0], self.recv.at[0], self.p.partner()).wait_send()
        remote(most, self.send.at[1], self.recv.at[7], self.p.partner()).wait_send()


class Weights:
    def __init__(self, place, wdo, wg, wm, we, send, recv):
        self.p = place
        self.refs = (wdo, wg, wm, we)
        self.send, self.recv = send, recv

    def region(self, piece, shard, count=1):
        wdo, wg, wm, we = self.refs
        if piece in (0, 4, 7):
            rows = pl.ds(pl.multiple_of(shard * 512, 512), 512 * count)
        else:
            rows = pl.ds(pl.multiple_of(shard * 256, 256), 256 * count)
        if piece == 0:
            return wdo.at[rows, pl.ds(128, 128)]
        if piece == 7:
            return wdo.at[rows, pl.ds(0, 128)]
        if piece == 4:
            return wdo.at[rows, pl.ds(256, 128)]
        if piece == 1:
            return wg.at[rows, :]
        if piece in (2, 5):
            return wm.at[(piece - 2) // 3, rows, :]
        return we.at[(piece - 3) // 3, pl.ds(shard, count)]

    def like(self, step):
        return (self.p.y + step) % NY * 2 + self.p.core

    def unlike(self, step):
        return (self.p.y + step) % NY * 2 + 1 - self.p.core

    def y_copy(self, piece, d, shard):
        ref = self.region(piece, shard)
        return remote(ref, self.send.at[piece], self.recv.at[piece, d - 1], self.p.at_y(d))

    def c_copy(self, piece, shard, count=1):
        ref = self.region(piece, shard, count)
        return remote(ref, self.send.at[piece], self.recv.at[piece, 3], self.p.partner())

    def start(self, piece):
        for d in (1, 3, 2):
            self.y_copy(piece, d, self.p.dp).start()
        self.c_copy(piece, self.p.dp).start()

    def forward(self, piece):
        for d in (1, 3, 2):
            shard = (self.p.y + NY - d) % NY * 2 + self.p.core
            self.y_copy(piece, d, shard).wait_recv()
            self.c_copy(piece, shard).start()

    def finish(self, piece):
        self.c_copy(piece, 0, 4).wait_recv()

    def drain(self):
        for piece in range(PIECES):
            self.c_copy(piece, 0, 7).wait_send()


def kernel(
    origin,
    tokens_h,
    lengths_h,
    gains_h,
    drive_h,
    opening_h,
    glu_h,
    merge_h,
    leaving_h,
    decay_h,
    turn_h,
    step_h,
    s_in_h,
    s_out_h,
    skip_h,
    carried_h,
    out_tokens_h,
    out_state_h,
    out_more,
    tokens,
    lengths,
    gains,
    drive,
    glu,
    decay,
    turn,
    step,
    s_in,
    s_out,
    skip,
    carried,
    out_tokens,
    out_state,
    wdo,
    wg,
    wm,
    we,
    gp,
    mp,
    gx,
    ga,
    gm,
    nx,
    tx,
    rx,
    pick,
    spread_seq,
    spread_slot,
    live_seq,
    live_slot,
    params,
    inject,
    readout_w,
    pushed,
    trail,
    counts,
    w_send,
    w_recv,
    g_send,
    g_recv,
    n_sem,
    l_sem,
    q_sem,
    e_sem,
):
    place = Place()
    own512 = pl.ds(pl.multiple_of(place.dp * 512, 512), 512)
    own256 = pl.ds(pl.multiple_of(place.dp * 256, 256), 256)
    own_lanes = pl.ds(pl.multiple_of(place.x * LANES, LANES), LANES)
    own_rows = pl.ds(pl.multiple_of(place.x * 128, 128), 128)
    local = {}
    for name, source, target in (
        ("tokens", tokens_h, tokens),
        ("lengths", lengths_h, lengths),
        ("open0", opening_h.at[0], wdo.at[own512, pl.ds(0, 128)]),
        ("drive", drive_h, drive),
        ("glu", glu_h, glu),
        ("merge0", merge_h.at[0], wm.at[0, own256, :]),
        ("exit0", leaving_h.at[0, own_rows, :], we.at[0, place.dp, :, own_lanes]),
        ("open1", opening_h.at[1], wdo.at[own512, pl.ds(256, 128)]),
        ("merge1", merge_h.at[1], wm.at[1, own256, :]),
        ("exit1", leaving_h.at[1, own_rows, :], we.at[1, place.dp, :, own_lanes]),
        ("decay", decay_h, decay),
        ("turn", turn_h, turn),
        ("step", step_h, step),
        ("s_in", s_in_h, s_in),
        ("s_out", s_out_h, s_out),
        ("skip", skip_h, skip),
        ("gains", gains_h, gains),
        ("carried", carried_h, carried),
        ("out0", out_state.at[0], out_state_h.at[0]),
        ("out1", out_state.at[1], out_state_h.at[1]),
        ("out_tokens", out_tokens, out_tokens_h),
    ):
        local[name] = pltpu.make_async_copy(source, target, l_sem.at[len(local)])
        if not name.startswith("out"):
            local[name].start()
    half = PART // 2
    barrier = pltpu.get_barrier_semaphore()
    peers = [place.at_x(d) for d in range(1, NX)] + [place.at_z(d) for d in range(1, NZ)]
    peers += [place.at_dp(d) for d in range(1, NDP)]
    for peer in peers:
        pl.semaphore_signal(barrier, inc=1, device_id=peer, device_id_type=MESH)

    gathers = {}
    for layer in range(2):
        for kind in range(3):
            for s in range(STREAMS):
                ref = gx.at[layer, s] if kind == 0 else ga.at[layer, kind - 1, s]
                index = (layer * 3 + kind) % 2 * STREAMS + s
                gathers[layer, kind, s] = Gather(place, ref, g_send.at[index], g_recv.at[index])
    weights = Weights(place, wdo, wg, wm, we, w_send, w_recv)

    local["lengths"].wait()
    lens = lengths[...].astype(F32)
    lens_rows = jnp.broadcast_to(lens, (256, 32)).astype(BF16)
    seq, col = iota((32, 256), 0), iota((32, 256), 1)
    row, other = iota((256, 256), 0), iota((256, 256), 1)
    size_slot = dot(lens_rows, ones_where(seq == jnp.bitwise_and(col, 31)))
    is_live_slot = lax.shift_right_logical(other, 5).astype(F32) < size_slot
    counted = ones_where(is_live_slot)
    size_seq = dot(lens_rows[0:8], ones_where(seq == lax.shift_right_logical(col, 3)))[0:1]
    is_live_seq = jnp.bitwise_and(iota((1, 256), 1), 7).astype(F32) < size_seq
    rank_seq = jnp.bitwise_and(other, 7) * 32 + lax.shift_right_logical(other, 3)
    number_seq = dot(counted[0:8], ones_where(row < rank_seq))[0:1]
    target = jnp.where(is_live_seq, number_seq - origin, -1.0)
    residuals = []
    local["tokens"].wait()
    for s in range(STREAMS):
        compact = ones_where((iota((PART, 256), 0) + s * PART).astype(F32) == target)
        residual = dot(compact, tokens[...]).astype(BF16)
        gathers[0, 0, s].put(residual)
        residuals.append(residual)

    counts[place.dp] = jnp.broadcast_to(jnp.sum(lens, axis=1, keepdims=True), (8, 128))

    pl.semaphore_wait(barrier, len(peers))
    for s in range(STREAMS):
        gathers[0, 0, s].start()
    local["drive"].wait()
    wdo[own512, 128:256] = drive[...].astype(F32).reshape(128, 512).T.astype(BF16)
    weights.start(0)
    local["glu"].wait()
    wg[own256, :] = glu[...].astype(F32).reshape(128, 256).T.astype(BF16)
    weights.start(1)
    local["open0"].wait()
    weights.start(7)
    local["merge0"].wait()
    weights.start(2)
    for layer in range(2):
        for e in X_ORDER:
            rows = pl.ds(pl.multiple_of((place.x + e) % NX * 128, 128), 128)
            pltpu.make_async_remote_copy(
                src_ref=leaving_h.at[layer, rows, :],
                dst_ref=we.at[layer, place.dp, :, own_lanes],
                send_sem=q_sem.at[layer, 0],
                recv_sem=q_sem.at[layer, 1],
                device_id=place.at_x(e),
                device_id_type=MESH,
            ).start()

    def quarters(layer):
        ref = we.at[layer, place.dp, :, pl.ds(0, 384)]
        copy = remote(ref, q_sem.at[layer, 0], q_sem.at[layer, 1], place.partner())
        copy.wait_recv()
        copy.wait_send()
    for d in range(1, NDP):
        remote(counts.at[place.dp], n_sem.at[0], n_sem.at[1], place.at_dp(d)).start()

    def forward(layer, kind):
        for s in range(STREAMS):
            for d in Z_ORDER:
                gathers[layer, kind, s].forward(d)

    target = jnp.where(is_live_slot[0:1], dot(counted[0:8], ones_where(row < other))[0:1] - origin, -1.0)
    for s in range(STREAMS):
        pick[s] = ones_where((iota((PART, 256), 0) + s * PART).astype(F32) == target)
    size = dot_nt(ones_where(iota((256, 32), 1) == jnp.bitwise_and(iota((256, 32), 0), 31)), lens_rows)
    number = dot_nt(ones_where(other < row), counted) - origin
    target = jnp.where(lax.shift_right_logical(row, 5).astype(F32) < size, number, -1.0)
    for s in range(STREAMS):
        spread_slot[s] = ones_where((iota((256, PART), 1) + s * PART).astype(F32) == target[:, 0:PART])
        live_slot[s] = ones_where((target >= s * PART) & (target < (s + 1) * PART), F32)
    forward(0, 0)
    quarters(0)
    quarters(1)
    for piece, name in enumerate(("exit0", "open1", "merge1", "exit1")):
        local[name].wait()
        weights.start(piece + 3)
    size = dot_nt(ones_where(iota((256, 32), 1) == lax.shift_right_logical(iota((256, 32), 0), 3)), lens_rows)
    rank = jnp.bitwise_and(row, 7) * 32 + lax.shift_right_logical(row, 3)
    number = dot_nt(ones_where(other < rank), counted) - origin
    target = jnp.where(jnp.bitwise_and(row, 7).astype(F32) < size, number, -1.0)[:, 0:128]
    for s in range(STREAMS):
        spread_seq[s] = ones_where((iota((256, PART), 1) + s * PART).astype(F32) == target[:, 0:PART])
    live_seq[...] = ones_where((target >= 0.0) & (target < ROWS), F32)

    for name in ("decay", "turn", "step", "s_in", "s_out", "skip", "gains", "carried"):
        local[name].wait()
    spread64 = ones_where(iota((64, 256), 0) == jnp.bitwise_and(iota((64, 256), 1), 63), F32)
    spread2 = ones_where(iota((64, 128), 0) == jnp.bitwise_and(iota((64, 128), 1), 63), F32)
    group4 = iota((4, 256), 0) == lax.shift_right_logical(iota((4, 256), 1), 6)
    in_group = lax.shift_right_logical(iota((64, 256), 0), 4) == lax.shift_right_logical(iota((64, 256), 1), 6)
    size_all = dot(step[...], ones_where(group4, F32), precision=HIGH)
    skip_all = dot(skip[...], spread2, precision=HIGH)
    for layer in range(2):
        rate = dot(decay[layer], spread64, precision=HIGH)
        rate = jnp.sum(jnp.where(group4, rate, 0.0), axis=0, keepdims=True)
        turning = dot(turn[layer], spread64, precision=HIGH)
        turning = jnp.sum(jnp.where(group4, turning, 0.0), axis=0, keepdims=True)
        length = size_all[layer : layer + 1]
        real = -rate
        magnitude = jnp.exp(length * real)
        decay_real = magnitude * jnp.cos(length * turning)
        decay_imag = magnitude * jnp.sin(length * turning)
        divisor = real * real + turning * turning
        params[layer, 0:1, :] = decay_real
        params[layer, 1:2, :] = decay_imag
        params[layer, 2:3, :] = ((decay_real - 1.0) * real + decay_imag * turning) / divisor
        params[layer, 3:4, :] = (decay_imag * real - (decay_real - 1.0) * turning) / divisor
        params[layer, 4:5, 0:128] = skip_all[layer : layer + 1]
        for part in range(2):
            lanes = slice(part * 256, part * 256 + 256)
            wide = jnp.where(in_group, dot(s_in[layer, part], spread64, precision=HIGH), 0.0)
            high = wide.astype(BF16)
            low = (wide - high.astype(F32)).astype(BF16)
            for k in range(2):
                inject[layer, k * 64 : k * 64 + 64, lanes] = high
                inject[layer, 128 + k * 64 : 192 + k * 64, lanes] = low
            wide = jnp.where(in_group, dot(s_out[layer, part], spread64, precision=HIGH), 0.0)
            wide = (wide if part == 0 else -wide).astype(BF16)
            readout_w[layer, 0:64, lanes] = wide
            readout_w[layer, 64:128, lanes] = wide
    weights.forward(0)

    lane = iota((PART, 128), 1)
    lane_half = iota((half, 128), 1)
    low256 = iota((256, 128), 1) < 64

    def build_gp():
        zero = jnp.zeros((256, 128), BF16)
        for k in range(8):
            plain = wg[k * 256 : k * 256 + 256, :]
            turned = swap_halves(plain.astype(F32)).astype(BF16)
            for layer in range(2):
                first, second = (plain, turned) if layer == 0 else (turned, plain)
                top = jnp.where(low256, first, zero).reshape(4, 64, 128)
                bottom = jnp.where(low256, zero, second).reshape(4, 64, 128)
                gp[layer, k * 512 : k * 512 + 512, :] = jnp.concatenate([top, bottom], axis=1).reshape(512, 128)

    def build_mp(layer):
        zero = jnp.zeros((4, 64, 128), BF16)
        for k in range(8):
            plain = wm[layer, k * 256 : k * 256 + 256, :].reshape(4, 64, 128)
            mp[layer, k * 512 : k * 512 + 512, 0:128] = jnp.concatenate([plain, zero], axis=1).reshape(512, 128)
            mp[layer, k * 512 : k * 512 + 512, 128:256] = jnp.concatenate([zero, plain], axis=1).reshape(512, 128)

    def project(buf, weight):
        total = None
        for k in range(NZ):
            term = dot(buf[k], weight(k * 512, 512))
            total = term if total is None else total + term
        return total

    gates, branches, waiting = {}, {}, []

    def enter(layer, s, buf):
        squares = None
        for k in range(NZ):
            value = buf[k].astype(F32)
            term = jnp.sum(value * value, axis=1, keepdims=True)
            squares = term if squares is None else squares + term
        inverse = lax.rsqrt(squares / (NZ * 512.0) + EPS)
        both = None
        for k in range(NZ):
            gain = gains[layer : layer + 1, k * 512 : k * 512 + 512]
            normed = (buf[k].astype(F32) * inverse * gain).astype(BF16)
            nx[s, k] = normed
            term = dot(normed, wdo[k * 512 : k * 512 + 512, 128:256])
            both = term if both is None else both + term
        mine = lane < 64 if layer == 0 else lane >= 64
        drives = jnp.where(mine, both, swap_halves(both))
        high = drives.astype(BF16).astype(F32)
        split = jnp.where(lane < 64, high, drives - high).astype(BF16)
        spread = dot(spread_slot[s], split).astype(BF16)
        moved = dot(jnp.concatenate([spread, spread], axis=1), inject[layer])
        hold_real, hold_imag = params[layer, 2:3, :], params[layer, 3:4, :]
        pushed[:, 0:256] = hold_real * moved[:, 0:256] - hold_imag * moved[:, 256:512]
        pushed[:, 256:512] = hold_real * moved[:, 256:512] + hold_imag * moved[:, 0:256]
        decay_real = jnp.broadcast_to(params[layer, 0:1, :], (32, 256))
        decay_imag = jnp.broadcast_to(params[layer, 1:2, :], (32, 256))
        before = carried if s == 0 else out_state
        state_real, state_imag = before[layer, 0], before[layer, 1]
        for t in range(8):
            now = slice(t * 32, t * 32 + 32)
            alive = live_slot[s, now, :] > 0.5
            next_real = decay_real * state_real - decay_imag * state_imag + pushed[now, 0:256]
            next_imag = decay_real * state_imag + decay_imag * state_real + pushed[now, 256:512]
            state_real = jnp.where(alive, next_real, state_real)
            state_imag = jnp.where(alive, next_imag, state_imag)
            trail[now, 0:256] = state_real.astype(BF16)
            trail[now, 256:512] = state_imag.astype(BF16)
        out_state[layer, 0] = state_real
        out_state[layer, 1] = state_imag
        chosen = dot(pick[s], trail[...]).astype(BF16)
        readout = dot_nt(chosen, readout_w[layer]) + params[layer, 4:5, 0:128] * drives
        inner = math.sqrt(2.0 / math.pi) * (readout + 0.044715 * (readout * readout * readout))
        activated = (readout * (0.5 * (1.0 + jnp.tanh(inner)))).astype(BF16).astype(F32)
        packed = jnp.where(lane_half < 64, activated[0:half], activated[half:PART])
        branches[s] = packed
        return packed.astype(BF16)

    def open_gates(layer):
        weights.finish(7 if layer == 0 else 4)
        for s in range(STREAMS):
            total = project(
                nx.at[s], lambda k, n: wdo[k : k + n, layer * 256 : layer * 256 + 128]
            )
            gates[s] = jax.nn.sigmoid(total)

    def switch(layer, s, buf):
        gating = project(buf, lambda k, n: gp[layer, k : k + n, :])
        return (branches[s] * jax.nn.sigmoid(gating)).astype(BF16)

    def join(layer, s, buf):
        merged = project(buf, lambda k, n: mp[layer, k : k + n, :])
        merged = jnp.concatenate([merged[:, 0:128], merged[:, 128:256]], axis=0)
        return (gates[s] * merged).astype(BF16)

    def spread_mixed(layer, s, value):
        lanes = pl.ds(pl.multiple_of(place.z * LANES, LANES), LANES)
        gm[layer, s, :, lanes] = value
        for d in Z_FAR:
            ref = gm.at[layer, s, :, lanes]
            remote(ref, e_sem.at[layer, s, 0], e_sem.at[layer, s, 1], place.at_z(d)).start()

    def leave(layer, s):
        ref = gm.at[layer, s, :, pl.ds(0, 896)]
        copy = remote(ref, e_sem.at[layer, s, 0], e_sem.at[layer, s, 1], place.partner())
        copy.wait_recv()
        waiting.append(copy)
        partial = dot(gm[layer, s], we[layer].reshape(1024, 512)).astype(BF16)
        for k in range(NX):
            tx[layer, s, k] = partial[:, k * 128 : k * 128 + 128]
        for e in X_ORDER:
            pltpu.make_async_remote_copy(
                src_ref=tx.at[layer, s, (place.x + e) % NX],
                dst_ref=rx.at[layer, s, place.x],
                send_sem=e_sem.at[layer, s, 2],
                recv_sem=e_sem.at[layer, s, 3],
                device_id=place.at_x(e),
                device_id_type=MESH,
            ).start()
        rx[layer, s, place.x] = tx[layer, s, place.x]

    def settle(layer, s):
        ref = rx.at[layer, s, pl.ds(0, 3)]
        copy = remote(ref, e_sem.at[layer, s, 2], e_sem.at[layer, s, 3], place.partner())
        copy.wait_recv()
        waiting.append(copy)
        branch = rx[layer, s, 0].astype(F32)
        for k in range(1, NX):
            branch = branch + rx[layer, s, k].astype(F32)
        residuals[s] = (residuals[s].astype(F32) + branch).astype(BF16)
        return residuals[s]

    def ready(layer, kind):
        if kind == 0 and layer == 0:
            weights.finish(0)
        elif kind == 1 and layer == 0:
            weights.finish(1)
            build_gp()
        elif kind == 2:
            weights.finish(2 + 3 * layer)
            build_mp(layer)
        elif kind == 3:
            weights.finish(3 + 3 * layer)

    relays = {(0, 0): (1, 7, 2), (0, 1): (3, 4), (0, 2): (5, 6)}
    for layer in range(2):
        for kind, compute in enumerate((enter, switch, join)):
            ready(layer, kind)
            for s in range(STREAMS):
                done = gathers[layer, kind, s]
                done.finish()
                value = compute(layer, s, done.buf)
                if kind < 2:
                    gathers[layer, kind + 1, s].put(value)
                    gathers[layer, kind + 1, s].start()
                else:
                    spread_mixed(layer, s, value)
            if kind < 2:
                forward(layer, kind + 1)
            for s in range(STREAMS):
                gathers[layer, kind, s].drain()
            if kind == 0:
                local[f"out{layer}"].start()
            for piece in relays.get((layer, kind), ()):
                weights.forward(piece)
            if kind == 0:
                open_gates(layer)
        ready(layer, 3)
        for s in range(STREAMS):
            leave(layer, s)
        for s in range(STREAMS):
            value = settle(layer, s)
            if layer == 0:
                gathers[1, 0, s].put(value)
                gathers[1, 0, s].start()
        if layer == 0:
            forward(1, 0)

    spread = None
    for s in range(STREAMS):
        term = dot(spread_seq[s], residuals[s])
        spread = term if spread is None else spread + term
    out_tokens[...] = jnp.where(live_seq[...] > 0.5, spread.astype(BF16), tokens[...])
    local["out_tokens"].start()
    theirs = remote(counts.at[pl.ds(0, NDP - 1)], n_sem.at[0], n_sem.at[1], place.partner())
    theirs.wait_recv()
    theirs.wait_send()
    out_more[0, 0] = (jnp.max(counts[...]) > ROWS).astype(jnp.int32)
    weights.drain()
    for copy in waiting:
        copy.wait_send()
    for name in ("out0", "out1", "out_tokens"):
        local[name].wait()


def layers(number):
    anywhere = pl.BlockSpec(memory_space=pltpu.HBM)
    half = PART // 2
    gather_count = 2 * STREAMS
    return pl.pallas_call(
        functools.partial(kernel, float(number * ROWS)),
        name=f"layers_{number}",
        out_shape=(
            jax.ShapeDtypeStruct((256, 128), BF16),
            jax.ShapeDtypeStruct((2, 2, 32, 256), F32),
            jax.ShapeDtypeStruct((1, 1), jnp.int32),
        ),
        in_specs=[anywhere] * 15,
        out_specs=(anywhere, anywhere, pl.BlockSpec(memory_space=pltpu.SMEM)),
        scratch_shapes=[
            pltpu.VMEM((256, 128), BF16),
            pltpu.VMEM((1, 32), jnp.int32),
            pltpu.VMEM((2, 4096), F32),
            pltpu.VMEM((2, 64, 512), BF16),
            pltpu.VMEM((2, 64, 256), BF16),
            pltpu.VMEM((2, 4, 64), F32),
            pltpu.VMEM((2, 4, 64), F32),
            pltpu.VMEM((2, 4), F32),
            pltpu.VMEM((2, 2, 64, 64), F32),
            pltpu.VMEM((2, 2, 64, 64), F32),
            pltpu.VMEM((2, 64), F32),
            pltpu.VMEM((2, 2, 32, 256), F32),
            pltpu.VMEM((256, 128), BF16),
            pltpu.VMEM((2, 2, 32, 256), F32),
            pltpu.VMEM((4096, 384), BF16),
            pltpu.VMEM((2048, 128), BF16),
            pltpu.VMEM((2, 2048, 128), BF16),
            pltpu.VMEM((2, NDP, 128, 512), BF16),
            pltpu.VMEM((2, 4096, 128), BF16),
            pltpu.VMEM((2, 4096, 256), BF16),
            pltpu.VMEM((2, STREAMS, NZ, PART, 512), BF16),
            pltpu.VMEM((2, 2, STREAMS, NZ, half, 512), BF16),
            pltpu.VMEM((2, STREAMS, PART, 1024), BF16),
            pltpu.VMEM((STREAMS, NZ, PART, 512), BF16),
            pltpu.VMEM((2, STREAMS, NX, PART, 128), BF16),
            pltpu.VMEM((2, STREAMS, NX, PART, 128), BF16),
            pltpu.VMEM((STREAMS, PART, 256), BF16),
            pltpu.VMEM((STREAMS, 256, PART), BF16),
            pltpu.VMEM((STREAMS, 256, PART), BF16),
            pltpu.VMEM((256, 128), F32),
            pltpu.VMEM((STREAMS, 256, 256), F32),
            pltpu.VMEM((2, 8, 256), F32),
            pltpu.VMEM((2, 256, 512), BF16),
            pltpu.VMEM((2, 128, 512), BF16),
            pltpu.VMEM((256, 512), F32),
            pltpu.VMEM((256, 512), BF16),
            pltpu.VMEM((NDP, 8, 128), F32),
            pltpu.SemaphoreType.DMA((PIECES,)),
            pltpu.SemaphoreType.DMA((PIECES, 4)),
            pltpu.SemaphoreType.DMA((gather_count, 2)),
            pltpu.SemaphoreType.DMA((gather_count, 8)),
            pltpu.SemaphoreType.DMA((2,)),
            pltpu.SemaphoreType.DMA((21,)),
            pltpu.SemaphoreType.DMA((2, 2)),
            pltpu.SemaphoreType.DMA((2, STREAMS, 4)),
        ],
        compiler_params=pltpu.CompilerParams(
            collective_id=number, has_side_effects=True, vmem_limit_bytes=60 * 1024 * 1024
        ),
    )


def shards(tokens, lengths, norm_gains, drive, opening, glu, merge, leaving, decay, turn, step, s_in, s_out, skip, carried):
    lengths = lengths.reshape(1, 32)
    rest = (
        norm_gains,
        drive.swapaxes(1, 2),
        opening,
        glu.swapaxes(1, 2),
        merge,
        leaving,
        decay,
        turn,
        step,
        s_in.swapaxes(3, 4).reshape(2, 2, 64, 64),
        s_out.reshape(2, 2, 64, 64),
        skip,
    )

    def some(number, tokens, state):
        return layers(number)(tokens, lengths, *rest, state)

    updated, state, more = some(0, tokens.reshape(256, 128), carried)
    updated, state = lax.cond(
        more[0, 0] != 0,
        lambda tokens, state: some(1, tokens, state)[0:2],
        lambda tokens, state: (tokens, state),
        updated,
        state,
    )
    return updated.reshape(32, 8, 128), state


def solution(mesh):
    placed = (
        P("dp", None, "tp"),
        P("dp"),
        P(),
        P(None, "dp", "tp"),
        P(None, "dp", "tp"),
        P(None, "dp", "tp"),
        P(None, "dp", "tp"),
        P(None, "dp", "tp"),
        P(None, "tp", None),
        P(None, "tp", None),
        P(None, "tp"),
        P(None, None, "tp", None, None),
        P(None, None, "tp", None, None),
        P(None, "tp"),
        P(None, None, "dp", "tp"),
    )
    return jax.shard_map(
        shards,
        mesh=mesh,
        in_specs=placed,
        out_specs=(P("dp", None, "tp"), P(None, None, "dp", "tp")),
        check_vma=False,
    )
```
